128 devices in a mesh: sp: 16 (over z, x), dp: 8 (over y, core).
Axes of the slice: x: 4, y: 4, z: 4, core: 2. Of those that a mesh axis runs over, the one named last changes fastest.
Arguments:
- hidden_in: bfloat16 [8, 2048, 2048], P('dp', 'sp'), may hold values from -6 to 6
- mix_cotangent: bfloat16 [8, 2048, 4096], P('dp', 'sp'), may hold values from -0.119628906 to 0.119628906
- query_weight: bfloat16 [2048, 4096], P('dp', 'sp'), may hold values from -0.125 to 0.125
- key_weight: bfloat16 [2048, 4096], P('dp', 'sp'), may hold values from -0.125 to 0.125
- value_weight: bfloat16 [2048, 4096], P('dp', 'sp'), may hold values from -0.125 to 0.125
- decay_log: float32 [16], P('sp'), may hold values from -0.034 to -0.000146484375, as said below
Outputs:
- grad_hidden: bfloat16 [8, 2048, 2048], P('dp', 'sp')
- grad_query: float32 [2048, 4096], P('dp', 'sp')
- grad_key: float32 [2048, 4096], P('dp', 'sp')
- grad_value: float32 [2048, 4096], P('dp', 'sp')
The draws below stay inside these ranges and needn't reach their ends.
Inputs may be any that keep to these rules, and one draw needn't show every extreme that they name: Each head's decay_log is negative.
All inputs are finite; a program needn't handle non-finite values.
Results may differ from the reference program's by a relative error of at most 0.015.
Values may be sent and summed in bfloat16 or wider, within the bound.
A program may use at most 64 MiB of HBM per device.

```python
import jax
import jax.numpy as jnp
from jax import lax

D = 2048
HEADS = 16
BLOCK = 128
WIDTH = 4096
SEQ_LEN = 2048
SEQS = 8
N_SP = 16


def draw_decay_log(key, part):
    key_fast = jax.random.fold_in(key, 11)
    key_quick = jax.random.fold_in(key, 12)
    key_slow = jax.random.fold_in(key, 13)
    fast = jax.random.bernoulli(key_fast, 0.5, (HEADS,))
    quick_rate = jax.random.uniform(key_quick, (HEADS,), jnp.float32, 0.01, 0.034)
    slow_rate = jax.random.uniform(key_slow, (HEADS,), jnp.float32, 0.3, 2.0) / SEQ_LEN
    return -jnp.where(fast, quick_rate, slow_rate).astype(jnp.float32)


def block_levels(own_key, extent, cuts, smallest, largest):
    gain = 1.0
    for position, parts in cuts:
        heights = jax.random.uniform(jax.random.fold_in(jax.random.fold_in(own_key, 6), position), (parts,), jnp.float32, smallest / len(cuts), largest / len(cuts))
        gain = gain * jnp.repeat(jnp.exp(heights), extent[position] // parts).reshape((-1,) + (1,) * (len(extent) - 1 - position))
    return gain


def noise(rng, extent, scale, reach, split=(), kind=jnp.bfloat16):
    array = scale * jax.random.normal(rng, extent, jnp.float32)
    if split:
        array = array * block_levels(rng, extent, split, -0.22, 0.18)
    return jnp.clip(array, -reach, reach).astype(kind)


def setup_inputs(seed: int = 0) -> dict:
    seeds = jax.random.split(jax.random.key(seed), 7)
    return {
        "hidden_in": noise(seeds[0], (SEQS, SEQ_LEN, D), 1.0, 6.0, ((0, 8), (1, 16))),
        "mix_cotangent": noise(seeds[1], (SEQS, SEQ_LEN, WIDTH), 0.02, 0.119628906, ((0, 8), (1, 16))),
        "query_weight": noise(seeds[2], (D, WIDTH), D ** -0.5, 0.125, ((0, 8), (1, 16))),
        "key_weight": noise(seeds[3], (D, WIDTH), D ** -0.5, 0.125, ((0, 8), (1, 16))),
        "value_weight": noise(seeds[4], (D, WIDTH), D ** -0.5, 0.125, ((0, 8), (1, 16))),
        "decay_log": draw_decay_log(jax.random.fold_in(seeds[6], 71), 0),
    }


def head_grads(queries, key_rows, values, cotangent, log_rate):
    length = queries.shape[0]
    head_dim = queries.shape[1]
    blocks = length // BLOCK
    scale = head_dim ** -0.5
    keys_scaled = (key_rows.astype(jnp.float32) * scale).astype(jnp.bfloat16)
    offsets = jnp.arange(BLOCK, dtype=jnp.float32)
    spread = offsets[:, None] - offsets[None, :]
    inner_decay = jnp.where(spread >= 0, jnp.exp(log_rate * jnp.maximum(spread, 0.0)), 0.0)
    query_decay = jnp.exp(log_rate * (offsets + 1.0))
    key_decay = jnp.exp(log_rate * (BLOCK - 1.0 - offsets))
    block_decay = jnp.exp(log_rate * BLOCK)

    def split_blocks(series):
        return series.reshape(blocks, BLOCK, series.shape[-1])

    def forward(carried, inputs):
        query_block, key_block, value_block, grad_block = inputs
        mixed = (jnp.dot(grad_block, value_block.T, preferred_element_type=jnp.float32) * inner_decay).astype(jnp.bfloat16)
        within = jnp.dot(mixed, key_block, preferred_element_type=jnp.float32)
        across = jnp.dot(grad_block, carried.astype(jnp.bfloat16).T, preferred_element_type=jnp.float32) * query_decay[:, None]
        weighted = (key_block.astype(jnp.float32) * key_decay[:, None]).astype(jnp.bfloat16)
        updated = carried * block_decay + jnp.dot(weighted.T, value_block, preferred_element_type=jnp.float32)
        return updated, (within + across, mixed)

    def backward(carried, inputs):
        query_block, key_block, value_block, grad_block, mixed = inputs
        scores = (jnp.dot(query_block, key_block.T, preferred_element_type=jnp.float32) * inner_decay).astype(jnp.bfloat16)
        state_bf = carried.astype(jnp.bfloat16)
        grad_v = jnp.dot(scores.T, grad_block, preferred_element_type=jnp.float32) + jnp.dot(key_block, state_bf, preferred_element_type=jnp.float32) * key_decay[:, None]
        grad_k = (jnp.dot(mixed.T, query_block, preferred_element_type=jnp.float32) + jnp.dot(value_block, state_bf.T, preferred_element_type=jnp.float32) * key_decay[:, None]) * scale
        weighted = (query_block.astype(jnp.float32) * query_decay[:, None]).astype(jnp.bfloat16)
        updated = carried * block_decay + jnp.dot(weighted.T, grad_block, preferred_element_type=jnp.float32)
        return updated, (grad_k, grad_v)

    inputs = (split_blocks(queries), split_blocks(keys_scaled), split_blocks(values), split_blocks(cotangent))
    initial = jnp.zeros((head_dim, values.shape[-1]), jnp.float32)
    final_state, (grad_q, mixed_all) = lax.scan(forward, initial, inputs)
    final_back, (grad_k, grad_v) = lax.scan(backward, initial, inputs + (mixed_all,), reverse=True)
    return grad_q.reshape(length, -1), grad_k.reshape(length, -1), grad_v.reshape(length, -1)


def group_grads(log_rates, queries, key_rows, values, cotangent):
    length = queries.shape[0]
    head_count = log_rates.shape[0]

    def by_head(series):
        return series.reshape(length, head_count, -1).transpose(1, 0, 2)

    def to_rows(series):
        return series.transpose(1, 0, 2).reshape(length, -1)

    grad_q, grad_k, grad_v = jax.vmap(head_grads)(by_head(queries), by_head(key_rows), by_head(values), by_head(cotangent), log_rates)
    return jnp.concatenate((to_rows(grad_q), to_rows(grad_k), to_rows(grad_v)), axis=1).astype(jnp.bfloat16)


def reference(hidden_in, mix_cotangent, query_weight, key_weight, value_weight, decay_log):
    weights = jnp.concatenate((query_weight, key_weight, value_weight), axis=1)
    all_width = query_weight.shape[1]
    model_width = query_weight.shape[0]

    def one_sequence(seq_pair):
        seq_rows, seq_cotangent = seq_pair
        projected = jnp.dot(seq_rows, weights, preferred_element_type=jnp.float32).astype(jnp.bfloat16)
        gradients = group_grads(decay_log, projected[:, :all_width], projected[:, all_width:2 * all_width], projected[:, 2 * all_width:], seq_cotangent)
        length = seq_rows.shape[0]
        split_grads = gradients.reshape(length, 3, N_SP, -1).astype(jnp.float32)
        split_weights = weights.reshape(model_width, 3, N_SP, -1).astype(jnp.float32)
        partials = jnp.einsum('ltgc,dtgc->gld', split_grads, split_weights)
        rounded = lax.optimization_barrier(partials.astype(jnp.bfloat16)).astype(jnp.float32)
        return jnp.sum(rounded, axis=0).astype(jnp.bfloat16), gradients

    grad_hidden, all_grads = lax.map(one_sequence, (hidden_in, mix_cotangent))
    flat_rows = hidden_in.reshape(-1, model_width)
    flat_grads = all_grads.reshape(-1, 3 * all_width)
    summed = lax.dot_general(flat_rows, flat_grads, (((0,), (0,)), ((), ())), preferred_element_type=jnp.float32) / SEQS
    return grad_hidden, summed[:, :all_width], summed[:, all_width:2 * all_width], summed[:, 2 * all_width:]
```

```python
import functools

import jax
import jax.numpy as jnp
from jax import lax
from jax.experimental import pallas as pl
from jax.experimental.pallas import tpu as pltpu
from jax.sharding import PartitionSpec as P

BLOCK = 128
SIDE = 4
FIRST = 640
F32 = jnp.float32
BF16 = jnp.bfloat16
MESH = pl.DeviceIdType.MESH
NN = (((1,), (0,)), ((), ()))
NT = (((1,), (1,)), ((), ()))
TN = (((0,), (0,)), ((), ()))
VMEM_LIMIT = 60 * 1024 * 1024
SEMS = 160


def dot(a, b, dims=NN):
    return lax.dot_general(a, b, dims, preferred_element_type=F32)


def span(start, size, step):
    return pl.ds(pl.multiple_of(start, step), size)


class Net:
    def __init__(self, send, recv, somewhere):
        self.send, self.recv, self.somewhere = send, recv, somewhere
        self.names, self.starts, self.pending = {}, 0, []

    def index(self, name, width=1):
        if name not in self.names:
            self.names[name] = sum(w for _, w in self.names.values()), width
        return self.names[name][0]

    def start(self, name, src, dst, where, offset=0, width=1, when=None):
        slot = self.index(name, width) + offset
        lane = self.starts
        self.starts += 1

        def make():
            return pltpu.make_async_remote_copy(
                src_ref=src, dst_ref=dst, send_sem=self.send.at[lane], recv_sem=self.recv.at[slot],
                device_id=where, device_id_type=MESH,
            )

        if when is None:
            make().start()
        else:
            pl.when(when)(lambda: make().start())
        self.pending.append((when, make))

    def wait(self, name, dst, offset=0, width=1, when=None):
        slot = self.index(name, width) + offset

        def run():
            pltpu.make_async_remote_copy(
                src_ref=dst, dst_ref=dst, send_sem=self.send.at[0], recv_sem=self.recv.at[slot],
                device_id=self.somewhere, device_id_type=MESH,
            ).wait_recv()

        if when is None:
            run()
        else:
            pl.when(when)(run)

    def drain(self):
        for when, make in self.pending:
            if when is None:
                make().wait_send()
            else:
                pl.when(when)(lambda make=make: make().wait_send())


def whole_kernel(
    rate, h_in, c_in, wq, wk, wv, dh, dq, dk, dv,
    h_all, c_all, w_all, p_all, g_all, state, back, rates, inner, inner_t, decays,
    pout, pin, psum, ra1, ra2, ra3, rb0, rb1, rb2, dbuf,
    ysend, yone, ykeep, yhome, yr1, yr2, yout, yend, send, recv,
):
    s = lax.axis_index("sp")
    d = lax.axis_index("dp")
    z, x = s // SIDE, s % SIDE
    y, c = d // 2, d % 2
    u = x // 2
    xl = x - 2 * u
    own = c == u
    away = c != u
    rows, width = h_in.shape
    depth, columns = wq.shape
    half = width // 2
    four = rows * SIDE
    two = rows * 2
    blocks = SIDE * SIDE
    scale = columns ** (-0.5)

    def at(zz=None, xx=None, yy=None, cc=None):
        zz, xx = z if zz is None else zz, x if xx is None else xx
        yy, cc = y if yy is None else yy, c if cc is None else cc
        return {"sp": zz * SIDE + xx, "dp": yy * 2 + cc}

    def turned(v, by):
        return (v + by + SIDE) % SIDE

    mate = at(cc=1 - c)
    pair = at(xx=x + 1 - 2 * xl)
    zs = {1: at(zz=turned(z, 1)), -1: at(zz=turned(z, -1))}
    ys = {1: at(yy=turned(y, 1)), -1: at(yy=turned(y, -1))}
    cross = 3 - x
    net = Net(send, recv, mate)

    barrier = pltpu.get_barrier_semaphore()
    peers = [mate, ys[1], ys[-1]]
    for k in range(1, blocks):
        other = (s + k) % blocks
        peers += [{"sp": other, "dp": d}, {"sp": other, "dp": y * 2 + 1 - c}]
    for where in peers:
        pl.semaphore_signal(barrier, inc=1, device_id=where, device_id_type=MESH)
    rates[0] = jnp.full(rates.shape[1:], rate[0], F32)
    pl.semaphore_wait(barrier, len(peers))

    def slot(r, col, b):
        return turned(z, r) * SIDE + 2 * (xl if col == 0 else 1 - xl) + b

    def h_ref(place, part, which):
        base = which * half
        lo, size = {"f": (0, half), "a": (0, FIRST), "b": (FIRST, half - FIRST)}[part]
        return h_all.at[span(place * rows, rows, rows), span(base + lo, size, 128)]

    def h_send(r, col, b, part, where, name):
        ref = h_ref(slot(r, col, b), part, c)
        net.start(name, ref, ref, where)

    def to_mate(r, col, b, part):
        h_send(r, col, b, part, mate, ("m", r, col, b, part))

    def h_wait(r, col, b, part, when=None):
        net.wait(("x", r, col, b, part), h_ref(slot(r, col, b), part, c), when=when)

    def w_ref(yy, cc, j):
        return w_all.at[span((yy * 2 + cc) * depth, depth, depth), pl.ds(j * columns, columns)]

    def w_first(j, w):
        ref = w_ref(y, c, j)
        net.start(("w0", j), w, ref, at(xx=cross, cc=u), offset=c, width=2)
        net.start(("w0", j), w, ref, mate, offset=c, width=2, when=away)

    weights = (wq, wk, wv)
    mine = span(c * half, half, half)
    theirs = span((1 - c) * half, half, half)
    net.start(("x", 0, 0, 0, "f"), h_in.at[:, theirs], h_ref(slot(0, 0, 0), "f", 1 - c), mate, when=own)
    w_first(0, wq)
    there = z * SIDE + 2 * (1 - xl) + 1
    for hf in range(2):
        net.start(
            ("x", 0, 0, 1, "f"), h_in.at[:, pl.ds(hf * half, half)], h_ref(there, "f", hf),
            at(xx=cross, cc=hf), when=away,
        )
    w_first(1, wk)
    w_first(2, wv)
    net.start(("rate",), rates.at[0], rates.at[1], at(xx=cross))

    @pl.when(own)
    def _():
        h_all[span(slot(0, 0, 0) * rows, rows, rows), mine] = h_in[:, mine]
        for j in range(3):
            w_all[span(d * depth, depth, depth), j * columns : (j + 1) * columns] = weights[j][...]

    def spread(b):
        for way in (1, -1):
            h_send(0, 0, b, "f", zs[way], ("x", -way, 0, b, "f"))
        h_send(0, 0, b, "f", pair, ("x", 0, 1, b, "f"))
        to_mate(0, 0, b, "f")

    def w_spread(j):
        for cc in range(2):
            net.wait(("w0", j), w_ref(y, cc, j), offset=cc, width=2, when=jnp.logical_or(away, c != cc))
            for way in (1, -1):
                net.start(("w1", j, -way, cc), w_ref(y, cc, j), w_ref(y, cc, j), ys[way])

    def w_forward(j):
        for way, cc in ((1, 0), (-1, 1)):
            ref = w_ref(turned(y, -way), cc, j)
            net.wait(("w1", j, -way, cc), ref)
            net.start(("w2", j, cc), ref, ref, ys[way])

    def from_pair(b):
        h_wait(0, 1, b, "f")
        for way in (1, -1):
            h_send(0, 1, b, "a", zs[way], ("x", -way, 1, b, "a"))
        to_mate(0, 1, b, "f")

    def from_side(b):
        fast = 1 if b == 0 else -1
        for r in (-fast, fast):
            h_wait(r, 0, b, "f")
            if r == -fast:
                h_send(r, 0, b, "f", zs[fast], ("x", 2, 0, b, "f"))
            h_send(r, 0, b, "b", pair, ("x", r, 1, b, "b"))
            to_mate(r, 0, b, "f")

    def from_corner(b):
        fast = 1 if b == 0 else -1
        for r in (-fast, fast):
            h_wait(r, 1, b, "a")
            if r == -fast:
                h_send(r, 1, b, "a", zs[fast], ("x", 2, 1, b, "a"))
            to_mate(r, 1, b, "a")

    h_wait(0, 0, 0, "f", when=away)
    spread(0)
    w_spread(0)
    h_wait(0, 0, 1, "f")
    spread(1)
    w_spread(1)
    from_pair(0)
    from_side(0)
    w_spread(2)
    w_forward(0)
    from_pair(1)
    from_side(1)
    from_corner(0)
    w_forward(1)
    from_corner(1)
    for b in range(2):
        h_wait(2, 0, b, "f")
        h_send(2, 0, b, "b", pair, ("x", 2, 1, b, "b"))
        to_mate(2, 0, b, "f")
    w_forward(2)

    def c_send(hop, when=None):
        head = (s + hop) % blocks
        hz, hx = head // SIDE, head % SIDE
        far = (hx // 2 - c) * (hx // 2 - c)
        net.start(
            ("c",), c_in.at[:, span(head * columns, columns, columns)],
            c_all.at[span(s * rows, rows, rows)],
            {"sp": hz * SIDE + hx + far * (3 - 2 * hx), "dp": y * 2 + c + far * (1 - 2 * c)},
            offset=s, width=blocks, when=when,
        )

    c_send(0, when=away)
    for hop in range(1, blocks):
        c_send(hop)

    @pl.when(own)
    def _():
        c_all[span(s * rows, rows, rows), :] = c_in[:, span(s * columns, columns, columns)]

    for r in (-1, 1):
        for b in range(2):
            h_wait(r, 1, b, "b")
            to_mate(r, 1, b, "b")
    for b in range(2):
        h_wait(2, 1, b, "a")
        to_mate(2, 1, b, "a")
    for b in range(2):
        h_wait(2, 1, b, "b")
        to_mate(2, 1, b, "b")

    for j in range(3):
        for way, cc in ((1, 1), (-1, 0)):
            net.wait(("w1", j, -way, cc), w_ref(turned(y, -way), cc, j))
        for cc in range(2):
            net.wait(("w2", j, cc), w_ref(turned(y, 2), cc, j))

    def mate_wait(r):
        for col in range(2):
            for b in range(2):
                for part in ("f",) if col == 0 or r == 0 else ("a", "b"):
                    net.wait(("m", r, col, b, part), h_ref(slot(r, col, b), part, 1 - c))

    def project(r, j):
        place = span(turned(z, r) * four, four, four)
        cols = span(j * columns, columns, columns)
        value = dot(h_all[place, :], w_all[:, cols]).astype(BF16)
        factor = jnp.where(j == 1, scale, 1.0).astype(F32)
        p_all[place, cols] = (value.astype(F32) * factor).astype(BF16)

    for r in (0, 1, -1):
        mate_wait(r)

    @pl.loop(0, 9)
    def _(t):
        o = t // 3
        project(o + o // 2, t % 3)

    mate_wait(2)

    @pl.loop(0, 3)
    def _(j):
        project(2, j)

    net.wait(("rate",), rates.at[1])
    for k in range(blocks):
        source = (s + k) % blocks
        net.wait(
            ("c",), c_all.at[span(source * rows, rows, rows)], offset=source, width=blocks,
            when=away if k == 0 else None,
        )

    pick = jnp.where(own, 1.0, 0.0).astype(F32)
    g = rates[0] * pick + rates[1] * (1.0 - pick)
    g_row = g[0:1, :]
    gap = (
        lax.broadcasted_iota(jnp.int32, (BLOCK, BLOCK), 0) - lax.broadcasted_iota(jnp.int32, (BLOCK, BLOCK), 1)
    ).astype(F32)
    place = lax.broadcasted_iota(jnp.int32, (BLOCK, columns), 0).astype(F32)
    g_sq = g_row[:, :BLOCK]
    inner[...] = jnp.where(gap >= 0, jnp.exp(g_sq * jnp.maximum(gap, 0.0)), 0.0)
    inner_t[...] = jnp.where(gap <= 0, jnp.exp(g_sq * jnp.maximum(-gap, 0.0)), 0.0)
    decays[0] = jnp.exp(g_row * (place + 1.0))
    decays[1] = jnp.exp(g_row * (BLOCK - 1.0 - place))
    block_decay = jnp.exp(g_row * BLOCK)
    state[...] = jnp.zeros_like(state)
    back[...] = jnp.zeros_like(back)
    parts = [slice(j * columns, (j + 1) * columns) for j in range(3)]

    def slot_of(i):
        iz, ix = i // SIDE, i % SIDE
        b = (ix // 2 - u) * (ix // 2 - u)
        return iz * SIDE + 2 * (ix + b * (3 - 2 * ix) - 2 * u) + b

    @pl.loop(0, blocks)
    def _(i):
        put = span(slot_of(i) * BLOCK, BLOCK, BLOCK)
        k, v = p_all[put, parts[1]], p_all[put, parts[2]]
        ct = c_all[span(i * BLOCK, BLOCK, BLOCK), :]
        mixed = (dot(ct, v, NT) * inner[...]).astype(BF16)
        held = state[...]
        grad_q = dot(mixed, k) + dot(ct, held.astype(BF16), NT) * decays[0]
        weighted = (k.astype(F32) * decays[1]).astype(BF16)
        state[...] = held * block_decay + dot(weighted, v, TN)
        g_all[put, parts[0]] = grad_q.astype(BF16)

        i = blocks - 1 - i
        put = span(slot_of(i) * BLOCK, BLOCK, BLOCK)
        q, k, v = (p_all[put, part] for part in parts)
        ct = c_all[span(i * BLOCK, BLOCK, BLOCK), :]
        mixed_t = (dot(v, ct, NT) * inner_t[...]).astype(BF16)
        scores_t = (dot(k, q, NT) * inner_t[...]).astype(BF16)
        held = back[...]
        held_bf = held.astype(BF16)
        grad_v = dot(scores_t, ct) + dot(k, held_bf) * decays[1]
        grad_k = (dot(mixed_t, q) + dot(v, held_bf, NT) * decays[1]) * scale
        weighted = (q.astype(F32) * decays[0]).astype(BF16)
        back[...] = held * block_decay + dot(weighted, ct, TN)
        g_all[put, parts[1]] = grad_k.astype(BF16)
        g_all[put, parts[2]] = grad_v.astype(BF16)

    alpha, beta = pl.ds(0, FIRST), pl.ds(FIRST, half - FIRST)
    chunk = half // 2

    def r_rows(r):
        return span(turned(z, r) * four, four, four)

    def pick_rows(r, hf):
        return span(turned(z, r) * four + hf * two, two, two)

    def other(r):
        lhs_rows = r_rows(r)

        @pl.loop(0, 2)
        def _(i):
            value = dot(g_all[lhs_rows, :], w_all[span((1 - c) * half + i * chunk, chunk, chunk), :], NT)
            pout[lhs_rows, span(i * chunk, chunk, chunk)] = value.astype(BF16)

        net.start(("p", r), pout.at[lhs_rows], pin.at[lhs_rows], mate)

    def summed(r):
        lhs_rows = r_rows(r)
        net.wait(("p", r), pin.at[lhs_rows])

        @pl.loop(0, 2)
        def _(i):
            value = dot(g_all[lhs_rows, :], w_all[span(c * half + i * chunk, chunk, chunk), :], NT)
            cols = span(i * chunk, chunk, chunk)
            psum[lhs_rows, cols] = (value + pin[lhs_rows, cols].astype(F32)).astype(BF16)

        net.start(("b0", r), psum.at[pick_rows(r, 1 - xl), beta], rb0.at[r % SIDE], pair)

    def add(place, cols, *refs):
        total = psum[place, cols].astype(F32)
        for ref in refs:
            total = total + ref.astype(F32)
        psum[place, cols] = total.astype(BF16)

    def alpha_send(r, hf, way, name, dst):
        net.start(name, psum.at[pick_rows(r, hf), alpha], dst, zs[way])

    def b_rows(r, b):
        return span(turned(z, r) * four + xl * two + b * rows, rows, rows)

    def beta_send(r, b, way, name, dst):
        net.start(name, psum.at[b_rows(r, b), beta], dst, zs[way])

    def a2(e, hf):
        return ra2.at[e, pl.ds(hf * two, two)]

    def b2(e, b):
        return rb2.at[e, pl.ds(b * rows, rows)]

    def w_grad(r, hf):
        cols = span((turned(y, r) * 2 + hf) * depth, depth, depth)
        return dot(h_all[:, cols], g_all[...], TN)

    def y2(e, hf):
        return yr2.at[e, pl.ds(hf * depth, depth)]

    other(2)

    @pl.loop(0, 2)
    def _(hf):
        ysend[hf] = w_grad(2, hf).astype(BF16)

    net.start(("y1", 0), ysend.at[0], yr1.at[0], ys[1])
    net.start(("y1", 1), ysend.at[1], yr1.at[1], ys[-1])
    summed(2)
    alpha_send(2, 0, 1, ("a1", 0), ra1.at[0])
    alpha_send(2, 1, -1, ("a1", 1), ra1.at[1])
    other(1)
    other(-1)
    summed(1)
    alpha_send(1, 1, 1, ("a2", 0, 1), a2(0, 1))
    summed(-1)
    alpha_send(-1, 0, -1, ("a2", 1, 0), a2(1, 0))

    @pl.loop(0, 2)
    def _(e):
        yone[e, 1 - e] = w_grad(1 + 2 * e, 1 - e).astype(BF16)

    net.start(("y2", 0, 1), yone.at[0, 1], y2(0, 1), ys[1])
    net.start(("y2", 1, 0), yone.at[1, 0], y2(1, 0), ys[-1])
    other(0)

    net.wait(("a1", 0), ra1.at[0])
    add(pick_rows(1, 0), alpha, ra1[0])
    alpha_send(1, 0, 1, ("a2", 0, 0), a2(0, 0))
    net.wait(("a1", 1), ra1.at[1])
    add(pick_rows(-1, 1), alpha, ra1[1])
    alpha_send(-1, 1, -1, ("a2", 1, 1), a2(1, 1))

    net.wait(("b0", 2), rb0.at[2])
    add(pick_rows(2, xl), beta, rb0[2])
    beta_send(2, 0, 1, ("b1", 0), rb1.at[0])
    beta_send(2, 1, -1, ("b1", 1), rb1.at[1])
    summed(0)

    @pl.loop(0, 2)
    def _(e):
        ykeep[e] = w_grad(1 + 2 * e, e)

    for e, way in ((0, 1), (1, -1)):
        net.wait(("y1", e), yr1.at[e])
        yone[e, e] = (ykeep[e] + yr1[e].astype(F32)).astype(BF16)
        net.start(("y2", e, e), yone.at[e, e], y2(e, e), ys[way])

    for r, b, way, e in ((1, 1, 1, 0), (-1, 0, -1, 1)):
        net.wait(("b0", r), rb0.at[r % SIDE])
        add(pick_rows(r, xl), beta, rb0[r % SIDE])
        beta_send(r, b, way, ("b2", e, b), b2(e, b))

    @pl.loop(0, 2)
    def _(hf):
        yhome[hf] = w_grad(0, hf)

    for r, b, way, e in ((1, 0, 1, 0), (-1, 1, -1, 1)):
        net.wait(("b1", e), rb1.at[e])
        add(b_rows(r, b), beta, rb1[e])
        beta_send(r, b, way, ("b2", e, b), b2(e, b))
    net.wait(("b0", 0), rb0.at[0])
    add(pick_rows(0, xl), beta, rb0[0])

    for e, hf in ((0, 1), (1, 0), (0, 0), (1, 1)):
        net.wait(("a2", e, hf), a2(e, hf))
    for hf in range(2):
        add(pick_rows(0, hf), alpha, ra2[0, hf * two : (hf + 1) * two], ra2[1, hf * two : (hf + 1) * two])
    net.start(("a3",), psum.at[pick_rows(0, 1 - xl), alpha], ra3, pair)

    def deliver(cols):
        lo = cols.start
        dst = dbuf.at[c, :, cols]
        net.start(("d", lo), psum.at[b_rows(0, 1), cols], dst, at(xx=cross, cc=u), offset=c, width=2)
        net.start(("d", lo), psum.at[b_rows(0, 0), cols], dst, mate, offset=c, width=2, when=away)

    for e, b in ((0, 1), (1, 0), (0, 0), (1, 1)):
        net.wait(("b2", e, b), b2(e, b))
    add(pick_rows(0, xl), beta, rb2[0], rb2[1])
    deliver(beta)

    for e, hf in ((0, 1), (1, 0), (0, 0), (1, 1)):
        net.wait(("y2", e, hf), y2(e, hf))
    for hf in range(2):
        lanes = slice(hf * depth, (hf + 1) * depth)
        total = yhome[hf] + yr2[0, lanes].astype(F32) + yr2[1, lanes].astype(F32)
        yhome[hf] = total
        yout[hf] = total.astype(BF16)
    net.start(("e", 0), yout.at[1 - c], yend.at[0], mate, when=own)
    for hf in range(2):
        net.start(("e", 1), yout.at[hf], yend.at[1], at(xx=cross, cc=hf), when=away)

    net.wait(("a3",), ra3)
    add(pick_rows(0, xl), alpha, ra3[...])
    deliver(alpha)

    net.wait(("e", 1), yend.at[1], when=own)
    net.wait(("e", 0), yend.at[0], when=away)
    net.wait(("e", 1), yend.at[1], when=away)

    @pl.when(own)
    def _():
        for j, out in enumerate((dq, dk, dv)):
            out[...] = (yhome[c, :, parts[j]] + yend[1, :, parts[j]].astype(F32)) * 0.125

    @pl.when(away)
    def _():
        for j, out in enumerate((dq, dk, dv)):
            out[...] = (yend[0, :, parts[j]].astype(F32) + yend[1, :, parts[j]].astype(F32)) * 0.125

    for cols in (beta, alpha):
        for hf in range(2):
            net.wait(
                ("d", cols.start), dbuf.at[hf, :, cols], offset=hf, width=2, when=jnp.logical_or(away, c != hf)
            )

    @pl.when(own)
    def _():
        dbuf[c] = psum[b_rows(0, 0), :]

    for hf in range(2):
        dh[:, hf * half : (hf + 1) * half] = dbuf[hf]
    net.drain()


def whole(rate, h, c, wq, wk, wv):
    rows, width = h.shape
    depth, columns = wq.shape
    blocks = SIDE * SIDE
    length = rows * blocks
    half = width // 2
    rest = half - FIRST
    vmem = pl.BlockSpec(memory_space=pltpu.VMEM)
    dma = pltpu.SemaphoreType.DMA

    def buf(*shape, kind=BF16):
        return pltpu.VMEM(shape, kind)

    return pl.pallas_call(
        whole_kernel,
        out_shape=(buf(rows, width),) + (buf(depth, columns, kind=F32),) * 3,
        in_specs=[pl.BlockSpec(memory_space=pltpu.SMEM)] + [vmem] * 5,
        out_specs=(vmem,) * 4,
        scratch_shapes=[
            buf(length, width),
            buf(length, columns),
            buf(depth * 8, 3 * columns),
            buf(length, 3 * columns),
            buf(length, 3 * columns),
            buf(columns, columns, kind=F32),
            buf(columns, columns, kind=F32),
            buf(2, 8, columns, kind=F32),
            buf(BLOCK, BLOCK, kind=F32),
            buf(BLOCK, BLOCK, kind=F32),
            buf(2, BLOCK, columns, kind=F32),
            buf(length, half),
            buf(length, half),
            buf(length, half),
            buf(2, 2 * rows, FIRST),
            buf(2, 4 * rows, FIRST),
            buf(2 * rows, FIRST),
            buf(SIDE, 2 * rows, rest),
            buf(2, rows, rest),
            buf(2, 2 * rows, rest),
            buf(2, rows, half),
            buf(2, depth, 3 * columns),
            buf(2, 2, depth, 3 * columns),
            buf(2, depth, 3 * columns, kind=F32),
            buf(2, depth, 3 * columns, kind=F32),
            buf(2, depth, 3 * columns),
            buf(2, 2 * depth, 3 * columns),
            buf(2, depth, 3 * columns),
            buf(2, depth, 3 * columns),
            dma((SEMS,)),
            dma((SEMS,)),
        ],
        compiler_params=pltpu.CompilerParams(
            collective_id=0, has_side_effects=True, vmem_limit_bytes=VMEM_LIMIT
        ),
        name="whole",
    )(rate, h, c, wq, wk, wv)


def finish_kernel(count, *refs):
    ins, outs, sems = refs[:count], refs[count : 2 * count], refs[2 * count]
    moves = [pltpu.make_async_copy(ins[i], outs[i], sems.at[i]) for i in range(count)]
    for move in moves:
        move.start()
    for move in moves:
        move.wait()


def finish(*arrays):
    count = len(arrays)
    return pl.pallas_call(
        functools.partial(finish_kernel, count),
        out_shape=tuple(jax.ShapeDtypeStruct(a.shape, a.dtype) for a in arrays),
        in_specs=[pl.BlockSpec(memory_space=pltpu.VMEM)] * count,
        out_specs=(pl.BlockSpec(memory_space=pl.ANY),) * count,
        scratch_shapes=[pltpu.SemaphoreType.DMA((count,))],
        compiler_params=pltpu.CompilerParams(vmem_limit_bytes=4 * 1024 * 1024),
        name="finish",
    )(*arrays)


def body(hidden_in, mix_cotangent, query_weight, key_weight, value_weight, decay_log):
    dh, dq, dk, dv = finish(
        *whole(decay_log, hidden_in[0], mix_cotangent[0], query_weight, key_weight, value_weight)
    )
    return dh[None], dq, dk, dv


def solution(mesh):
    placed = (
        P("dp", "sp", None),
        P("dp", "sp", None),
        P("dp", "sp"),
        P("dp", "sp"),
        P("dp", "sp"),
        P("sp"),
    )
    return jax.shard_map(
        body,
        mesh=mesh,
        in_specs=placed,
        out_specs=(P("dp", "sp", None), P("dp", "sp"), P("dp", "sp"), P("dp", "sp")),
        check_vma=False,
    )
```

```python
import functools

import jax
import jax.numpy as jnp
from jax import lax
from jax.experimental import pallas as pl
from jax.experimental.pallas import tpu as pltpu
from jax.sharding import PartitionSpec as P

BLOCK = 128
SIDE = 4
FIRST = 640
EARLY = 384
F32 = jnp.float32
BF16 = jnp.bfloat16
MESH = pl.DeviceIdType.MESH
NN = (((1,), (0,)), ((), ()))
NT = (((1,), (1,)), ((), ()))
TN = (((0,), (0,)), ((), ()))
VMEM_LIMIT = 60 * 1024 * 1024
SEMS = 256


def dot(a, b, dims=NN):
    return lax.dot_general(a, b, dims, preferred_element_type=F32)


def span(start, size, step):
    return pl.ds(pl.multiple_of(start, step), size)


class Net:
    def __init__(self, send, recv, somewhere):
        self.send, self.recv, self.somewhere = send, recv, somewhere
        self.names, self.starts, self.pending = {}, 0, []

    def index(self, name, width=1):
        if name not in self.names:
            self.names[name] = sum(w for _, w in self.names.values()), width
        return self.names[name][0]

    def start(self, name, src, dst, where, offset=0, width=1, when=None):
        slot = self.index(name, width) + offset
        lane = self.starts
        self.starts += 1

        def make():
            return pltpu.make_async_remote_copy(
                src_ref=src, dst_ref=dst, send_sem=self.send.at[lane], recv_sem=self.recv.at[slot],
                device_id=where, device_id_type=MESH,
            )

        if when is None:
            make().start()
        else:
            pl.when(when)(lambda: make().start())
        self.pending.append((when, make))

    def wait(self, name, dst, offset=0, width=1, when=None):
        slot = self.index(name, width) + offset

        def run():
            pltpu.make_async_remote_copy(
                src_ref=dst, dst_ref=dst, send_sem=self.send.at[0], recv_sem=self.recv.at[slot],
                device_id=self.somewhere, device_id_type=MESH,
            ).wait_recv()

        if when is None:
            run()
        else:
            pl.when(when)(run)

    def drain(self):
        for when, make in self.pending:
            if when is None:
                make().wait_send()
            else:
                pl.when(when)(lambda make=make: make().wait_send())


def whole_kernel(
    rate, h_in, c_in, wq, wk, wv, dh, dq, dk, dv,
    h_all, c_all, w_all, p_all, g_all, g_turn, state, back, rates, inner, inner_t, decays,
    pout, pin, psum, ra1, ra2, ra3, rb0, rb1, rb2, dbuf,
    ysend, yone, yhome, yr1, yr2, yout, yend, send, recv,
):
    s = lax.axis_index("sp")
    d = lax.axis_index("dp")
    z, x = s // SIDE, s % SIDE
    y, c = d // 2, d % 2
    u = x // 2
    xl = x - 2 * u
    own = c == u
    away = c != u
    rows, width = h_in.shape
    depth, columns = wq.shape
    half = width // 2
    four = rows * SIDE
    two = rows * 2
    blocks = SIDE * SIDE
    scale = columns ** (-0.5)

    def at(zz=None, xx=None, yy=None, cc=None):
        zz, xx = z if zz is None else zz, x if xx is None else xx
        yy, cc = y if yy is None else yy, c if cc is None else cc
        return {"sp": zz * SIDE + xx, "dp": yy * 2 + cc}

    def turned(v, by):
        return (v + by + SIDE) % SIDE

    mate = at(cc=1 - c)
    pair = at(xx=x + 1 - 2 * xl)
    zs = {1: at(zz=turned(z, 1)), -1: at(zz=turned(z, -1))}
    ys = {1: at(yy=turned(y, 1)), -1: at(yy=turned(y, -1))}
    cross = 3 - x
    net = Net(send, recv, mate)
    weights = (wq, wk, wv)

    barrier = pltpu.get_barrier_semaphore()
    peers = [mate, ys[1], ys[-1]]
    for k in range(1, blocks):
        other = (s + k) % blocks
        peers += [{"sp": other, "dp": d}, {"sp": other, "dp": y * 2 + 1 - c}]
    for where in peers:
        pl.semaphore_signal(barrier, inc=1, device_id=where, device_id_type=MESH)
    rates[0] = jnp.full(rates.shape[1:], rate[0], F32)
    pl.semaphore_wait(barrier, len(peers))

    def slot(r, col, b):
        return turned(z, r) * SIDE + 2 * (xl if col == 0 else 1 - xl) + b

    def h_ref(place, part, which):
        base = which * half
        lo, size = {"f": (0, half), "a": (0, FIRST), "b": (FIRST, half - FIRST)}[part]
        return h_all.at[span(place * rows, rows, rows), span(base + lo, size, 128)]

    def h_send(r, col, b, part, where, name):
        ref = h_ref(slot(r, col, b), part, c)
        net.start(name, ref, ref, where)

    def to_mate(r, col, b, part):
        h_send(r, col, b, part, mate, ("m", r, col, b, part))

    def h_wait(r, col, b, part, when=None):
        net.wait(("x", r, col, b, part), h_ref(slot(r, col, b), part, c), when=when)

    def w_ref(yy, cc, j):
        return w_all.at[span((yy * 2 + cc) * depth, depth, depth), pl.ds(j * columns, columns)]

    def w_near(j):
        net.start(("w0", j), weights[j], w_ref(y, c, j), mate, offset=c, width=2, when=away)

    def w_cross(j, who):
        net.start(("w0", j), weights[j], w_ref(y, c, j), at(xx=cross, cc=u), offset=c, width=2, when=who)

    mine = span(c * half, half, half)
    theirs = span((1 - c) * half, half, half)
    net.start(("x", 0, 0, 0, "f"), h_in.at[:, theirs], h_ref(slot(0, 0, 0), "f", 1 - c), mate, when=own)
    there = z * SIDE + 2 * (1 - xl) + 1
    for hf in range(2):
        net.start(
            ("x", 0, 0, 1, "f"), h_in.at[:, pl.ds(hf * half, half)], h_ref(there, "f", hf),
            at(xx=cross, cc=hf), when=away,
        )
    for j in range(3):
        w_near(j)
    for j in range(3):
        w_cross(j, away)
    net.start(("rate",), rates.at[0], rates.at[1], at(xx=cross))

    @pl.when(own)
    def _():
        h_all[span(slot(0, 0, 0) * rows, rows, rows), mine] = h_in[:, mine]
        for j in range(3):
            w_all[span(d * depth, depth, depth), j * columns : (j + 1) * columns] = weights[j][...]

    def spread(b):
        for way in (1, -1):
            h_send(0, 0, b, "f", zs[way], ("x", -way, 0, b, "f"))
        h_send(0, 0, b, "f", pair, ("x", 0, 1, b, "f"))
        to_mate(0, 0, b, "f")

    def w_spread(j, who):
        for cc in range(2):
            far = who if who is away else jnp.logical_and(own, c != cc)
            net.wait(("w0", j), w_ref(y, cc, j), offset=cc, width=2, when=far)
            for way in (1, -1):
                net.start(("w1", j, -way, cc), w_ref(y, cc, j), w_ref(y, cc, j), ys[way], when=who)

    def w_forward(j, who):
        for way, cc in ((1, 0), (-1, 1)):
            ref = w_ref(turned(y, -way), cc, j)
            net.wait(("w1", j, -way, cc), ref, when=who)
            net.start(("w2", j, cc), ref, ref, ys[way], when=who)

    def from_pair(b):
        h_wait(0, 1, b, "f")
        for way in (1, -1):
            h_send(0, 1, b, "a", zs[way], ("x", -way, 1, b, "a"))
        to_mate(0, 1, b, "f")

    def from_side(b):
        fast = 1 if b == 0 else -1
        for r in (-fast, fast):
            h_wait(r, 0, b, "f")
            if r == -fast:
                h_send(r, 0, b, "f", zs[fast], ("x", 2, 0, b, "f"))
            h_send(r, 0, b, "b", pair, ("x", r, 1, b, "b"))
            to_mate(r, 0, b, "f")

    def from_corner(b):
        fast = 1 if b == 0 else -1
        for r in (-fast, fast):
            h_wait(r, 1, b, "a")
            if r == -fast:
                h_send(r, 1, b, "a", zs[fast], ("x", 2, 1, b, "a"))
            to_mate(r, 1, b, "a")

    def from_far(b):
        h_wait(2, 0, b, "f")
        h_send(2, 0, b, "b", pair, ("x", 2, 1, b, "b"))
        to_mate(2, 0, b, "f")

    h_wait(0, 0, 0, "f", when=away)
    spread(0)
    for j in range(3):
        w_spread(j, own)
    h_wait(0, 0, 1, "f")
    spread(1)
    for j in range(3):
        w_cross(j, own)
    from_side(0)
    from_pair(0)
    w_forward(0, own)
    w_spread(0, away)
    from_side(1)
    from_pair(1)
    w_forward(1, own)
    w_spread(1, away)
    w_forward(2, own)
    w_spread(2, away)
    from_far(0)
    from_corner(0)
    w_forward(0, away)
    from_far(1)
    from_corner(1)
    w_forward(1, away)

    def c_send(hop, when=None):
        head = (s + hop) % blocks
        hz, hx = head // SIDE, head % SIDE
        far = (hx // 2 - c) * (hx // 2 - c)
        net.start(
            ("c",), c_in.at[:, span(head * columns, columns, columns)],
            c_all.at[span(s * rows, rows, rows)],
            {"sp": hz * SIDE + hx + far * (3 - 2 * hx), "dp": y * 2 + c + far * (1 - 2 * c)},
            offset=s, width=blocks, when=when,
        )

    c_send(0, when=away)
    for hop in range(1, blocks):
        c_send(hop)

    @pl.when(own)
    def _():
        c_all[span(s * rows, rows, rows), :] = c_in[:, span(s * columns, columns, columns)]

    for r in (-1, 1):
        for b in range(2):
            h_wait(r, 1, b, "b")
            to_mate(r, 1, b, "b")
    w_forward(2, away)
    for b in range(2):
        h_wait(2, 1, b, "a")
        to_mate(2, 1, b, "a")
    for b in range(2):
        h_wait(2, 1, b, "b")
        to_mate(2, 1, b, "b")

    for j in range(3):
        for way, cc in ((1, 1), (-1, 0)):
            net.wait(("w1", j, -way, cc), w_ref(turned(y, -way), cc, j))
        for cc in range(2):
            net.wait(("w2", j, cc), w_ref(turned(y, 2), cc, j))

    def mate_wait(r):
        for col in range(2):
            for b in range(2):
                for part in ("f",) if col == 0 or r == 0 else ("a", "b"):
                    net.wait(("m", r, col, b, part), h_ref(slot(r, col, b), part, 1 - c))

    def project(r, j):
        place = span(turned(z, r) * four, four, four)
        cols = span(j * columns, columns, columns)
        value = dot(h_all[place, :], w_all[:, cols]).astype(BF16)
        factor = jnp.where(j == 1, scale, 1.0).astype(F32)
        p_all[place, cols] = (value.astype(F32) * factor).astype(BF16)

    for r in (0, 1, -1):
        mate_wait(r)

    @pl.loop(0, 9)
    def _(t):
        o = t // 3
        project(o + o // 2, t % 3)

    mate_wait(2)

    @pl.loop(0, 3)
    def _(j):
        project(2, j)

    net.wait(("rate",), rates.at[1])
    for k in range(blocks):
        source = (s + k) % blocks
        net.wait(
            ("c",), c_all.at[span(source * rows, rows, rows)], offset=source, width=blocks,
            when=away if k == 0 else None,
        )

    pick = jnp.where(own, 1.0, 0.0).astype(F32)
    g = rates[0] * pick + rates[1] * (1.0 - pick)
    g_row = g[0:1, :]
    gap = (
        lax.broadcasted_iota(jnp.int32, (BLOCK, BLOCK), 0) - lax.broadcasted_iota(jnp.int32, (BLOCK, BLOCK), 1)
    ).astype(F32)
    place = lax.broadcasted_iota(jnp.int32, (BLOCK, columns), 0).astype(F32)
    g_sq = g_row[:, :BLOCK]
    inner[...] = jnp.where(gap >= 0, jnp.exp(g_sq * jnp.maximum(gap, 0.0)), 0.0)
    inner_t[...] = jnp.where(gap <= 0, jnp.exp(g_sq * jnp.maximum(-gap, 0.0)), 0.0)
    decays[0] = jnp.exp(g_row * (place + 1.0))
    decays[1] = jnp.exp(g_row * (BLOCK - 1.0 - place))
    block_decay = jnp.exp(g_row * BLOCK)
    state[...] = jnp.zeros_like(state)
    back[...] = jnp.zeros_like(back)
    parts = [slice(j * columns, (j + 1) * columns) for j in range(3)]

    def slot_of(i):
        iz, ix = i // SIDE, i % SIDE
        b = (ix // 2 - u) * (ix // 2 - u)
        return iz * SIDE + 2 * (ix + b * (3 - 2 * ix) - 2 * u) + b

    @pl.loop(0, blocks)
    def _(i):
        put = span(slot_of(i) * BLOCK, BLOCK, BLOCK)
        k, v = p_all[put, parts[1]], p_all[put, parts[2]]
        ct = c_all[span(i * BLOCK, BLOCK, BLOCK), :]
        mixed = (dot(ct, v, NT) * inner[...]).astype(BF16)
        held = state[...]
        grad_q = dot(mixed, k) + dot(ct, held.astype(BF16), NT) * decays[0]
        weighted = (k.astype(F32) * decays[1]).astype(BF16)
        state[...] = held * block_decay + dot(weighted, v, TN)
        grad_q = grad_q.astype(BF16)
        g_all[put, parts[0]] = grad_q
        g_turn[parts[0], put] = grad_q.T

        i = blocks - 1 - i
        put = span(slot_of(i) * BLOCK, BLOCK, BLOCK)
        q, k, v = (p_all[put, part] for part in parts)
        ct = c_all[span(i * BLOCK, BLOCK, BLOCK), :]
        mixed_t = (dot(v, ct, NT) * inner_t[...]).astype(BF16)
        scores_t = (dot(k, q, NT) * inner_t[...]).astype(BF16)
        held = back[...]
        held_bf = held.astype(BF16)
        grad_v = dot(scores_t, ct) + dot(k, held_bf) * decays[1]
        grad_k = (dot(mixed_t, q) + dot(v, held_bf, NT) * decays[1]) * scale
        weighted = (q.astype(F32) * decays[0]).astype(BF16)
        back[...] = held * block_decay + dot(weighted, ct, TN)
        for part, grad in ((parts[1], grad_k.astype(BF16)), (parts[2], grad_v.astype(BF16))):
            g_all[put, part] = grad
            g_turn[part, put] = grad.T

    pieces = (pl.ds(0, EARLY), pl.ds(EARLY, FIRST - EARLY))
    beta = pl.ds(FIRST, half - FIRST)
    chunk = half // 2

    def r_rows(r):
        return span(turned(z, r) * four, four, four)

    def pick_rows(r, hf):
        return span(turned(z, r) * four + hf * two, two, two)

    def other(r):
        lhs_rows = r_rows(r)

        @pl.loop(0, 2)
        def _(i):
            value = dot(g_all[lhs_rows, :], w_all[span((1 - c) * half + i * chunk, chunk, chunk), :], NT)
            pout[lhs_rows, span(i * chunk, chunk, chunk)] = value.astype(BF16)

        net.start(("p", r), pout.at[lhs_rows], pin.at[lhs_rows], mate)

    def summed(r):
        lhs_rows = r_rows(r)
        net.wait(("p", r), pin.at[lhs_rows])

        @pl.loop(0, 2)
        def _(i):
            value = dot(g_all[lhs_rows, :], w_all[span(c * half + i * chunk, chunk, chunk), :], NT)
            cols = span(i * chunk, chunk, chunk)
            psum[lhs_rows, cols] = (value + pin[lhs_rows, cols].astype(F32)).astype(BF16)

        net.start(("b0", r), psum.at[pick_rows(r, 1 - xl), beta], rb0.at[r % SIDE], pair)

    def add(place, cols, *refs):
        total = psum[place, cols].astype(F32)
        for ref in refs:
            total = total + ref.astype(F32)
        psum[place, cols] = total.astype(BF16)

    def a1(i, e):
        return ra1.at[e, :, pieces[i]]

    def a2(i, e, hf):
        return ra2.at[e, pl.ds(hf * two, two), pieces[i]]

    def a3(i):
        return ra3.at[:, pieces[i]]

    def alpha_send(i, r, hf, way, name, dst):
        net.start(name, psum.at[pick_rows(r, hf), pieces[i]], dst, zs[way])

    def alpha_first(i):
        alpha_send(i, 2, 0, 1, ("a1", i, 0), a1(i, 0))
        alpha_send(i, 2, 1, -1, ("a1", i, 1), a1(i, 1))

    def alpha_plain(i, r):
        e = 0 if r == 1 else 1
        alpha_send(i, r, 1 - e, r, ("a2", i, e, 1 - e), a2(i, e, 1 - e))

    def alpha_added(i):
        for e, r in ((0, 1), (1, -1)):
            net.wait(("a1", i, e), a1(i, e))
            add(pick_rows(r, e), pieces[i], a1(i, e)[...])
            alpha_send(i, r, e, r, ("a2", i, e, e), a2(i, e, e))

    def alpha_last(i):
        for e, hf in ((0, 1), (1, 0), (0, 0), (1, 1)):
            net.wait(("a2", i, e, hf), a2(i, e, hf))
        for hf in range(2):
            add(pick_rows(0, hf), pieces[i], a2(i, 0, hf)[...], a2(i, 1, hf)[...])
        net.start(("a3", i), psum.at[pick_rows(0, 1 - xl), pieces[i]], a3(i), pair)

    def deliver(cols):
        lo = cols.start
        dst = dbuf.at[c, :, cols]
        net.start(("d", lo), psum.at[b_rows(0, 1), cols], dst, at(xx=cross, cc=u), offset=c, width=2)
        net.start(("d", lo), psum.at[b_rows(0, 0), cols], dst, mate, offset=c, width=2, when=away)

    def alpha_deliver(i):
        net.wait(("a3", i), a3(i))
        add(pick_rows(0, xl), pieces[i], a3(i)[...])
        deliver(pieces[i])

    def b_rows(r, b):
        return span(turned(z, r) * four + xl * two + b * rows, rows, rows)

    def b2(e, b):
        return rb2.at[e, pl.ds(b * rows, rows)]

    def beta_send(r, b, way, name, dst):
        net.start(name, psum.at[b_rows(r, b), beta], dst, zs[way])

    def beta_take(r):
        net.wait(("b0", r), rb0.at[r % SIDE])
        add(pick_rows(r, xl), beta, rb0[r % SIDE])

    def beta_first():
        beta_take(2)
        beta_send(2, 0, 1, ("b1", 0), rb1.at[0])
        beta_send(2, 1, -1, ("b1", 1), rb1.at[1])

    def beta_plain():
        for r, b, e in ((1, 1, 0), (-1, 0, 1)):
            beta_take(r)
            beta_send(r, b, r, ("b2", e, b), b2(e, b))

    def beta_added():
        for r, b, e in ((1, 0, 0), (-1, 1, 1)):
            net.wait(("b1", e), rb1.at[e])
            add(b_rows(r, b), beta, rb1[e])
            beta_send(r, b, r, ("b2", e, b), b2(e, b))

    def beta_last():
        beta_take(0)
        for e, b in ((0, 1), (1, 0), (0, 0), (1, 1)):
            net.wait(("b2", e, b), b2(e, b))
        add(pick_rows(0, xl), beta, rb2[0], rb2[1])
        deliver(beta)

    lanes = [pl.ds(hf * depth, depth) for hf in range(2)]

    def w_grad(r, j):
        cols = span(turned(y, r) * 2 * depth, 2 * depth, depth)
        return dot(g_turn[parts[j], :], h_all[:, cols])

    def y_first(j):
        ysend[j] = w_grad(2, j).astype(BF16)
        for e, way in ((0, 1), (1, -1)):
            net.start(("y1", j, e), ysend.at[j, :, lanes[e]], yr1.at[j, e], ys[way])

    def y2(j, e, hf):
        return yr2.at[j, e, :, lanes[hf]]

    def y_second(j):
        for e, r in ((0, 1), (1, -1)):
            value = w_grad(r, j)
            keep = value[:, e * depth : (e + 1) * depth]
            yone[j, e, :, lanes[1 - e]] = value[:, (1 - e) * depth : (2 - e) * depth].astype(BF16)
            net.start(("y2", j, e, 1 - e), yone.at[j, e, :, lanes[1 - e]], y2(j, e, 1 - e), ys[r])
            net.wait(("y1", j, e), yr1.at[j, e])
            yone[j, e, :, lanes[e]] = (keep + yr1[j, e].astype(F32)).astype(BF16)
            net.start(("y2", j, e, e), yone.at[j, e, :, lanes[e]], y2(j, e, e), ys[r])

    def y_home(j):
        yhome[j] = w_grad(0, j)

    def y_last(j):
        for e, hf in ((0, 1), (1, 0), (0, 0), (1, 1)):
            net.wait(("y2", j, e, hf), y2(j, e, hf))
        total = yhome[j] + yr2[j, 0].astype(F32) + yr2[j, 1].astype(F32)
        yhome[j] = total
        yout[j] = total.astype(BF16)
        half_of = span((1 - c) * depth, depth, depth)
        net.start(("e", j, 0), yout.at[j, :, half_of], yend.at[j, 0], mate, when=own)
        for hf in range(2):
            net.start(("e", j, 1), yout.at[j, :, lanes[hf]], yend.at[j, 1], at(xx=cross, cc=hf), when=away)

    other(2)
    y_first(0)
    y_first(1)
    summed(2)
    alpha_first(0)
    alpha_first(1)
    other(1)
    y_first(2)
    other(-1)
    summed(1)
    alpha_plain(0, 1)
    summed(-1)
    alpha_plain(0, -1)
    y_second(0)
    alpha_added(0)
    alpha_plain(1, 1)
    alpha_plain(1, -1)
    other(0)
    y_second(1)
    alpha_added(1)
    beta_first()
    summed(0)
    y_second(2)
    beta_plain()
    for j in range(3):
        y_home(j)
    y_last(0)
    alpha_last(0)
    y_last(1)
    alpha_last(1)
    alpha_deliver(0)
    beta_added()
    y_last(2)
    alpha_deliver(1)
    beta_last()

    for j in range(3):
        net.wait(("e", j, 1), yend.at[j, 1])
        net.wait(("e", j, 0), yend.at[j, 0], when=away)

    @pl.when(own)
    def _():
        here = span(c * depth, depth, depth)
        for j, out in enumerate((dq, dk, dv)):
            out[...] = (yhome[j, :, here] + yend[j, 1].astype(F32)).T * 0.125

    @pl.when(away)
    def _():
        for j, out in enumerate((dq, dk, dv)):
            out[...] = (yend[j, 0].astype(F32) + yend[j, 1].astype(F32)).T * 0.125

    for cols in pieces + (beta,):
        for hf in range(2):
            net.wait(
                ("d", cols.start), dbuf.at[hf, :, cols], offset=hf, width=2, when=jnp.logical_or(away, c != hf)
            )

    @pl.when(own)
    def _():
        dbuf[c] = psum[b_rows(0, 0), :]

    for hf in range(2):
        dh[:, hf * half : (hf + 1) * half] = dbuf[hf]
    net.drain()


def whole(rate, h, c, wq, wk, wv):
    rows, width = h.shape
    depth, columns = wq.shape
    blocks = SIDE * SIDE
    length = rows * blocks
    half = width // 2
    rest = half - FIRST
    vmem = pl.BlockSpec(memory_space=pltpu.VMEM)
    dma = pltpu.SemaphoreType.DMA

    def buf(*shape, kind=BF16):
        return pltpu.VMEM(shape, kind)

    return pl.pallas_call(
        whole_kernel,
        out_shape=(buf(rows, width),) + (buf(depth, columns, kind=F32),) * 3,
        in_specs=[pl.BlockSpec(memory_space=pltpu.SMEM)] + [vmem] * 5,
        out_specs=(vmem,) * 4,
        scratch_shapes=[
            buf(length, width),
            buf(length, columns),
            buf(depth * 8, 3 * columns),
            buf(length, 3 * columns),
            buf(length, 3 * columns),
            buf(3 * columns, length),
            buf(columns, columns, kind=F32),
            buf(columns, columns, kind=F32),
            buf(2, 8, columns, kind=F32),
            buf(BLOCK, BLOCK, kind=F32),
            buf(BLOCK, BLOCK, kind=F32),
            buf(2, BLOCK, columns, kind=F32),
            buf(length, half),
            buf(length, half),
            buf(length, half),
            buf(2, 2 * rows, FIRST),
            buf(2, 4 * rows, FIRST),
            buf(2 * rows, FIRST),
            buf(SIDE, 2 * rows, rest),
            buf(2, rows, rest),
            buf(2, 2 * rows, rest),
            buf(2, rows, half),
            buf(3, columns, 2 * depth),
            buf(3, 2, columns, 2 * depth),
            buf(3, columns, 2 * depth, kind=F32),
            buf(3, 2, columns, depth),
            buf(3, 2, columns, 2 * depth),
            buf(3, columns, 2 * depth),
            buf(3, 2, columns, depth),
            dma((SEMS,)),
            dma((SEMS,)),
        ],
        compiler_params=pltpu.CompilerParams(
            collective_id=0, has_side_effects=True, vmem_limit_bytes=VMEM_LIMIT
        ),
        name="whole",
    )(rate, h, c, wq, wk, wv)


def finish_kernel(count, *refs):
    ins, outs, sems = refs[:count], refs[count : 2 * count], refs[2 * count]
    moves = [pltpu.make_async_copy(ins[i], outs[i], sems.at[i]) for i in range(count)]
    for move in moves:
        move.start()
    for move in moves:
        move.wait()


def finish(*arrays):
    count = len(arrays)
    return pl.pallas_call(
        functools.partial(finish_kernel, count),
        out_shape=tuple(jax.ShapeDtypeStruct(a.shape, a.dtype) for a in arrays),
        in_specs=[pl.BlockSpec(memory_space=pltpu.VMEM)] * count,
        out_specs=(pl.BlockSpec(memory_space=pl.ANY),) * count,
        scratch_shapes=[pltpu.SemaphoreType.DMA((count,))],
        compiler_params=pltpu.CompilerParams(vmem_limit_bytes=4 * 1024 * 1024),
        name="finish",
    )(*arrays)


def body(hidden_in, mix_cotangent, query_weight, key_weight, value_weight, decay_log):
    dh, dq, dk, dv = finish(
        *whole(decay_log, hidden_in[0], mix_cotangent[0], query_weight, key_weight, value_weight)
    )
    return dh[None], dq, dk, dv


def solution(mesh):
    placed = (
        P("dp", "sp", None),
        P("dp", "sp", None),
        P("dp", "sp"),
        P("dp", "sp"),
        P("dp", "sp"),
        P("sp"),
    )
    return jax.shard_map(
        body,
        mesh=mesh,
        in_specs=placed,
        out_specs=(P("dp", "sp", None), P("dp", "sp"), P("dp", "sp"), P("dp", "sp")),
        check_vma=False,
    )
```

```python
import functools

import jax
import jax.numpy as jnp
from jax import lax
from jax.experimental import pallas as pl
from jax.experimental.pallas import tpu as pltpu
from jax.sharding import PartitionSpec as P

BLOCK = 256
SIDE = 4
FIRST = 640
EARLY = 384
F32 = jnp.float32
BF16 = jnp.bfloat16
MESH = pl.DeviceIdType.MESH
NN = (((1,), (0,)), ((), ()))
NT = (((1,), (1,)), ((), ()))
TN = (((0,), (0,)), ((), ()))
VMEM_LIMIT = 60 * 1024 * 1024
GROUP = 4 * 1024 * 1024
CELL = 32 * 1024
SENDS = 9
RECVS = 125


def dot(a, b, dims=NN):
    return lax.dot_general(a, b, dims, preferred_element_type=F32)


def span(start, size, step):
    return pl.ds(pl.multiple_of(start, step), size)


class Net:
    def __init__(self, send, recv, meter, small, somewhere):
        self.send, self.recv, self.somewhere = send, recv, somewhere
        self.meter, self.small = meter, small
        self.names, self.total, self.groups, self.open = {}, 0, [], {}

    def index(self, name, width=1):
        if name not in self.names:
            self.names[name] = self.total
            self.total += width
        return self.names[name]

    def lane(self, kind, when, size):
        group = self.open.get(kind)
        if group is None or self.groups[group][1] + size > GROUP:
            self.open[kind] = group = len(self.groups)
            self.groups.append([when, 0])
        self.groups[group][1] += size
        return group

    def copy(self, src, dst, lane, slot, where):
        return pltpu.make_async_remote_copy(
            src_ref=src, dst_ref=dst, send_sem=self.send.at[lane], recv_sem=self.recv.at[slot],
            device_id=where, device_id_type=MESH,
        )

    def start(self, name, src, dst, where, offset=0, width=1, when=None):
        slot = self.index(name, width) + offset
        size = 2 if src.dtype == BF16 else 4
        for extent in src.shape:
            size *= extent
        lane = self.lane(id(when) if size % CELL == 0 else name, when, size)
        if when is None:
            self.copy(src, dst, lane, slot, where).start()
        else:
            pl.when(when)(lambda: self.copy(src, dst, lane, slot, where).start())

    def wait(self, name, dst, offset=0, width=1, when=None):
        slot = self.index(name, width) + offset
        if when is None:
            self.copy(dst, dst, 0, slot, self.somewhere).wait_recv()
        else:
            pl.when(when)(lambda: self.copy(dst, dst, 0, slot, self.somewhere).wait_recv())

    def drain(self):
        for lane, (when, size) in enumerate(self.groups):
            ref = self.meter.at[pl.ds(0, size // (2 * self.meter.shape[1]))] if size % CELL == 0 else self.small

            def run():
                self.copy(ref, ref, lane, 0, self.somewhere).wait_send()

            if when is None:
                run()
            else:
                pl.when(when)(run)


def whole_kernel(
    rate, h_far, c_far, wq, wk, wv, dh, dq, dk, dv,
    h_all, c_all, w_all, p_all, g_all, g_turn, state, back, rates, inner, inner_t, decays,
    pout, pin, psum, ra1, ra2, ra3, rb0, rb1, rb2, dbuf,
    ysend, yone, yhome, yr1, yr2, yout, yend, h_in, c_in, w_in, local, send, recv,
):
    s = lax.axis_index("sp")
    d = lax.axis_index("dp")
    z, x = s // SIDE, s % SIDE
    y, c = d // 2, d % 2
    u = x // 2
    xl = x - 2 * u
    own = c == u
    away = c != u
    rows, width = h_in.shape
    depth, columns = wq.shape
    half = width // 2
    four = rows * SIDE
    two = rows * 2
    blocks = SIDE * SIDE
    scale = columns ** (-0.5)

    def at(zz=None, xx=None, yy=None, cc=None):
        zz, xx = z if zz is None else zz, x if xx is None else xx
        yy, cc = y if yy is None else yy, c if cc is None else cc
        return {"sp": zz * SIDE + xx, "dp": yy * 2 + cc}

    def turned(v, by):
        return (v + by + SIDE) % SIDE

    mate = at(cc=1 - c)
    pair = at(xx=x + 1 - 2 * xl)
    zs = {1: at(zz=turned(z, 1)), -1: at(zz=turned(z, -1))}
    ys = {1: at(yy=turned(y, 1)), -1: at(yy=turned(y, -1))}
    cross = 3 - x
    net = Net(send, recv, h_all, rates.at[0], mate)
    weights = [w_in.at[j] for j in range(3)]
    loads = [
        pltpu.make_async_copy(src, dst, local.at[i])
        for i, (src, dst) in enumerate(zip((h_far, wq, wk, wv, c_far), [h_in] + weights + [c_in]))
    ]
    for load in loads:
        load.start()

    barrier = pltpu.get_barrier_semaphore()
    peers = [mate, ys[1], ys[-1]]
    for k in range(1, blocks):
        other = (s + k) % blocks
        peers += [{"sp": other, "dp": d}, {"sp": other, "dp": y * 2 + 1 - c}]
    for where in peers:
        pl.semaphore_signal(barrier, inc=1, device_id=where, device_id_type=MESH)
    rates[0] = jnp.full(rates.shape[1:], rate[0], F32)
    loads[0].wait()
    pl.semaphore_wait(barrier, len(peers))

    def r_rows(r):
        return span(turned(z, r) * four, four, four)

    def slot(r, col, b):
        return turned(z, r) * SIDE + 2 * (xl if col == 0 else 1 - xl) + b

    def h_ref(place, part, which):
        base = which * half
        lo, size = {"f": (0, half), "a": (0, FIRST), "b": (FIRST, half - FIRST)}[part]
        return h_all.at[span(place * rows, rows, rows), span(base + lo, size, 128)]

    def h_send(r, col, b, part, where, name):
        ref = h_ref(slot(r, col, b), part, c)
        net.start(name, ref, ref, where)

    def to_mate(r, col, b, part):
        h_send(r, col, b, part, mate, ("m", r))

    def h_wait(r, col, b, part, when=None):
        net.wait(("x", r, col, b, part), h_ref(slot(r, col, b), part, c), when=when)

    def w_ref(yy, cc, j):
        return w_all.at[span((yy * 2 + cc) * depth, depth, depth), pl.ds(j * columns, columns)]

    def w_near(j):
        net.start(("w0", j), weights[j], w_ref(y, c, j), mate, offset=c, width=2, when=away)

    def w_cross(j, who):
        net.start(("w0", j), weights[j], w_ref(y, c, j), at(xx=cross, cc=u), offset=c, width=2, when=who)

    mine = span(c * half, half, half)
    theirs = span((1 - c) * half, half, half)
    net.start(("x", 0, 0, 0, "f"), h_in.at[:, theirs], h_ref(slot(0, 0, 0), "f", 1 - c), mate, when=own)
    there = z * SIDE + 2 * (1 - xl) + 1
    for hf in range(2):
        net.start(
            ("x", 0, 0, 1, "f"), h_in.at[:, pl.ds(hf * half, half)], h_ref(there, "f", hf),
            at(xx=cross, cc=hf), when=away,
        )
    for load in loads[1:4]:
        load.wait()
    for j in range(3):
        w_near(j)
    for j in range(3):
        w_cross(j, away)
    net.start(("rate",), rates.at[0], rates.at[1], at(xx=cross))

    @pl.when(own)
    def _():
        h_all[span(slot(0, 0, 0) * rows, rows, rows), mine] = h_in[:, mine]
        for j in range(3):
            w_all[span(d * depth, depth, depth), j * columns : (j + 1) * columns] = weights[j][...]

    def spread(b):
        for way in (1, -1):
            h_send(0, 0, b, "f", zs[way], ("x", -way, 0, b, "f"))
        h_send(0, 0, b, "f", pair, ("x", 0, 1, b, "f"))
        to_mate(0, 0, b, "f")

    def w_spread(j, who):
        for cc in range(2):
            far = who if who is away else jnp.logical_and(own, c != cc)
            net.wait(("w0", j), w_ref(y, cc, j), offset=cc, width=2, when=far)
            for way in (1, -1):
                net.start(("w1", j, -way, cc), w_ref(y, cc, j), w_ref(y, cc, j), ys[way], when=who)

    def w_forward(j, who):
        for way, cc in ((1, 0), (-1, 1)):
            ref = w_ref(turned(y, -way), cc, j)
            net.wait(("w1", j, -way, cc), ref, when=who)
            net.start(("w2", j, cc), ref, ref, ys[way], when=who)

    def from_pair(b):
        h_wait(0, 1, b, "f")
        for way in (1, -1):
            h_send(0, 1, b, "a", zs[way], ("x", -way, 1, b, "a"))
        to_mate(0, 1, b, "f")

    def from_side(b):
        fast = 1 if b == 0 else -1
        for r in (-fast, fast):
            h_wait(r, 0, b, "f")
            if r == -fast:
                h_send(r, 0, b, "f", zs[fast], ("x", 2, 0, b, "f"))
            h_send(r, 0, b, "b", pair, ("x", r, 1, b, "b"))
            to_mate(r, 0, b, "f")

    def from_corner(b):
        fast = 1 if b == 0 else -1
        for r in (-fast, fast):
            h_wait(r, 1, b, "a")
            if r == -fast:
                h_send(r, 1, b, "a", zs[fast], ("x", 2, 1, b, "a"))
            to_mate(r, 1, b, "a")

    def from_far(b):
        h_wait(2, 0, b, "f")
        h_send(2, 0, b, "b", pair, ("x", 2, 1, b, "b"))
        to_mate(2, 0, b, "f")

    def c_send(dz, dx):
        hz, hx = turned(z, dz), turned(x, dx)
        head = hz * SIDE + hx
        far = (hx // 2 - c) * (hx // 2 - c)
        net.start(
            ("c",), c_in.at[:, span(head * columns, columns, columns)],
            c_all.at[span(s * rows, rows, rows)],
            {"sp": hz * SIDE + hx + far * (3 - 2 * hx), "dp": y * 2 + c + far * (1 - 2 * c)},
            offset=s, width=blocks, when=away if (dz, dx) == (0, 0) else None,
        )

    diagonal = [(dz, (dz + k) % SIDE) for k in range(SIDE) for dz in (2, 1, 3, 0)]

    h_wait(0, 0, 0, "f", when=away)
    spread(0)
    for j in range(3):
        w_spread(j, own)
    h_wait(0, 0, 1, "f")
    spread(1)
    for j in range(3):
        w_cross(j, own)
    from_side(0)
    from_pair(0)
    w_forward(0, own)
    w_spread(0, away)
    from_side(1)
    from_pair(1)
    w_forward(1, own)
    w_spread(1, away)
    w_forward(2, own)
    w_spread(2, away)
    loads[4].wait()
    for dz, dx in diagonal[:8]:
        c_send(dz, dx)

    @pl.when(own)
    def _():
        c_all[span(s * rows, rows, rows), :] = c_in[:, span(s * columns, columns, columns)]

    from_far(0)
    from_corner(0)
    w_forward(0, away)
    from_far(1)
    from_corner(1)
    w_forward(1, away)

    for dz, dx in diagonal[8:]:
        c_send(dz, dx)

    for r in (-1, 1):
        for b in range(2):
            h_wait(r, 1, b, "b")
            to_mate(r, 1, b, "b")
    w_forward(2, away)

    def mate_wait(r):
        net.wait(("m", r), h_all.at[r_rows(r), theirs])

    def project(first, step, count):
        @pl.loop(0, 3 * count)
        def _(t):
            place = span(turned(z, first + step * (t // 3)) * four, four, four)
            j = t % 3
            cols = span(j * columns, columns, columns)
            value = dot(h_all[place, :], w_all[:, cols]).astype(BF16)
            factor = jnp.where(j == 1, scale, 1.0).astype(F32)
            p_all[place, cols] = (value.astype(F32) * factor).astype(BF16)

    for j in range(3):
        for way, cc in ((1, 1), (-1, 0)):
            net.wait(("w1", j, -way, cc), w_ref(turned(y, -way), cc, j))
        for cc in range(2):
            net.wait(("w2", j, cc), w_ref(turned(y, 2), cc, j))
    mate_wait(0)
    project(0, 0, 1)
    for part in ("a", "b"):
        for b in range(2):
            h_wait(2, 1, b, part)
            to_mate(2, 1, b, part)
    mate_wait(1)
    mate_wait(-1)
    project(1, 2, 2)
    mate_wait(2)
    project(2, 0, 1)

    net.wait(("rate",), rates.at[1])
    for k in range(blocks):
        source = (s + k) % blocks
        net.wait(
            ("c",), c_all.at[span(source * rows, rows, rows)], offset=source, width=blocks,
            when=away if k == 0 else None,
        )

    pick = jnp.where(own, 1.0, 0.0).astype(F32)
    g = rates[0] * pick + rates[1] * (1.0 - pick)
    g_row = g[0:1, :]
    gap = (
        lax.broadcasted_iota(jnp.int32, (BLOCK, BLOCK), 0) - lax.broadcasted_iota(jnp.int32, (BLOCK, BLOCK), 1)
    ).astype(F32)
    place = lax.broadcasted_iota(jnp.int32, (BLOCK, columns), 0).astype(F32)
    inner[...] = jnp.where(gap >= 0, jnp.exp(g_row * jnp.maximum(gap, 0.0)), 0.0)
    inner_t[...] = jnp.where(gap <= 0, jnp.exp(g_row * jnp.maximum(-gap, 0.0)), 0.0)
    decays[0] = jnp.exp(g_row * (place + 1.0))
    decays[1] = jnp.exp(g_row * (BLOCK - 1.0 - place))
    block_decay = jnp.exp(g_row * BLOCK)
    state[...] = jnp.zeros_like(state)
    back[...] = jnp.zeros_like(back)
    parts = [slice(j * columns, (j + 1) * columns) for j in range(3)]
    count = BLOCK // rows

    def slots(i):
        places = []
        for w in range(count):
            p = i * count + w
            pz, px = p // SIDE, p % SIDE
            b = (px // 2 - u) * (px // 2 - u)
            places.append(span((pz * SIDE + 2 * (px + b * (3 - 2 * px) - 2 * u) + b) * rows, rows, rows))
        return places

    def get(places, part):
        return jnp.concatenate([p_all[place, part] for place in places], axis=0)

    def put(places, part, grad):
        grad = grad.astype(BF16)
        for w, place in enumerate(places):
            g_all[place, part] = grad[w * rows : (w + 1) * rows]
        grad = grad.T
        for w, place in enumerate(places):
            g_turn[part, place] = grad[:, w * rows : (w + 1) * rows]

    def forward(i):
        places = slots(i)
        k, v = get(places, parts[1]), get(places, parts[2])
        ct = c_all[span(i * BLOCK, BLOCK, BLOCK), :]
        mixed = (dot(ct, v, NT) * inner[...]).astype(BF16)
        held = state[...]
        grad_q = dot(mixed, k) + dot(ct, held.astype(BF16), NT) * decays[0]
        weighted = (k.astype(F32) * decays[1]).astype(BF16)
        state[...] = held * block_decay + dot(weighted, v, TN)
        put(places, parts[0], grad_q)

    def backward(i):
        places = slots(i)
        q, k, v = (get(places, part) for part in parts)
        ct = c_all[span(i * BLOCK, BLOCK, BLOCK), :]
        mixed_t = (dot(v, ct, NT) * inner_t[...]).astype(BF16)
        scores_t = (dot(k, q, NT) * inner_t[...]).astype(BF16)
        held = back[...]
        held_bf = held.astype(BF16)
        grad_v = dot(scores_t, ct) + dot(k, held_bf) * decays[1]
        grad_k = (dot(mixed_t, q) + dot(v, held_bf, NT) * decays[1]) * scale
        weighted = (q.astype(F32) * decays[0]).astype(BF16)
        back[...] = held * block_decay + dot(weighted, ct, TN)
        put(places, parts[1], grad_k)
        put(places, parts[2], grad_v)

    steps = rows * blocks // BLOCK

    @pl.loop(0, steps // 2)
    def _(t):
        for w in range(2):
            forward(2 * t + w)
            backward(steps - 1 - 2 * t - w)

    pieces = (pl.ds(0, EARLY), pl.ds(EARLY, FIRST - EARLY))
    beta = pl.ds(FIRST, half - FIRST)
    chunk = half // 2

    def pick_rows(r, hf):
        return span(turned(z, r) * four + hf * two, two, two)

    def other(r):
        lhs_rows = r_rows(r)

        @pl.loop(0, 2)
        def _(i):
            value = dot(g_all[lhs_rows, :], w_all[span((1 - c) * half + i * chunk, chunk, chunk), :], NT)
            pout[lhs_rows, span(i * chunk, chunk, chunk)] = value.astype(BF16)

        net.start(("p", r), pout.at[lhs_rows], pin.at[lhs_rows], mate)

    def summed(r):
        lhs_rows = r_rows(r)
        net.wait(("p", r), pin.at[lhs_rows])

        @pl.loop(0, 2)
        def _(i):
            value = dot(g_all[lhs_rows, :], w_all[span(c * half + i * chunk, chunk, chunk), :], NT)
            cols = span(i * chunk, chunk, chunk)
            psum[lhs_rows, cols] = (value + pin[lhs_rows, cols].astype(F32)).astype(BF16)

        net.start(("b0", r), psum.at[pick_rows(r, 1 - xl), beta], rb0.at[r % SIDE], pair)

    def add(place, cols, *refs):
        total = psum[place, cols].astype(F32)
        for ref in refs:
            total = total + ref.astype(F32)
        psum[place, cols] = total.astype(BF16)

    def a1(i, e):
        return ra1.at[e, :, pieces[i]]

    def a2(i, e, hf):
        return ra2.at[e, pl.ds(hf * two, two), pieces[i]]

    def a3(i):
        return ra3.at[:, pieces[i]]

    def alpha_send(i, r, hf, way, name, dst):
        net.start(name, psum.at[pick_rows(r, hf), pieces[i]], dst, zs[way])

    def alpha_first(i):
        alpha_send(i, 2, 0, 1, ("a1", i, 0), a1(i, 0))
        alpha_send(i, 2, 1, -1, ("a1", i, 1), a1(i, 1))

    def alpha_plain(i, r):
        e = 0 if r == 1 else 1
        alpha_send(i, r, 1 - e, r, ("a2", i, e, 1 - e), a2(i, e, 1 - e))

    def alpha_added(i):
        for e, r in ((0, 1), (1, -1)):
            net.wait(("a1", i, e), a1(i, e))
            add(pick_rows(r, e), pieces[i], a1(i, e)[...])
            alpha_send(i, r, e, r, ("a2", i, e, e), a2(i, e, e))

    def alpha_last(i):
        for e, hf in ((0, 1), (1, 0), (0, 0), (1, 1)):
            net.wait(("a2", i, e, hf), a2(i, e, hf))
        for hf in range(2):
            add(pick_rows(0, hf), pieces[i], a2(i, 0, hf)[...], a2(i, 1, hf)[...])
        net.start(("a3", i), psum.at[pick_rows(0, 1 - xl), pieces[i]], a3(i), pair)

    def deliver(cols):
        lo = cols.start
        dst = dbuf.at[c, :, cols]
        net.start(("d", lo), psum.at[b_rows(0, 1), cols], dst, at(xx=cross, cc=u), offset=c, width=2)
        net.start(("d", lo), psum.at[b_rows(0, 0), cols], dst, mate, offset=c, width=2, when=away)

    def alpha_deliver(i):
        net.wait(("a3", i), a3(i))
        add(pick_rows(0, xl), pieces[i], a3(i)[...])
        deliver(pieces[i])

    def b_rows(r, b):
        return span(turned(z, r) * four + xl * two + b * rows, rows, rows)

    def b2(e, b):
        return rb2.at[e, pl.ds(b * rows, rows)]

    def beta_send(r, b, way, name, dst):
        net.start(name, psum.at[b_rows(r, b), beta], dst, zs[way])

    def beta_take(r):
        net.wait(("b0", r), rb0.at[r % SIDE])
        add(pick_rows(r, xl), beta, rb0[r % SIDE])

    def beta_first():
        beta_take(2)
        beta_send(2, 0, 1, ("b1", 0), rb1.at[0])
        beta_send(2, 1, -1, ("b1", 1), rb1.at[1])

    def beta_plain():
        for r, b, e in ((1, 1, 0), (-1, 0, 1)):
            beta_take(r)
            beta_send(r, b, r, ("b2", e, b), b2(e, b))

    def beta_added():
        for r, b, e in ((1, 0, 0), (-1, 1, 1)):
            net.wait(("b1", e), rb1.at[e])
            add(b_rows(r, b), beta, rb1[e])
            beta_send(r, b, r, ("b2", e, b), b2(e, b))

    def beta_last():
        beta_take(0)
        for e, b in ((0, 1), (1, 0), (0, 0), (1, 1)):
            net.wait(("b2", e, b), b2(e, b))
        add(pick_rows(0, xl), beta, rb2[0], rb2[1])
        deliver(beta)

    lanes = [pl.ds(hf * depth, depth) for hf in range(2)]

    def w_grad(r, j):
        cols = span(turned(y, r) * 2 * depth, 2 * depth, depth)
        return dot(g_turn[parts[j], :], h_all[:, cols])

    def y_first(j):
        ysend[j] = w_grad(2, j).astype(BF16)
        for e, way in ((0, 1), (1, -1)):
            net.start(("y1", j, e), ysend.at[j, :, lanes[e]], yr1.at[j, e], ys[way])

    def y2(j, e, hf):
        return yr2.at[j, e, :, lanes[hf]]

    def y_second(j):
        for e, r in ((0, 1), (1, -1)):
            value = w_grad(r, j)
            keep = value[:, e * depth : (e + 1) * depth]
            yone[j, e, :, lanes[1 - e]] = value[:, (1 - e) * depth : (2 - e) * depth].astype(BF16)
            net.start(("y2", j, e, 1 - e), yone.at[j, e, :, lanes[1 - e]], y2(j, e, 1 - e), ys[r])
            net.wait(("y1", j, e), yr1.at[j, e])
            yone[j, e, :, lanes[e]] = (keep + yr1[j, e].astype(F32)).astype(BF16)
            net.start(("y2", j, e, e), yone.at[j, e, :, lanes[e]], y2(j, e, e), ys[r])

    def y_home(j):
        yhome[j] = w_grad(0, j)

    def y_last(j):
        for e, hf in ((0, 1), (1, 0), (0, 0), (1, 1)):
            net.wait(("y2", j, e, hf), y2(j, e, hf))
        total = yhome[j] + yr2[j, 0].astype(F32) + yr2[j, 1].astype(F32)
        yhome[j] = total
        yout[j] = total.astype(BF16)
        half_of = span((1 - c) * depth, depth, depth)
        net.start(("e", j, 0), yout.at[j, :, half_of], yend.at[j, 0], mate, when=own)
        for hf in range(2):
            net.start(("e", j, 1), yout.at[j, :, lanes[hf]], yend.at[j, 1], at(xx=cross, cc=hf), when=away)

    other(2)
    y_first(0)
    y_first(1)
    summed(2)
    alpha_first(0)
    alpha_first(1)
    other(1)
    y_first(2)
    other(-1)
    summed(1)
    alpha_plain(0, 1)
    summed(-1)
    alpha_plain(0, -1)
    y_second(0)
    alpha_added(0)
    alpha_plain(1, 1)
    alpha_plain(1, -1)
    other(0)
    y_second(1)
    alpha_added(1)
    beta_first()
    summed(0)
    y_second(2)
    beta_plain()
    for j in range(3):
        y_home(j)
    y_last(0)
    alpha_last(0)
    y_last(1)
    alpha_last(1)
    alpha_deliver(0)
    beta_added()
    y_last(2)
    alpha_deliver(1)
    beta_last()

    for j in range(3):
        net.wait(("e", j, 1), yend.at[j, 1])
        net.wait(("e", j, 0), yend.at[j, 0], when=away)

    @pl.when(own)
    def _():
        here = span(c * depth, depth, depth)
        for j, out in enumerate((dq, dk, dv)):
            out[...] = (yhome[j, :, here] + yend[j, 1].astype(F32)).T * 0.125

    @pl.when(away)
    def _():
        for j, out in enumerate((dq, dk, dv)):
            out[...] = (yend[j, 0].astype(F32) + yend[j, 1].astype(F32)).T * 0.125

    for cols in pieces + (beta,):
        for hf in range(2):
            net.wait(
                ("d", cols.start), dbuf.at[hf, :, cols], offset=hf, width=2, when=jnp.logical_or(away, c != hf)
            )

    @pl.when(own)
    def _():
        dbuf[c] = psum[b_rows(0, 0), :]

    for hf in range(2):
        dh[:, hf * half : (hf + 1) * half] = dbuf[hf]
    net.drain()
    assert len(net.groups) <= SENDS and net.total <= RECVS, (len(net.groups), net.total)


def whole(rate, h, c, wq, wk, wv):
    rows, width = h.shape
    depth, columns = wq.shape
    blocks = SIDE * SIDE
    length = rows * blocks
    half = width // 2
    rest = half - FIRST
    vmem = pl.BlockSpec(memory_space=pltpu.VMEM)
    dma = pltpu.SemaphoreType.DMA

    def buf(*shape, kind=BF16):
        return pltpu.VMEM(shape, kind)

    return pl.pallas_call(
        whole_kernel,
        out_shape=(buf(rows, width),) + (buf(depth, columns, kind=F32),) * 3,
        in_specs=[pl.BlockSpec(memory_space=pltpu.SMEM)] + [pl.BlockSpec(memory_space=pl.ANY)] * 5,
        out_specs=(vmem,) * 4,
        scratch_shapes=[
            buf(length, width),
            buf(length, columns),
            buf(depth * 8, 3 * columns),
            buf(length, 3 * columns),
            buf(length, 3 * columns),
            buf(3 * columns, length),
            buf(columns, columns, kind=F32),
            buf(columns, columns, kind=F32),
            buf(2, 8, columns, kind=F32),
            buf(BLOCK, BLOCK, kind=F32),
            buf(BLOCK, BLOCK, kind=F32),
            buf(2, BLOCK, columns, kind=F32),
            buf(length, half),
            buf(length, half),
            buf(length, half),
            buf(2, 2 * rows, FIRST),
            buf(2, 4 * rows, FIRST),
            buf(2 * rows, FIRST),
            buf(SIDE, 2 * rows, rest),
            buf(2, rows, rest),
            buf(2, 2 * rows, rest),
            buf(2, rows, half),
            buf(3, columns, 2 * depth),
            buf(3, 2, columns, 2 * depth),
            buf(3, columns, 2 * depth, kind=F32),
            buf(3, 2, columns, depth),
            buf(3, 2, columns, 2 * depth),
            buf(3, columns, 2 * depth),
            buf(3, 2, columns, depth),
            buf(rows, width),
            buf(rows, columns * blocks),
            buf(3, depth, columns),
            dma((5,)),
            dma((SENDS,)),
            dma((RECVS,)),
        ],
        compiler_params=pltpu.CompilerParams(
            collective_id=0, has_side_effects=True, vmem_limit_bytes=VMEM_LIMIT
        ),
        name="whole",
    )(rate, h, c, wq, wk, wv)


def finish_kernel(count, *refs):
    ins, outs, sems = refs[:count], refs[count : 2 * count], refs[2 * count]
    moves = [pltpu.make_async_copy(ins[i], outs[i], sems.at[i]) for i in range(count)]
    for move in moves:
        move.start()
    for move in moves:
        move.wait()


def finish(*arrays):
    count = len(arrays)
    return pl.pallas_call(
        functools.partial(finish_kernel, count),
        out_shape=tuple(jax.ShapeDtypeStruct(a.shape, a.dtype) for a in arrays),
        in_specs=[pl.BlockSpec(memory_space=pltpu.VMEM)] * count,
        out_specs=(pl.BlockSpec(memory_space=pl.ANY),) * count,
        scratch_shapes=[pltpu.SemaphoreType.DMA((count,))],
        compiler_params=pltpu.CompilerParams(vmem_limit_bytes=4 * 1024 * 1024),
        name="finish",
    )(*arrays)


def body(hidden_in, mix_cotangent, query_weight, key_weight, value_weight, decay_log):
    dh, dq, dk, dv = finish(
        *whole(decay_log, hidden_in[0], mix_cotangent[0], query_weight, key_weight, value_weight)
    )
    return dh[None], dq, dk, dv


def solution(mesh):
    placed = (
        P("dp", "sp", None),
        P("dp", "sp", None),
        P("dp", "sp"),
        P("dp", "sp"),
        P("dp", "sp"),
        P("sp"),
    )
    return jax.shard_map(
        body,
        mesh=mesh,
        in_specs=placed,
        out_specs=(P("dp", "sp", None), P("dp", "sp"), P("dp", "sp"), P("dp", "sp")),
        check_vma=False,
    )
```

```python
import functools

import jax
import jax.numpy as jnp
from jax import lax
from jax.experimental import pallas as pl
from jax.experimental.pallas import tpu as pltpu
from jax.sharding import PartitionSpec as P

BLOCK = 256
SIDE = 4
FIRST = 640
EARLY = 384
F32 = jnp.float32
BF16 = jnp.bfloat16
MESH = pl.DeviceIdType.MESH
NN = (((1,), (0,)), ((), ()))
NT = (((1,), (1,)), ((), ()))
TN = (((0,), (0,)), ((), ()))
VMEM_LIMIT = 60 * 1024 * 1024
GROUP = 4 * 1024 * 1024
CELL = 32 * 1024
SENDS = 9
RECVS = 120


def dot(a, b, dims=NN):
    return lax.dot_general(a, b, dims, preferred_element_type=F32)


def span(start, size, step):
    return pl.ds(pl.multiple_of(start, step), size)


class Net:
    def __init__(self, send, recv, meter, small, somewhere):
        self.send, self.recv, self.somewhere = send, recv, somewhere
        self.meter, self.small = meter, small
        self.names, self.total, self.groups, self.open = {}, 0, [], {}

    def index(self, name, width=1):
        if name not in self.names:
            self.names[name] = self.total
            self.total += width
        return self.names[name]

    def lane(self, kind, when, size):
        group = self.open.get(kind)
        if group is None or self.groups[group][1] + size > GROUP:
            self.open[kind] = group = len(self.groups)
            self.groups.append([when, 0])
        self.groups[group][1] += size
        return group

    def copy(self, src, dst, lane, slot, where):
        return pltpu.make_async_remote_copy(
            src_ref=src, dst_ref=dst, send_sem=self.send.at[lane], recv_sem=self.recv.at[slot],
            device_id=where, device_id_type=MESH,
        )

    def start(self, name, src, dst, where, offset=0, width=1, when=None):
        slot = self.index(name, width) + offset
        size = 2 if src.dtype == BF16 else 4
        for extent in src.shape:
            size *= extent
        lane = self.lane(id(when) if size % CELL == 0 else name, when, size)
        if when is None:
            self.copy(src, dst, lane, slot, where).start()
        else:
            pl.when(when)(lambda: self.copy(src, dst, lane, slot, where).start())

    def wait(self, name, dst, offset=0, width=1, when=None):
        slot = self.index(name, width) + offset
        if when is None:
            self.copy(dst, dst, 0, slot, self.somewhere).wait_recv()
        else:
            pl.when(when)(lambda: self.copy(dst, dst, 0, slot, self.somewhere).wait_recv())

    def drain(self):
        for lane, (when, size) in enumerate(self.groups):
            ref = self.meter.at[pl.ds(0, size // (2 * self.meter.shape[1]))] if size % CELL == 0 else self.small

            def run():
                self.copy(ref, ref, lane, 0, self.somewhere).wait_send()

            if when is None:
                run()
            else:
                pl.when(when)(run)


def whole_kernel(
    rate, h_far, c_far, wq, wk, wv, dh, dq, dk, dv,
    h_all, c_all, w_all, p_all, g_all, g_turn, state, back, rates, inner, inner_t, decays,
    pout, pin, psum, ra1, ra2, ra3, rb0, rb1, rb2, dbuf,
    ysend, yone, yhome, yr1, yr2, yout, yend, h_in, c_in, w_in, local, send, recv,
):
    s = lax.axis_index("sp")
    d = lax.axis_index("dp")
    z, x = s // SIDE, s % SIDE
    y, c = d // 2, d % 2
    u = x // 2
    xl = x - 2 * u
    own = c == u
    away = c != u
    rows, width = h_in.shape
    depth, columns = wq.shape
    half = width // 2
    four = rows * SIDE
    two = rows * 2
    blocks = SIDE * SIDE
    scale = columns ** (-0.5)

    def at(zz=None, xx=None, yy=None, cc=None):
        zz, xx = z if zz is None else zz, x if xx is None else xx
        yy, cc = y if yy is None else yy, c if cc is None else cc
        return {"sp": zz * SIDE + xx, "dp": yy * 2 + cc}

    def turned(v, by):
        return (v + by + SIDE) % SIDE

    mate = at(cc=1 - c)
    pair = at(xx=x + 1 - 2 * xl)
    zs = {1: at(zz=turned(z, 1)), -1: at(zz=turned(z, -1))}
    ys = {1: at(yy=turned(y, 1)), -1: at(yy=turned(y, -1))}
    cross = 3 - x
    net = Net(send, recv, h_all, rates.at[0], mate)
    weights = [w_in.at[j] for j in range(3)]
    loads = [
        pltpu.make_async_copy(src, dst, local.at[i])
        for i, (src, dst) in enumerate(zip((h_far, wq, wk, wv, c_far), [h_in] + weights + [c_in]))
    ]
    for load in loads:
        load.start()

    barrier = pltpu.get_barrier_semaphore()
    peers = [mate, ys[1], ys[-1]]
    for k in range(1, blocks):
        other = (s + k) % blocks
        peers += [{"sp": other, "dp": d}, {"sp": other, "dp": y * 2 + 1 - c}]
    for where in peers:
        pl.semaphore_signal(barrier, inc=1, device_id=where, device_id_type=MESH)
    rates[0] = jnp.full(rates.shape[1:], rate[0], F32)
    loads[0].wait()
    pl.semaphore_wait(barrier, len(peers))

    def r_rows(r):
        return span(turned(z, r) * four, four, four)

    def slot(r, col, b):
        return turned(z, r) * SIDE + 2 * (xl if col == 0 else 1 - xl) + b

    def h_ref(place, part, which):
        base = which * half
        lo, size = {"f": (0, half), "a": (0, FIRST), "b": (FIRST, half - FIRST)}[part]
        return h_all.at[span(place * rows, rows, rows), span(base + lo, size, 128)]

    def h_send(r, col, b, part, where, name):
        ref = h_ref(slot(r, col, b), part, c)
        net.start(name, ref, ref, where)

    def to_mate(r, col, b, part):
        h_send(r, col, b, part, mate, ("m", r))

    def h_wait(r, col, b, part, when=None):
        net.wait(("x", r, col, b, part), h_ref(slot(r, col, b), part, c), when=when)

    def w_ref(yy, cc, j):
        return w_all.at[span((yy * 2 + cc) * depth, depth, depth), pl.ds(j * columns, columns)]

    def w_near(j):
        net.start(("w0", j), weights[j], w_ref(y, c, j), mate, offset=c, width=2, when=away)

    def w_cross(j, who):
        net.start(("w0", j), weights[j], w_ref(y, c, j), at(xx=cross, cc=u), offset=c, width=2, when=who)

    mine = span(c * half, half, half)
    theirs = span((1 - c) * half, half, half)
    net.start(("x", 0, 0, 0, "f"), h_in.at[:, theirs], h_ref(slot(0, 0, 0), "f", 1 - c), mate, when=own)
    there = z * SIDE + 2 * (1 - xl) + 1
    for hf in range(2):
        net.start(
            ("x", 0, 0, 1, "f"), h_in.at[:, pl.ds(hf * half, half)], h_ref(there, "f", hf),
            at(xx=cross, cc=hf), when=away,
        )
    for load in loads[1:4]:
        load.wait()
    for j in range(3):
        w_near(j)
    for j in range(3):
        w_cross(j, away)
    net.start(("rate",), rates.at[0], rates.at[1], at(xx=cross))

    @pl.when(own)
    def _():
        h_all[span(slot(0, 0, 0) * rows, rows, rows), mine] = h_in[:, mine]
        for j in range(3):
            w_all[span(d * depth, depth, depth), j * columns : (j + 1) * columns] = weights[j][...]

    def spread(b):
        for way in (1, -1):
            h_send(0, 0, b, "f", zs[way], ("x", -way, 0, b, "f"))
        h_send(0, 0, b, "f", pair, ("x", 0, 1, b, "f"))
        to_mate(0, 0, b, "f")

    def w_spread(j, who):
        for cc in range(2):
            far = who if who is away else jnp.logical_and(own, c != cc)
            net.wait(("w0", j), w_ref(y, cc, j), offset=cc, width=2, when=far)
            for way in (1, -1):
                name = ("w1", j, -way) if (way == 1) == (cc == 0) else ("wt", j)
                net.start(name, w_ref(y, cc, j), w_ref(y, cc, j), ys[way], when=who)

    def w_forward(j, who):
        for way, cc in ((1, 0), (-1, 1)):
            ref = w_ref(turned(y, -way), cc, j)
            net.wait(("w1", j, -way), ref, when=who)
            net.start(("wt", j), ref, ref, ys[way], when=who)

    def from_pair(b):
        h_wait(0, 1, b, "f")
        for way in (1, -1):
            h_send(0, 1, b, "a", zs[way], ("x", -way, 1, b, "a"))
        to_mate(0, 1, b, "f")

    def from_side(b):
        fast = 1 if b == 0 else -1
        for r in (-fast, fast):
            h_wait(r, 0, b, "f")
            if r == -fast:
                h_send(r, 0, b, "f", zs[fast], ("x", 2, 0, b, "f"))
            h_send(r, 0, b, "b", pair, ("x", r, 1, b, "b"))
            to_mate(r, 0, b, "f")

    def from_corner(b):
        fast = 1 if b == 0 else -1
        for r in (-fast, fast):
            h_wait(r, 1, b, "a")
            if r == -fast:
                h_send(r, 1, b, "a", zs[fast], ("x", 2, 1, b, "a"))
            to_mate(r, 1, b, "a")

    def from_far(b):
        h_wait(2, 0, b, "f")
        h_send(2, 0, b, "b", pair, ("x", 2, 1, b, "b"))
        to_mate(2, 0, b, "f")

    def c_send(dz, dx):
        hz, hx = turned(z, dz), turned(x, dx)
        head = hz * SIDE + hx
        far = (hx // 2 - c) * (hx // 2 - c)
        net.start(
            ("c",), c_in.at[:, span(head * columns, columns, columns)],
            c_all.at[span(s * rows, rows, rows)],
            {"sp": hz * SIDE + hx + far * (3 - 2 * hx), "dp": y * 2 + c + far * (1 - 2 * c)},
            offset=s, width=blocks, when=away if (dz, dx) == (0, 0) else None,
        )

    diagonal = [(dz, (dz + k) % SIDE) for k in range(SIDE) for dz in (2, 1, 3, 0)]

    h_wait(0, 0, 0, "f", when=away)
    spread(0)
    for j in range(3):
        w_spread(j, own)
    h_wait(0, 0, 1, "f")
    spread(1)
    for j in range(3):
        w_cross(j, own)
    from_side(0)
    from_pair(0)
    w_forward(0, own)
    w_spread(0, away)
    from_side(1)
    from_pair(1)
    w_forward(1, own)
    w_spread(1, away)
    w_forward(2, own)
    w_spread(2, away)
    loads[4].wait()
    for dz, dx in diagonal[:8]:
        c_send(dz, dx)

    @pl.when(own)
    def _():
        c_all[span(s * rows, rows, rows), :] = c_in[:, span(s * columns, columns, columns)]

    def w_ready(who):
        for j in range(3):
            net.wait(("wt", j), w_all.at[pl.ds(0, 4 * depth), pl.ds(j * columns, columns)], when=who)

    def mate_wait(r):
        net.wait(("m", r), h_all.at[r_rows(r), theirs])

    def project(first, step, count):
        @pl.loop(0, 3 * count)
        def _(t):
            place = span(turned(z, first + step * (t // 3)) * four, four, four)
            j = t % 3
            cols = span(j * columns, columns, columns)
            value = dot(h_all[place, :], w_all[:, cols]).astype(BF16)
            factor = jnp.where(j == 1, scale, 1.0).astype(F32)
            p_all[place, cols] = (value.astype(F32) * factor).astype(BF16)

    def betas(b):
        for r in (-1, 1):
            h_wait(r, 1, b, "b")
            to_mate(r, 1, b, "b")

    from_far(0)
    betas(0)
    w_forward(0, away)
    w_forward(1, away)
    mate_wait(0)
    w_ready(own)
    pl.when(own)(lambda: project(0, 0, 1))
    w_forward(2, away)
    from_corner(0)
    betas(1)
    from_far(1)
    from_corner(1)
    for dz, dx in diagonal[8:]:
        c_send(dz, dx)
    w_ready(away)
    pl.when(away)(lambda: project(0, 0, 1))
    for part in ("a", "b"):
        for b in range(2):
            h_wait(2, 1, b, part)
            to_mate(2, 1, b, part)
    mate_wait(1)
    mate_wait(-1)
    project(1, 2, 2)
    mate_wait(2)
    project(2, 0, 1)

    net.wait(("rate",), rates.at[1])
    for k in range(blocks):
        source = (s + k) % blocks
        net.wait(
            ("c",), c_all.at[span(source * rows, rows, rows)], offset=source, width=blocks,
            when=away if k == 0 else None,
        )

    pick = jnp.where(own, 1.0, 0.0).astype(F32)
    g = rates[0] * pick + rates[1] * (1.0 - pick)
    g_row = g[0:1, :]
    gap = (
        lax.broadcasted_iota(jnp.int32, (BLOCK, BLOCK), 0) - lax.broadcasted_iota(jnp.int32, (BLOCK, BLOCK), 1)
    ).astype(F32)
    place = lax.broadcasted_iota(jnp.int32, (BLOCK, columns), 0).astype(F32)
    inner[...] = jnp.where(gap >= 0, jnp.exp(g_row * jnp.maximum(gap, 0.0)), 0.0)
    inner_t[...] = jnp.where(gap <= 0, jnp.exp(g_row * jnp.maximum(-gap, 0.0)), 0.0)
    decays[0] = jnp.exp(g_row * (place + 1.0))
    decays[1] = jnp.exp(g_row * (BLOCK - 1.0 - place))
    block_decay = jnp.exp(g_row * BLOCK)
    state[...] = jnp.zeros_like(state)
    back[...] = jnp.zeros_like(back)
    parts = [slice(j * columns, (j + 1) * columns) for j in range(3)]
    count = BLOCK // rows

    def slots(i):
        places = []
        for w in range(count):
            p = i * count + w
            pz, px = p // SIDE, p % SIDE
            b = (px // 2 - u) * (px // 2 - u)
            places.append(span((pz * SIDE + 2 * (px + b * (3 - 2 * px) - 2 * u) + b) * rows, rows, rows))
        return places

    def get(places, part):
        return jnp.concatenate([p_all[place, part] for place in places], axis=0)

    def put(places, part, grad):
        grad = grad.astype(BF16)
        for w, place in enumerate(places):
            g_all[place, part] = grad[w * rows : (w + 1) * rows]
        grad = grad.T
        for w, place in enumerate(places):
            g_turn[part, place] = grad[:, w * rows : (w + 1) * rows]

    def forward(i):
        places = slots(i)
        k, v = get(places, parts[1]), get(places, parts[2])
        ct = c_all[span(i * BLOCK, BLOCK, BLOCK), :]
        mixed = (dot(ct, v, NT) * inner[...]).astype(BF16)
        held = state[...]
        grad_q = dot(mixed, k) + dot(ct, held.astype(BF16), NT) * decays[0]
        weighted = (k.astype(F32) * decays[1]).astype(BF16)
        state[...] = held * block_decay + dot(weighted, v, TN)
        put(places, parts[0], grad_q)

    def backward(i):
        places = slots(i)
        q, k, v = (get(places, part) for part in parts)
        ct = c_all[span(i * BLOCK, BLOCK, BLOCK), :]
        mixed_t = (dot(v, ct, NT) * inner_t[...]).astype(BF16)
        scores_t = (dot(k, q, NT) * inner_t[...]).astype(BF16)
        held = back[...]
        held_bf = held.astype(BF16)
        grad_v = dot(scores_t, ct) + dot(k, held_bf) * decays[1]
        grad_k = (dot(mixed_t, q) + dot(v, held_bf, NT) * decays[1]) * scale
        weighted = (q.astype(F32) * decays[0]).astype(BF16)
        back[...] = held * block_decay + dot(weighted, ct, TN)
        put(places, parts[1], grad_k)
        put(places, parts[2], grad_v)

    steps = rows * blocks // BLOCK

    @pl.loop(0, steps // 2)
    def _(t):
        for w in range(2):
            forward(2 * t + w)
            backward(steps - 1 - 2 * t - w)

    pieces = (pl.ds(0, EARLY), pl.ds(EARLY, FIRST - EARLY))
    beta = pl.ds(FIRST, half - FIRST)
    chunk = half // 2

    def pick_rows(r, hf):
        return span(turned(z, r) * four + hf * two, two, two)

    def other(r, i):
        cols = span(i * chunk, chunk, chunk)
        value = dot(g_all[r_rows(r), :], w_all[span((1 - c) * half + i * chunk, chunk, chunk), :], NT)
        pout[r_rows(r), cols] = value.astype(BF16)
        net.start(("p", r, i), pout.at[r_rows(r), cols], pin.at[r_rows(r), cols], mate)

    def summed(r, i):
        cols = span(i * chunk, chunk, chunk)
        net.wait(("p", r, i), pin.at[r_rows(r), cols])
        value = dot(g_all[r_rows(r), :], w_all[span(c * half + i * chunk, chunk, chunk), :], NT)
        psum[r_rows(r), cols] = (value + pin[r_rows(r), cols].astype(F32)).astype(BF16)
        if i == 1:
            net.start(("b0", r), psum.at[pick_rows(r, 1 - xl), beta], rb0.at[r % SIDE], pair)

    def add(place, cols, *refs):
        total = psum[place, cols].astype(F32)
        for ref in refs:
            total = total + ref.astype(F32)
        psum[place, cols] = total.astype(BF16)

    def a1(i, e):
        return ra1.at[e, :, pieces[i]]

    def a2(i, e, hf):
        return ra2.at[e, pl.ds(hf * two, two), pieces[i]]

    def a3(i):
        return ra3.at[:, pieces[i]]

    def alpha_send(i, r, hf, way, name, dst):
        net.start(name, psum.at[pick_rows(r, hf), pieces[i]], dst, zs[way])

    def alpha_first(i):
        alpha_send(i, 2, 0, 1, ("a1", i, 0), a1(i, 0))
        alpha_send(i, 2, 1, -1, ("a1", i, 1), a1(i, 1))

    def alpha_plain(i, r):
        e = 0 if r == 1 else 1
        alpha_send(i, r, 1 - e, r, ("a2", i, e, 1 - e), a2(i, e, 1 - e))

    def alpha_added(i):
        for e, r in ((0, 1), (1, -1)):
            net.wait(("a1", i, e), a1(i, e))
            add(pick_rows(r, e), pieces[i], a1(i, e)[...])
            alpha_send(i, r, e, r, ("a2", i, e, e), a2(i, e, e))

    def alpha_last(i):
        for e, hf in ((0, 1), (1, 0), (0, 0), (1, 1)):
            net.wait(("a2", i, e, hf), a2(i, e, hf))
        for hf in range(2):
            add(pick_rows(0, hf), pieces[i], a2(i, 0, hf)[...], a2(i, 1, hf)[...])
        net.start(("a3", i), psum.at[pick_rows(0, 1 - xl), pieces[i]], a3(i), pair)

    def deliver(cols):
        lo = cols.start
        dst = dbuf.at[c, :, cols]
        net.start(("d", lo), psum.at[b_rows(0, 1), cols], dst, at(xx=cross, cc=u), offset=c, width=2)
        net.start(("d", lo), psum.at[b_rows(0, 0), cols], dst, mate, offset=c, width=2, when=away)

    def alpha_deliver(i):
        net.wait(("a3", i), a3(i))
        add(pick_rows(0, xl), pieces[i], a3(i)[...])
        deliver(pieces[i])

    def b_rows(r, b):
        return span(turned(z, r) * four + xl * two + b * rows, rows, rows)

    def b2(e, b):
        return rb2.at[e, pl.ds(b * rows, rows)]

    def beta_send(r, b, way, name, dst):
        net.start(name, psum.at[b_rows(r, b), beta], dst, zs[way])

    def beta_take(r):
        net.wait(("b0", r), rb0.at[r % SIDE])
        add(pick_rows(r, xl), beta, rb0[r % SIDE])

    def beta_first():
        beta_take(2)
        beta_send(2, 0, 1, ("b1", 0), rb1.at[0])
        beta_send(2, 1, -1, ("b1", 1), rb1.at[1])

    def beta_plain():
        for r, b, e in ((1, 1, 0), (-1, 0, 1)):
            beta_take(r)
            beta_send(r, b, r, ("b2", e, b), b2(e, b))

    def beta_added():
        for r, b, e in ((1, 0, 0), (-1, 1, 1)):
            net.wait(("b1", e), rb1.at[e])
            add(b_rows(r, b), beta, rb1[e])
            beta_send(r, b, r, ("b2", e, b), b2(e, b))

    def beta_last():
        beta_take(0)
        for e, b in ((0, 1), (1, 0), (0, 0), (1, 1)):
            net.wait(("b2", e, b), b2(e, b))
        add(pick_rows(0, xl), beta, rb2[0], rb2[1])
        deliver(beta)

    lanes = [pl.ds(hf * depth, depth) for hf in range(2)]

    def w_grad(r, j):
        cols = span(turned(y, r) * 2 * depth, 2 * depth, depth)
        return dot(g_turn[parts[j], :], h_all[:, cols])

    def y_first(j):
        ysend[j] = w_grad(2, j).astype(BF16)
        for e, way in ((0, 1), (1, -1)):
            net.start(("y1", j, e), ysend.at[j, :, lanes[e]], yr1.at[j, e], ys[way])

    def y2(j, e, hf):
        return yr2.at[j, e, :, lanes[hf]]

    def y_second(j):
        for e, r in ((0, 1), (1, -1)):
            value = w_grad(r, j)
            keep = value[:, e * depth : (e + 1) * depth]
            yone[j, e, :, lanes[1 - e]] = value[:, (1 - e) * depth : (2 - e) * depth].astype(BF16)
            net.start(("y2", j, e, 1 - e), yone.at[j, e, :, lanes[1 - e]], y2(j, e, 1 - e), ys[r])
            net.wait(("y1", j, e), yr1.at[j, e])
            yone[j, e, :, lanes[e]] = (keep + yr1[j, e].astype(F32)).astype(BF16)
            net.start(("y2", j, e, e), yone.at[j, e, :, lanes[e]], y2(j, e, e), ys[r])

    def y_home(j):
        yhome[j] = w_grad(0, j)

    def y_last(j):
        for e, hf in ((0, 1), (1, 0), (0, 0), (1, 1)):
            net.wait(("y2", j, e, hf), y2(j, e, hf))
        total = yhome[j] + yr2[j, 0].astype(F32) + yr2[j, 1].astype(F32)
        yhome[j] = total
        yout[j] = total.astype(BF16)
        half_of = span((1 - c) * depth, depth, depth)
        net.start(("e", j, 0), yout.at[j, :, half_of], yend.at[j, 0], mate, when=own)
        for hf in range(2):
            net.start(("e", j, 1), yout.at[j, :, lanes[hf]], yend.at[j, 1], at(xx=cross, cc=hf), when=away)

    y_first(0)
    other(2, 0)
    other(2, 1)
    y_first(1)
    summed(2, 0)
    alpha_first(0)
    summed(2, 1)
    alpha_first(1)
    y_first(2)
    other(1, 0)
    other(1, 1)
    other(-1, 0)
    other(-1, 1)
    y_second(0)
    summed(1, 0)
    alpha_plain(0, 1)
    summed(-1, 0)
    alpha_plain(0, -1)
    summed(1, 1)
    summed(-1, 1)
    alpha_added(0)
    alpha_plain(1, 1)
    alpha_plain(1, -1)
    y_second(1)
    other(0, 0)
    other(0, 1)
    alpha_added(1)
    beta_first()
    summed(0, 0)
    summed(0, 1)
    y_second(2)
    beta_plain()
    for j in range(3):
        y_home(j)
    y_last(0)
    alpha_last(0)
    y_last(1)
    alpha_last(1)
    alpha_deliver(0)
    beta_added()
    y_last(2)
    alpha_deliver(1)
    beta_last()

    for j in range(3):
        net.wait(("e", j, 1), yend.at[j, 1])
        net.wait(("e", j, 0), yend.at[j, 0], when=away)

    @pl.when(own)
    def _():
        here = span(c * depth, depth, depth)
        for j, out in enumerate((dq, dk, dv)):
            out[...] = (yhome[j, :, here] + yend[j, 1].astype(F32)).T * 0.125

    @pl.when(away)
    def _():
        for j, out in enumerate((dq, dk, dv)):
            out[...] = (yend[j, 0].astype(F32) + yend[j, 1].astype(F32)).T * 0.125

    for cols in pieces + (beta,):
        for hf in range(2):
            net.wait(
                ("d", cols.start), dbuf.at[hf, :, cols], offset=hf, width=2, when=jnp.logical_or(away, c != hf)
            )

    @pl.when(own)
    def _():
        dbuf[c] = psum[b_rows(0, 0), :]

    for hf in range(2):
        dh[:, hf * half : (hf + 1) * half] = dbuf[hf]
    net.drain()
    assert len(net.groups) <= SENDS and net.total <= RECVS, (len(net.groups), net.total)


def whole(rate, h, c, wq, wk, wv):
    rows, width = h.shape
    depth, columns = wq.shape
    blocks = SIDE * SIDE
    length = rows * blocks
    half = width // 2
    rest = half - FIRST
    vmem = pl.BlockSpec(memory_space=pltpu.VMEM)
    dma = pltpu.SemaphoreType.DMA

    def buf(*shape, kind=BF16):
        return pltpu.VMEM(shape, kind)

    return pl.pallas_call(
        whole_kernel,
        out_shape=(buf(rows, width),) + (buf(depth, columns, kind=F32),) * 3,
        in_specs=[pl.BlockSpec(memory_space=pltpu.SMEM)] + [pl.BlockSpec(memory_space=pl.ANY)] * 5,
        out_specs=(vmem,) * 4,
        scratch_shapes=[
            buf(length, width),
            buf(length, columns),
            buf(depth * 8, 3 * columns),
            buf(length, 3 * columns),
            buf(length, 3 * columns),
            buf(3 * columns, length),
            buf(columns, columns, kind=F32),
            buf(columns, columns, kind=F32),
            buf(2, 8, columns, kind=F32),
            buf(BLOCK, BLOCK, kind=F32),
            buf(BLOCK, BLOCK, kind=F32),
            buf(2, BLOCK, columns, kind=F32),
            buf(length, half),
            buf(length, half),
            buf(length, half),
            buf(2, 2 * rows, FIRST),
            buf(2, 4 * rows, FIRST),
            buf(2 * rows, FIRST),
            buf(SIDE, 2 * rows, rest),
            buf(2, rows, rest),
            buf(2, 2 * rows, rest),
            buf(2, rows, half),
            buf(3, columns, 2 * depth),
            buf(3, 2, columns, 2 * depth),
            buf(3, columns, 2 * depth, kind=F32),
            buf(3, 2, columns, depth),
            buf(3, 2, columns, 2 * depth),
            buf(3, columns, 2 * depth),
            buf(3, 2, columns, depth),
            buf(rows, width),
            buf(rows, columns * blocks),
            buf(3, depth, columns),
            dma((5,)),
            dma((SENDS,)),
            dma((RECVS,)),
        ],
        compiler_params=pltpu.CompilerParams(
            collective_id=0, has_side_effects=True, vmem_limit_bytes=VMEM_LIMIT
        ),
        name="whole",
    )(rate, h, c, wq, wk, wv)


def finish_kernel(count, *refs):
    ins, outs, sems = refs[:count], refs[count : 2 * count], refs[2 * count]
    moves = [pltpu.make_async_copy(ins[i], outs[i], sems.at[i]) for i in range(count)]
    for move in moves:
        move.start()
    for move in moves:
        move.wait()


def finish(*arrays):
    count = len(arrays)
    return pl.pallas_call(
        functools.partial(finish_kernel, count),
        out_shape=tuple(jax.ShapeDtypeStruct(a.shape, a.dtype) for a in arrays),
        in_specs=[pl.BlockSpec(memory_space=pltpu.VMEM)] * count,
        out_specs=(pl.BlockSpec(memory_space=pl.ANY),) * count,
        scratch_shapes=[pltpu.SemaphoreType.DMA((count,))],
        compiler_params=pltpu.CompilerParams(vmem_limit_bytes=4 * 1024 * 1024),
        name="finish",
    )(*arrays)


def body(hidden_in, mix_cotangent, query_weight, key_weight, value_weight, decay_log):
    dh, dq, dk, dv = finish(
        *whole(decay_log, hidden_in[0], mix_cotangent[0], query_weight, key_weight, value_weight)
    )
    return dh[None], dq, dk, dv


def solution(mesh):
    placed = (
        P("dp", "sp", None),
        P("dp", "sp", None),
        P("dp", "sp"),
        P("dp", "sp"),
        P("dp", "sp"),
        P("sp"),
    )
    return jax.shard_map(
        body,
        mesh=mesh,
        in_specs=placed,
        out_specs=(P("dp", "sp", None), P("dp", "sp"), P("dp", "sp"), P("dp", "sp")),
        check_vma=False,
    )
```

```python
import functools

import jax
import jax.numpy as jnp
from jax import lax
from jax.experimental import pallas as pl
from jax.experimental.pallas import tpu as pltpu
from jax.sharding import PartitionSpec as P

BLOCK = 256
SIDE = 4
FIRST = 640
PIECES = ((512, 128), (0, 256), (256, 256))
EAGER = 12
F32 = jnp.float32
BF16 = jnp.bfloat16
MESH = pl.DeviceIdType.MESH
NN = (((1,), (0,)), ((), ()))
NT = (((1,), (1,)), ((), ()))
TN = (((0,), (0,)), ((), ()))
VMEM_LIMIT = 60 * 1024 * 1024
GROUP = 4 * 1024 * 1024
CELL = 32 * 1024
SENDS = 9
RECVS = 83


def dot(a, b, dims=NN):
    return lax.dot_general(a, b, dims, preferred_element_type=F32)


def span(start, size, step):
    return pl.ds(pl.multiple_of(start, step), size)


class Net:
    def __init__(self, send, recv, meter, small, somewhere):
        self.send, self.recv, self.somewhere = send, recv, somewhere
        self.meter, self.small = meter, small
        self.names, self.total, self.groups, self.open = {}, 0, [], {}

    def index(self, name, width=1):
        if name not in self.names:
            self.names[name] = self.total
            self.total += width
        return self.names[name]

    def lane(self, kind, when, size):
        group = self.open.get(kind)
        if group is None or self.groups[group][1] + size > GROUP:
            self.open[kind] = group = len(self.groups)
            self.groups.append([when, 0])
        self.groups[group][1] += size
        return group

    def copy(self, src, dst, lane, slot, where):
        return pltpu.make_async_remote_copy(
            src_ref=src, dst_ref=dst, send_sem=self.send.at[lane], recv_sem=self.recv.at[slot],
            device_id=where, device_id_type=MESH,
        )

    def start(self, name, src, dst, where, offset=0, width=1, when=None):
        slot = self.index(name, width) + offset
        size = 2 if src.dtype == BF16 else 4
        for extent in src.shape:
            size *= extent
        lane = self.lane(id(when) if size % CELL == 0 else name, when, size)
        if when is None:
            self.copy(src, dst, lane, slot, where).start()
        else:
            pl.when(when)(lambda: self.copy(src, dst, lane, slot, where).start())

    def wait(self, name, dst, offset=0, width=1, when=None):
        slot = self.index(name, width) + offset
        if when is None:
            self.copy(dst, dst, 0, slot, self.somewhere).wait_recv()
        else:
            pl.when(when)(lambda: self.copy(dst, dst, 0, slot, self.somewhere).wait_recv())

    def drain(self):
        for lane, (when, size) in enumerate(self.groups):
            ref = self.meter.at[pl.ds(0, size // (2 * self.meter.shape[1]))] if size % CELL == 0 else self.small

            def run():
                self.copy(ref, ref, lane, 0, self.somewhere).wait_send()

            if when is None:
                run()
            else:
                pl.when(when)(run)


def whole_kernel(
    rate, h_far, c_far, wq, wk, wv, dh, dq, dk, dv,
    h_all, c_all, w_all, p_all, g_all, g_turn, state, back, rates, inner, inner_t, decays,
    pout, pin, psum, ra1, ra2, ra3, rb0, rb1, rb2, dbuf,
    ysend, yone, yhome, yr1, yr2, yout, yend, h_in, c_in, w_in, local, send, recv,
):
    s = lax.axis_index("sp")
    d = lax.axis_index("dp")
    z, x = s // SIDE, s % SIDE
    y, c = d // 2, d % 2
    u = x // 2
    xl = x - 2 * u
    own = c == u
    away = c != u
    rows, width = h_in.shape
    depth, columns = wq.shape
    half = width // 2
    four = rows * SIDE
    two = rows * 2
    blocks = SIDE * SIDE
    scale = columns ** (-0.5)

    def at(zz=None, xx=None, yy=None, cc=None):
        zz, xx = z if zz is None else zz, x if xx is None else xx
        yy, cc = y if yy is None else yy, c if cc is None else cc
        return {"sp": zz * SIDE + xx, "dp": yy * 2 + cc}

    def turned(v, by):
        return (v + by + SIDE) % SIDE

    mate = at(cc=1 - c)
    pair = at(xx=x + 1 - 2 * xl)
    zs = {1: at(zz=turned(z, 1)), -1: at(zz=turned(z, -1))}
    ys = {1: at(yy=turned(y, 1)), -1: at(yy=turned(y, -1))}
    cross = 3 - x
    net = Net(send, recv, h_all, rates.at[0], mate)
    weights = [w_in.at[j] for j in range(3)]
    loads = [
        pltpu.make_async_copy(src, dst, local.at[i])
        for i, (src, dst) in enumerate(zip((h_far, wq, wk, wv, c_far), [h_in] + weights + [c_in]))
    ]
    for load in loads:
        load.start()

    barrier = pltpu.get_barrier_semaphore()
    peers = [mate, ys[1], ys[-1]]
    for k in range(1, blocks):
        other = (s + k) % blocks
        peers += [{"sp": other, "dp": d}, {"sp": other, "dp": y * 2 + 1 - c}]
    for where in peers:
        pl.semaphore_signal(barrier, inc=1, device_id=where, device_id_type=MESH)
    rates[0] = jnp.full(rates.shape[1:], rate[0], F32)
    loads[0].wait()
    pl.semaphore_wait(barrier, len(peers))

    def r_rows(r):
        return span(turned(z, r) * four, four, four)

    def slot(r, col, b):
        return turned(z, r) * SIDE + 2 * (xl if col == 0 else 1 - xl) + b

    def h_ref(place, part, which):
        base = which * half
        lo, size = {"f": (0, half), "a": (0, FIRST), "b": (FIRST, half - FIRST)}[part]
        return h_all.at[span(place * rows, rows, rows), span(base + lo, size, 128)]

    def h_send(r, col, b, part, where, name):
        ref = h_ref(slot(r, col, b), part, c)
        net.start(name, ref, ref, where)

    def to_mate(r, col, b, part):
        h_send(r, col, b, part, mate, ("m", r))

    def h_wait(r, col, b, part, when=None):
        net.wait(("x", r, col, b, part), h_ref(slot(r, col, b), part, c), when=when)

    def w_ref(yy, cc, j):
        return w_all.at[span((yy * 2 + cc) * depth, depth, depth), pl.ds(j * columns, columns)]

    def w_near(j):
        net.start(("w0", j), weights[j], w_ref(y, c, j), mate, offset=c, width=2, when=away)

    def w_cross(j, who):
        net.start(("w0", j), weights[j], w_ref(y, c, j), at(xx=cross, cc=u), offset=c, width=2, when=who)

    mine = span(c * half, half, half)
    theirs = span((1 - c) * half, half, half)
    net.start(("x", 0, 0, 0, "f"), h_in.at[:, theirs], h_ref(slot(0, 0, 0), "f", 1 - c), mate, when=own)
    there = z * SIDE + 2 * (1 - xl) + 1
    for hf in range(2):
        net.start(
            ("x", 0, 0, 1, "f"), h_in.at[:, pl.ds(hf * half, half)], h_ref(there, "f", hf),
            at(xx=cross, cc=hf), when=away,
        )
    for load in loads[1:4]:
        load.wait()
    for j in range(3):
        w_near(j)
    for j in range(3):
        w_cross(j, away)
    net.start(("rate",), rates.at[0], rates.at[1], at(xx=cross))

    @pl.when(own)
    def _():
        h_all[span(slot(0, 0, 0) * rows, rows, rows), mine] = h_in[:, mine]
        for j in range(3):
            w_all[span(d * depth, depth, depth), j * columns : (j + 1) * columns] = weights[j][...]

    def spread(b):
        for way in (1, -1):
            h_send(0, 0, b, "f", zs[way], ("x", -way, 0, b, "f"))
        h_send(0, 0, b, "f", pair, ("x", 0, 1, b, "f"))
        to_mate(0, 0, b, "f")

    def w_spread(j, who):
        for cc in range(2):
            far = who if who is away else jnp.logical_and(own, c != cc)
            net.wait(("w0", j), w_ref(y, cc, j), offset=cc, width=2, when=far)
            for way in (1, -1):
                name = ("w1", j, -way) if (way == 1) == (cc == 0) else ("wt", j)
                net.start(name, w_ref(y, cc, j), w_ref(y, cc, j), ys[way], when=who)

    def w_forward(j, who):
        for way, cc in ((1, 0), (-1, 1)):
            ref = w_ref(turned(y, -way), cc, j)
            net.wait(("w1", j, -way), ref, when=who)
            net.start(("wt", j), ref, ref, ys[way], when=who)

    def from_pair(b):
        h_wait(0, 1, b, "f")
        for way in (1, -1):
            h_send(0, 1, b, "a", zs[way], ("x", -way, 1, b, "a"))
        to_mate(0, 1, b, "f")

    def from_side(b):
        for r in (-1, 1):
            h_wait(r, 0, b, "f")
            h_send(r, 0, b, "b", pair, ("x", r, 1, b, "b"))
            to_mate(r, 0, b, "f")

    def side_forward(b):
        fast = 1 if b == 0 else -1
        h_send(-fast, 0, b, "f", zs[fast], ("x", 2, 0, b, "f"))

    def from_corner(b):
        fast = 1 if b == 0 else -1
        for r in (-fast, fast):
            h_wait(r, 1, b, "a")
            if r == -fast:
                h_send(r, 1, b, "a", zs[fast], ("x", 2, 1, b, "a"))
            to_mate(r, 1, b, "a")

    def from_far(b):
        h_wait(2, 0, b, "f")
        h_send(2, 0, b, "b", pair, ("x", 2, 1, b, "b"))
        to_mate(2, 0, b, "f")

    def c_send(dz, dx):
        hz, hx = turned(z, dz), turned(x, dx)
        head = hz * SIDE + hx
        far = (hx // 2 - c) * (hx // 2 - c)
        net.start(
            ("c",), c_in.at[:, span(head * columns, columns, columns)],
            c_all.at[span(s * rows, rows, rows)],
            {"sp": hz * SIDE + hx + far * (3 - 2 * hx), "dp": y * 2 + c + far * (1 - 2 * c)},
            when=away if (dz, dx) == (0, 0) else None,
        )

    diagonal = [(dz, (dz + k) % SIDE) for k in range(SIDE) for dz in (2, 1, 3, 0)]

    h_wait(0, 0, 0, "f", when=away)
    spread(0)
    for j in range(3):
        w_spread(j, own)
    h_wait(0, 0, 1, "f")
    spread(1)
    for j in range(3):
        w_cross(j, own)
    from_side(0)
    from_pair(0)
    w_forward(0, own)
    w_spread(0, away)
    from_side(1)
    from_pair(1)
    side_forward(0)
    side_forward(1)
    w_forward(1, own)
    w_spread(1, away)
    w_forward(2, own)
    w_spread(2, away)

    def w_ready(j):
        net.wait(("wt", j), w_all.at[pl.ds(0, 4 * depth), pl.ds(j * columns, columns)])

    def mate_wait(r):
        net.wait(("m", r), h_all.at[r_rows(r), theirs])

    def project(row, j):
        place = span(row * four, four, four)
        cols = span(j * columns, columns, columns)
        value = dot(h_all[place, :], w_all[:, cols]).astype(BF16)
        factor = jnp.where(j == 1, scale, 1.0).astype(F32)
        p_all[place, cols] = (value.astype(F32) * factor).astype(BF16)

    def project_near(j):
        @pl.loop(0, 3)
        def _(t):
            project(turned(z, t + t // 2), j)

    def betas(b):
        for r in (-1, 1):
            h_wait(r, 1, b, "b")
            to_mate(r, 1, b, "b")

    def fars(part):
        for b in range(2):
            h_wait(2, 1, b, part)
            to_mate(2, 1, b, part)

    from_corner(0)
    betas(0)
    w_forward(0, away)
    from_corner(1)
    loads[4].wait()
    for dz, dx in diagonal[:EAGER]:
        c_send(dz, dx)
    betas(1)
    w_forward(1, away)
    w_forward(2, away)
    for r in (0, 1, -1):
        mate_wait(r)
    w_ready(0)
    project_near(0)
    from_far(0)
    from_far(1)
    for dz, dx in diagonal[EAGER:]:
        c_send(dz, dx)

    @pl.when(own)
    def _():
        c_all[span(s * rows, rows, rows), :] = c_in[:, span(s * columns, columns, columns)]

    w_ready(1)
    project_near(1)
    w_ready(2)
    project_near(2)
    fars("a")
    fars("b")
    mate_wait(2)
    @pl.loop(0, 3)
    def _(j):
        project(turned(z, 2), j)

    net.wait(("rate",), rates.at[1])
    for who, taken in ((own, blocks - 1), (away, blocks)):
        net.wait(("c",), c_all.at[pl.ds(0, taken * rows)], when=who)

    pick = jnp.where(own, 1.0, 0.0).astype(F32)
    g = rates[0] * pick + rates[1] * (1.0 - pick)
    g_row = g[0:1, :]
    gap = (
        lax.broadcasted_iota(jnp.int32, (BLOCK, BLOCK), 0) - lax.broadcasted_iota(jnp.int32, (BLOCK, BLOCK), 1)
    ).astype(F32)
    place = lax.broadcasted_iota(jnp.int32, (BLOCK, columns), 0).astype(F32)
    inner[...] = jnp.where(gap >= 0, jnp.exp(g_row * jnp.maximum(gap, 0.0)), 0.0)
    inner_t[...] = jnp.where(gap <= 0, jnp.exp(g_row * jnp.maximum(-gap, 0.0)), 0.0)
    decays[0] = jnp.exp(g_row * (place + 1.0))
    decays[1] = jnp.exp(g_row * (BLOCK - 1.0 - place))
    block_decay = jnp.exp(g_row * BLOCK)
    state[...] = jnp.zeros_like(state)
    back[...] = jnp.zeros_like(back)
    parts = [slice(j * columns, (j + 1) * columns) for j in range(3)]
    count = BLOCK // rows

    def slots(i):
        places = []
        for w in range(count):
            p = i * count + w
            pz, px = p // SIDE, p % SIDE
            b = (px // 2 - u) * (px // 2 - u)
            places.append(span((pz * SIDE + 2 * (px + b * (3 - 2 * px) - 2 * u) + b) * rows, rows, rows))
        return places

    def get(places, part):
        return jnp.concatenate([p_all[place, part] for place in places], axis=0)

    def put(places, part, grad):
        grad = grad.astype(BF16)
        for w, place in enumerate(places):
            g_all[place, part] = grad[w * rows : (w + 1) * rows]
        grad = grad.T
        for w, place in enumerate(places):
            g_turn[part, place] = grad[:, w * rows : (w + 1) * rows]

    def forward(i):
        places = slots(i)
        k, v = get(places, parts[1]), get(places, parts[2])
        ct = c_all[span(i * BLOCK, BLOCK, BLOCK), :]
        mixed = (dot(ct, v, NT) * inner[...]).astype(BF16)
        held = state[...]
        grad_q = dot(mixed, k) + dot(ct, held.astype(BF16), NT) * decays[0]
        weighted = (k.astype(F32) * decays[1]).astype(BF16)
        state[...] = held * block_decay + dot(weighted, v, TN)
        put(places, parts[0], grad_q)

    def backward(i):
        places = slots(i)
        q, k, v = (get(places, part) for part in parts)
        ct = c_all[span(i * BLOCK, BLOCK, BLOCK), :]
        mixed_t = (dot(v, ct, NT) * inner_t[...]).astype(BF16)
        scores_t = (dot(k, q, NT) * inner_t[...]).astype(BF16)
        held = back[...]
        held_bf = held.astype(BF16)
        grad_v = dot(scores_t, ct) + dot(k, held_bf) * decays[1]
        grad_k = (dot(mixed_t, q) + dot(v, held_bf, NT) * decays[1]) * scale
        weighted = (q.astype(F32) * decays[0]).astype(BF16)
        back[...] = held * block_decay + dot(weighted, ct, TN)
        put(places, parts[1], grad_k)
        put(places, parts[2], grad_v)

    steps = rows * blocks // BLOCK

    @pl.loop(0, steps // 2)
    def _(t):
        for w in range(2):
            forward(2 * t + w)
            backward(steps - 1 - 2 * t - w)

    pieces = tuple(pl.ds(first, size) for first, size in PIECES)
    beta = pl.ds(FIRST, half - FIRST)
    chunk = half // 2

    def pick_rows(r, hf):
        return span(turned(z, r) * four + hf * two, two, two)

    def other(r, i):
        cols = span(i * chunk, chunk, chunk)
        value = dot(g_all[r_rows(r), :], w_all[span((1 - c) * half + i * chunk, chunk, chunk), :], NT)
        pout[r_rows(r), cols] = value.astype(BF16)
        net.start(("p", r, i), pout.at[r_rows(r), cols], pin.at[r_rows(r), cols], mate)

    def summed(r, i):
        cols = span(i * chunk, chunk, chunk)
        net.wait(("p", r, i), pin.at[r_rows(r), cols])
        value = dot(g_all[r_rows(r), :], w_all[span(c * half + i * chunk, chunk, chunk), :], NT)
        psum[r_rows(r), cols] = (value + pin[r_rows(r), cols].astype(F32)).astype(BF16)
        if i == 1:
            net.start(("b0", r), psum.at[pick_rows(r, 1 - xl), beta], rb0.at[r % SIDE], pair)

    def add(place, cols, *refs):
        total = psum[place, cols].astype(F32)
        for ref in refs:
            total = total + ref.astype(F32)
        psum[place, cols] = total.astype(BF16)

    def a1(i, e):
        return ra1.at[e, :, pieces[i]]

    def a2(i, e, hf):
        return ra2.at[e, pl.ds(hf * two, two), pieces[i]]

    def a3(i):
        return ra3.at[:, pieces[i]]

    def alpha_send(i, r, hf, way, name, dst):
        net.start(name, psum.at[pick_rows(r, hf), pieces[i]], dst, zs[way])

    def alpha_first(i):
        alpha_send(i, 2, 0, 1, ("a1", i, 0), a1(i, 0))
        alpha_send(i, 2, 1, -1, ("a1", i, 1), a1(i, 1))

    def alpha_plain(i, r):
        e = 0 if r == 1 else 1
        alpha_send(i, r, 1 - e, r, ("a2", i), a2(i, e, 1 - e))

    def alpha_added(i):
        for e, r in ((0, 1), (1, -1)):
            net.wait(("a1", i, e), a1(i, e))
            add(pick_rows(r, e), pieces[i], a1(i, e)[...])
            alpha_send(i, r, e, r, ("a2", i), a2(i, e, e))

    def alpha_last(i):
        net.wait(("a2", i), ra2.at[:, :, pieces[i]])
        for hf in range(2):
            add(pick_rows(0, hf), pieces[i], a2(i, 0, hf)[...], a2(i, 1, hf)[...])
        net.start(("a3", i), psum.at[pick_rows(0, 1 - xl), pieces[i]], a3(i), pair)

    def deliver(cols):
        dst = dbuf.at[c, :, cols]
        net.start(("d",), psum.at[b_rows(0, 1), cols], dst, at(xx=cross, cc=u), offset=c, width=2)
        net.start(("d",), psum.at[b_rows(0, 0), cols], dst, mate, offset=c, width=2, when=away)

    def alpha_deliver(i):
        net.wait(("a3", i), a3(i))
        add(pick_rows(0, xl), pieces[i], a3(i)[...])
        deliver(pieces[i])

    def b_rows(r, b):
        return span(turned(z, r) * four + xl * two + b * rows, rows, rows)

    def b2(e, b):
        return rb2.at[e, pl.ds(b * rows, rows)]

    def beta_send(r, b, way, name, dst):
        net.start(name, psum.at[b_rows(r, b), beta], dst, zs[way])

    def beta_take(r):
        net.wait(("b0", r), rb0.at[r % SIDE])
        add(pick_rows(r, xl), beta, rb0[r % SIDE])

    def beta_first():
        beta_take(2)
        beta_send(2, 0, 1, ("b1", 0), rb1.at[0])
        beta_send(2, 1, -1, ("b1", 1), rb1.at[1])

    def beta_plain():
        for r, b, e in ((1, 1, 0), (-1, 0, 1)):
            beta_take(r)
            beta_send(r, b, r, ("b2",), b2(e, b))

    def beta_added():
        for r, b, e in ((1, 0, 0), (-1, 1, 1)):
            net.wait(("b1", e), rb1.at[e])
            add(b_rows(r, b), beta, rb1[e])
            beta_send(r, b, r, ("b2",), b2(e, b))

    def beta_last():
        beta_take(0)
        net.wait(("b2",), rb2)
        add(pick_rows(0, xl), beta, rb2[0], rb2[1])
        deliver(beta)

    lanes = [pl.ds(hf * depth, depth) for hf in range(2)]

    def w_grad(r, j):
        cols = span(turned(y, r) * 2 * depth, 2 * depth, depth)
        return dot(g_turn[parts[j], :], h_all[:, cols])

    def y_first(j):
        ysend[j] = w_grad(2, j).astype(BF16)
        for e, way in ((0, 1), (1, -1)):
            net.start(("y1", j, e), ysend.at[j, :, lanes[e]], yr1.at[j, e], ys[way])

    def y2(j, e, hf):
        return yr2.at[j, e, :, lanes[hf]]

    def y_second(j):
        for e, r in ((0, 1), (1, -1)):
            value = w_grad(r, j)
            keep = value[:, e * depth : (e + 1) * depth]
            yone[j, e, :, lanes[1 - e]] = value[:, (1 - e) * depth : (2 - e) * depth].astype(BF16)
            net.start(("y2", j), yone.at[j, e, :, lanes[1 - e]], y2(j, e, 1 - e), ys[r])
            net.wait(("y1", j, e), yr1.at[j, e])
            yone[j, e, :, lanes[e]] = (keep + yr1[j, e].astype(F32)).astype(BF16)
            net.start(("y2", j), yone.at[j, e, :, lanes[e]], y2(j, e, e), ys[r])

    def y_home(j):
        yhome[j] = w_grad(0, j)

    def y_last(j):
        net.wait(("y2", j), yr2.at[j])
        total = yhome[j] + yr2[j, 0].astype(F32) + yr2[j, 1].astype(F32)
        yhome[j] = total
        yout[j] = total.astype(BF16)
        half_of = span((1 - c) * depth, depth, depth)
        net.start(("e", 0), yout.at[j, :, half_of], yend.at[j, 0], mate, when=own)
        for hf in range(2):
            net.start(("e", 1), yout.at[j, :, lanes[hf]], yend.at[j, 1], at(xx=cross, cc=hf), when=away)

    y_first(0)
    other(2, 1)
    other(2, 0)
    y_first(1)
    summed(2, 1)
    alpha_first(0)
    summed(2, 0)
    alpha_first(1)
    alpha_first(2)
    y_first(2)
    other(1, 1)
    other(-1, 1)
    other(1, 0)
    other(-1, 0)
    y_second(0)
    summed(1, 1)
    alpha_plain(0, 1)
    summed(-1, 1)
    alpha_plain(0, -1)
    summed(1, 0)
    alpha_plain(1, 1)
    summed(-1, 0)
    alpha_plain(1, -1)
    beta_first()
    alpha_added(0)
    y_second(1)
    other(0, 1)
    other(0, 0)
    alpha_added(1)
    alpha_plain(2, 1)
    alpha_plain(2, -1)
    alpha_added(2)
    y_second(2)
    summed(0, 1)
    summed(0, 0)
    y_home(0)
    y_last(0)
    y_home(1)
    y_home(2)
    beta_plain()
    alpha_last(0)
    y_last(1)
    alpha_last(1)
    beta_added()
    alpha_deliver(0)
    alpha_last(2)
    alpha_deliver(1)
    y_last(2)
    beta_last()
    alpha_deliver(2)

    net.wait(("e", 1), yend.at[:, 1])
    net.wait(("e", 0), yend.at[:, 0], when=away)

    @pl.when(own)
    def _():
        here = span(c * depth, depth, depth)
        for j, out in enumerate((dq, dk, dv)):
            out[...] = (yhome[j, :, here] + yend[j, 1].astype(F32)).T * 0.125

    @pl.when(away)
    def _():
        for j, out in enumerate((dq, dk, dv)):
            out[...] = (yend[j, 0].astype(F32) + yend[j, 1].astype(F32)).T * 0.125

    for hf in range(2):
        net.wait(("d",), dbuf.at[hf], offset=hf, width=2, when=jnp.logical_or(away, c != hf))

    @pl.when(own)
    def _():
        dbuf[c] = psum[b_rows(0, 0), :]

    for hf in range(2):
        dh[:, hf * half : (hf + 1) * half] = dbuf[hf]
    net.drain()
    assert len(net.groups) <= SENDS and net.total <= RECVS, (len(net.groups), net.total)


def whole(rate, h, c, wq, wk, wv):
    rows, width = h.shape
    depth, columns = wq.shape
    blocks = SIDE * SIDE
    length = rows * blocks
    half = width // 2
    rest = half - FIRST
    vmem = pl.BlockSpec(memory_space=pltpu.VMEM)
    dma = pltpu.SemaphoreType.DMA

    def buf(*shape, kind=BF16):
        return pltpu.VMEM(shape, kind)

    return pl.pallas_call(
        whole_kernel,
        out_shape=(buf(rows, width),) + (buf(depth, columns, kind=F32),) * 3,
        in_specs=[pl.BlockSpec(memory_space=pltpu.SMEM)] + [pl.BlockSpec(memory_space=pl.ANY)] * 5,
        out_specs=(vmem,) * 4,
        scratch_shapes=[
            buf(length, width),
            buf(length, columns),
            buf(depth * 8, 3 * columns),
            buf(length, 3 * columns),
            buf(length, 3 * columns),
            buf(3 * columns, length),
            buf(columns, columns, kind=F32),
            buf(columns, columns, kind=F32),
            buf(2, 8, columns, kind=F32),
            buf(BLOCK, BLOCK, kind=F32),
            buf(BLOCK, BLOCK, kind=F32),
            buf(2, BLOCK, columns, kind=F32),
            buf(length, half),
            buf(length, half),
            buf(length, half),
            buf(2, 2 * rows, FIRST),
            buf(2, 4 * rows, FIRST),
            buf(2 * rows, FIRST),
            buf(SIDE, 2 * rows, rest),
            buf(2, rows, rest),
            buf(2, 2 * rows, rest),
            buf(2, rows, half),
            buf(3, columns, 2 * depth),
            buf(3, 2, columns, 2 * depth),
            buf(3, columns, 2 * depth, kind=F32),
            buf(3, 2, columns, depth),
            buf(3, 2, columns, 2 * depth),
            buf(3, columns, 2 * depth),
            buf(3, 2, columns, depth),
            buf(rows, width),
            buf(rows, columns * blocks),
            buf(3, depth, columns),
            dma((5,)),
            dma((SENDS,)),
            dma((RECVS,)),
        ],
        compiler_params=pltpu.CompilerParams(
            collective_id=0, has_side_effects=True, vmem_limit_bytes=VMEM_LIMIT
        ),
        name="whole",
    )(rate, h, c, wq, wk, wv)


def finish_kernel(count, *refs):
    ins, outs, sems = refs[:count], refs[count : 2 * count], refs[2 * count]
    moves = [pltpu.make_async_copy(ins[i], outs[i], sems.at[i]) for i in range(count)]
    for move in moves:
        move.start()
    for move in moves:
        move.wait()


def finish(*arrays):
    count = len(arrays)
    return pl.pallas_call(
        functools.partial(finish_kernel, count),
        out_shape=tuple(jax.ShapeDtypeStruct(a.shape, a.dtype) for a in arrays),
        in_specs=[pl.BlockSpec(memory_space=pltpu.VMEM)] * count,
        out_specs=(pl.BlockSpec(memory_space=pl.ANY),) * count,
        scratch_shapes=[pltpu.SemaphoreType.DMA((count,))],
        compiler_params=pltpu.CompilerParams(vmem_limit_bytes=4 * 1024 * 1024),
        name="finish",
    )(*arrays)


def body(hidden_in, mix_cotangent, query_weight, key_weight, value_weight, decay_log):
    dh, dq, dk, dv = finish(
        *whole(decay_log, hidden_in[0], mix_cotangent[0], query_weight, key_weight, value_weight)
    )
    return dh[None], dq, dk, dv


def solution(mesh):
    placed = (
        P("dp", "sp", None),
        P("dp", "sp", None),
        P("dp", "sp"),
        P("dp", "sp"),
        P("dp", "sp"),
        P("sp"),
    )
    return jax.shard_map(
        body,
        mesh=mesh,
        in_specs=placed,
        out_specs=(P("dp", "sp", None), P("dp", "sp"), P("dp", "sp"), P("dp", "sp")),
        check_vma=False,
    )
```

```python
import functools

import jax
import jax.numpy as jnp
from jax import lax
from jax.experimental import pallas as pl
from jax.experimental.pallas import tpu as pltpu
from jax.sharding import PartitionSpec as P

BLOCK = 256
SIDE = 4
FIRST = 640
BACK = 512
PIECES = ((0, 256), (256, 256))
EAGER = 12
DEEP = 4
F32 = jnp.float32
BF16 = jnp.bfloat16
MESH = pl.DeviceIdType.MESH
NN = (((1,), (0,)), ((), ()))
NT = (((1,), (1,)), ((), ()))
TN = (((0,), (0,)), ((), ()))
VMEM_LIMIT = 60 * 1024 * 1024
GROUP = 4 * 1024 * 1024
CELL = 32 * 1024
SENDS = 9
RECVS = 79


def dot(a, b, dims=NN):
    return lax.dot_general(a, b, dims, preferred_element_type=F32)


def span(start, size, step):
    return pl.ds(pl.multiple_of(start, step), size)


class Net:
    def __init__(self, send, recv, meter, small, somewhere):
        self.send, self.recv, self.somewhere = send, recv, somewhere
        self.meter, self.small = meter, small
        self.names, self.total, self.groups, self.open = {}, 0, [], {}

    def index(self, name, width=1):
        if name not in self.names:
            self.names[name] = self.total
            self.total += width
        return self.names[name]

    def lane(self, kind, when, size):
        group = self.open.get(kind)
        if group is None or self.groups[group][1] + size > GROUP:
            self.open[kind] = group = len(self.groups)
            self.groups.append([when, 0])
        self.groups[group][1] += size
        return group

    def copy(self, src, dst, lane, slot, where):
        return pltpu.make_async_remote_copy(
            src_ref=src, dst_ref=dst, send_sem=self.send.at[lane], recv_sem=self.recv.at[slot],
            device_id=where, device_id_type=MESH,
        )

    def start(self, name, src, dst, where, offset=0, width=1, when=None):
        slot = self.index(name, width) + offset
        size = 2 if src.dtype == BF16 else 4
        for extent in src.shape:
            size *= extent
        lane = self.lane(id(when) if size % CELL == 0 else name, when, size)
        if when is None:
            self.copy(src, dst, lane, slot, where).start()
        else:
            pl.when(when)(lambda: self.copy(src, dst, lane, slot, where).start())

    def wait(self, name, dst, offset=0, width=1, when=None):
        slot = self.index(name, width) + offset
        if when is None:
            self.copy(dst, dst, 0, slot, self.somewhere).wait_recv()
        else:
            pl.when(when)(lambda: self.copy(dst, dst, 0, slot, self.somewhere).wait_recv())

    def drain(self):
        for lane, (when, size) in enumerate(self.groups):
            ref = self.meter.at[pl.ds(0, size // (2 * self.meter.shape[1]))] if size % CELL == 0 else self.small

            def run():
                self.copy(ref, ref, lane, 0, self.somewhere).wait_send()

            if when is None:
                run()
            else:
                pl.when(when)(run)


def whole_kernel(
    rate, h_far, c_far, wq, wk, wv, dh, dq, dk, dv,
    h_all, c_all, w_all, w_turn, p_all, g_all, g_turn, state, back, rates, inner, inner_t, decays,
    pout, pin, psum, ra1, ra2, ra3, rb0, rb1, rb2, dbuf,
    ysend, yone, yhome, yr1, yr2, yout, yend, h_in, c_in, w_in, local, send, recv,
):
    s = lax.axis_index("sp")
    d = lax.axis_index("dp")
    z, x = s // SIDE, s % SIDE
    y, c = d // 2, d % 2
    u = x // 2
    xl = x - 2 * u
    own = c == u
    away = c != u
    rows, width = h_in.shape
    depth, columns = wq.shape
    half = width // 2
    four = rows * SIDE
    two = rows * 2
    blocks = SIDE * SIDE
    scale = columns ** (-0.5)

    def at(zz=None, xx=None, yy=None, cc=None):
        zz, xx = z if zz is None else zz, x if xx is None else xx
        yy, cc = y if yy is None else yy, c if cc is None else cc
        return {"sp": zz * SIDE + xx, "dp": yy * 2 + cc}

    def turned(v, by):
        return (v + by + SIDE) % SIDE

    mate = at(cc=1 - c)
    pair = at(xx=x + 1 - 2 * xl)
    zs = {1: at(zz=turned(z, 1)), -1: at(zz=turned(z, -1))}
    ys = {1: at(yy=turned(y, 1)), -1: at(yy=turned(y, -1))}
    cross = 3 - x
    net = Net(send, recv, h_all, rates.at[0], mate)
    weights = [w_in.at[j] for j in range(3)]
    loads = [
        pltpu.make_async_copy(src, dst, local.at[i])
        for i, (src, dst) in enumerate(zip((h_far, wq, wk, wv, c_far), [h_in] + weights + [c_in]))
    ]
    for load in loads:
        load.start()

    barrier = pltpu.get_barrier_semaphore()
    peers = [mate, ys[1], ys[-1]]
    for k in range(1, blocks):
        other = (s + k) % blocks
        peers += [{"sp": other, "dp": d}, {"sp": other, "dp": y * 2 + 1 - c}]
    for where in peers:
        pl.semaphore_signal(barrier, inc=1, device_id=where, device_id_type=MESH)
    rates[0] = jnp.full(rates.shape[1:], rate[0], F32)
    loads[0].wait()
    pl.semaphore_wait(barrier, len(peers))

    def r_rows(r):
        return span(turned(z, r) * four, four, four)

    def slot(r, col, b):
        return turned(z, r) * SIDE + 2 * (xl if col == 0 else 1 - xl) + b

    def h_ref(place, part, which):
        base = which * half
        lo, size = {"f": (0, half), "a": (0, FIRST), "b": (FIRST, half - FIRST)}[part]
        return h_all.at[span(place * rows, rows, rows), span(base + lo, size, 128)]

    def h_send(r, col, b, part, where, name):
        ref = h_ref(slot(r, col, b), part, c)
        net.start(name, ref, ref, where)

    def to_mate(r, col, b, part):
        h_send(r, col, b, part, mate, ("m", r))

    def h_wait(r, col, b, part, when=None):
        net.wait(("x", r, col, b, part), h_ref(slot(r, col, b), part, c), when=when)

    def w_ref(yy, cc, j):
        return w_all.at[span((yy * 2 + cc) * depth, depth, depth), pl.ds(j * columns, columns)]

    def w_near(j):
        net.start(("w0", j), weights[j], w_ref(y, c, j), mate, offset=c, width=2, when=away)

    def w_cross(j, who):
        net.start(("w0", j), weights[j], w_ref(y, c, j), at(xx=cross, cc=u), offset=c, width=2, when=who)

    mine = span(c * half, half, half)
    theirs = span((1 - c) * half, half, half)
    net.start(("x", 0, 0, 0, "f"), h_in.at[:, theirs], h_ref(slot(0, 0, 0), "f", 1 - c), mate, when=own)
    there = z * SIDE + 2 * (1 - xl) + 1
    for hf in range(2):
        net.start(
            ("x", 0, 0, 1, "f"), h_in.at[:, pl.ds(hf * half, half)], h_ref(there, "f", hf),
            at(xx=cross, cc=hf), when=away,
        )
    for load in loads[1:4]:
        load.wait()
    for j in range(3):
        w_near(j)
    for j in range(3):
        w_cross(j, away)
    net.start(("rate",), rates.at[0], rates.at[1], at(xx=cross))

    @pl.when(own)
    def _():
        h_all[span(slot(0, 0, 0) * rows, rows, rows), mine] = h_in[:, mine]
        for j in range(3):
            w_all[span(d * depth, depth, depth), j * columns : (j + 1) * columns] = weights[j][...]

    def spread(b):
        for way in (1, -1):
            h_send(0, 0, b, "f", zs[way], ("x", -way, 0, b, "f"))
        h_send(0, 0, b, "f", pair, ("x", 0, 1, b, "f"))
        to_mate(0, 0, b, "f")

    def w_spread(j, who):
        for cc in range(2):
            far = who if who is away else jnp.logical_and(own, c != cc)
            net.wait(("w0", j), w_ref(y, cc, j), offset=cc, width=2, when=far)
            for way in (1, -1):
                name = ("w1", j, -way) if (way == 1) == (cc == 0) else ("wt", j)
                net.start(name, w_ref(y, cc, j), w_ref(y, cc, j), ys[way], when=who)

    def w_forward(j, who):
        for way, cc in ((1, 0), (-1, 1)):
            ref = w_ref(turned(y, -way), cc, j)
            net.wait(("w1", j, -way), ref, when=who)
            net.start(("wt", j), ref, ref, ys[way], when=who)

    def from_pair(b):
        h_wait(0, 1, b, "f")
        for way in (1, -1):
            h_send(0, 1, b, "a", zs[way], ("x", -way, 1, b, "a"))
        to_mate(0, 1, b, "f")

    def from_side(b):
        for r in (-1, 1):
            h_wait(r, 0, b, "f")
            h_send(r, 0, b, "b", pair, ("x", r, 1, b, "b"))
            to_mate(r, 0, b, "f")

    def side_forward(b):
        fast = 1 if b == 0 else -1
        h_send(-fast, 0, b, "f", zs[fast], ("x", 2, 0, b, "f"))

    def from_corner(b):
        fast = 1 if b == 0 else -1
        for r in (-fast, fast):
            h_wait(r, 1, b, "a")
            if r == -fast:
                h_send(r, 1, b, "a", zs[fast], ("x", 2, 1, b, "a"))
            to_mate(r, 1, b, "a")

    def from_far(b):
        h_wait(2, 0, b, "f")
        h_send(2, 0, b, "b", pair, ("x", 2, 1, b, "b"))
        to_mate(2, 0, b, "f")

    def c_send(dz, dx):
        hz, hx = turned(z, dz), turned(x, dx)
        head = hz * SIDE + hx
        far = (hx // 2 - c) * (hx // 2 - c)
        net.start(
            ("c",), c_in.at[:, span(head * columns, columns, columns)],
            c_all.at[span(s * rows, rows, rows)],
            {"sp": hz * SIDE + hx + far * (3 - 2 * hx), "dp": y * 2 + c + far * (1 - 2 * c)},
            when=away if (dz, dx) == (0, 0) else None,
        )

    diagonal = [(dz, (dz + k) % SIDE) for k in range(SIDE) for dz in (2, 1, 3, 0)]

    h_wait(0, 0, 0, "f", when=away)
    spread(0)
    for j in range(3):
        w_spread(j, own)
    h_wait(0, 0, 1, "f")
    spread(1)
    for j in range(3):
        w_cross(j, own)
    from_side(0)
    from_pair(0)
    w_forward(0, own)
    w_spread(0, away)
    from_side(1)
    from_pair(1)
    side_forward(0)
    side_forward(1)
    w_forward(1, own)
    w_spread(1, away)
    w_forward(2, own)
    w_spread(2, away)

    def w_ready(j):
        net.wait(("wt", j), w_all.at[pl.ds(0, 4 * depth), pl.ds(j * columns, columns)])

    def mate_wait(r):
        net.wait(("m", r), h_all.at[r_rows(r), theirs])

    def project(row, j):
        place = span(row * four, four, four)
        cols = span(j * columns, columns, columns)
        value = dot(h_all[place, :], w_all[:, cols]).astype(BF16)
        factor = jnp.where(j == 1, scale, 1.0).astype(F32)
        p_all[place, cols] = (value.astype(F32) * factor).astype(BF16)

    def turn_weight(j):
        @pl.loop(0, SIDE)
        def _(t):
            place = span(t * 2 * depth, 2 * depth, 2 * depth)
            w_turn[pl.ds(j * columns, columns), place] = w_all[place, pl.ds(j * columns, columns)].T

    def project_near(j):
        @pl.loop(0, 3)
        def _(t):
            project(turned(z, t + t // 2), j)

    def betas(b):
        for r in (-1, 1):
            h_wait(r, 1, b, "b")
            to_mate(r, 1, b, "b")

    def fars(part):
        for b in range(2):
            h_wait(2, 1, b, part)
            to_mate(2, 1, b, part)

    from_corner(0)
    betas(0)
    w_forward(0, away)
    from_corner(1)
    loads[4].wait()
    for dz, dx in diagonal[:EAGER]:
        c_send(dz, dx)
    betas(1)
    w_forward(1, away)
    w_forward(2, away)
    for r in (0, 1, -1):
        mate_wait(r)
    w_ready(0)
    project_near(0)
    turn_weight(0)
    from_far(0)
    from_far(1)
    for dz, dx in diagonal[EAGER:]:
        c_send(dz, dx)

    @pl.when(own)
    def _():
        c_all[span(s * rows, rows, rows), :] = c_in[:, span(s * columns, columns, columns)]

    w_ready(1)
    project_near(1)
    w_ready(2)
    project_near(2)
    fars("a")
    fars("b")
    turn_weight(1)
    turn_weight(2)
    mate_wait(2)
    @pl.loop(0, 3)
    def _(j):
        project(turned(z, 2), j)

    net.wait(("rate",), rates.at[1])
    for who, taken in ((own, blocks - 1), (away, blocks)):
        net.wait(("c",), c_all.at[pl.ds(0, taken * rows)], when=who)

    pick = jnp.where(own, 1.0, 0.0).astype(F32)
    g = rates[0] * pick + rates[1] * (1.0 - pick)
    g_row = g[0:1, :]
    gap = (
        lax.broadcasted_iota(jnp.int32, (BLOCK, BLOCK), 0) - lax.broadcasted_iota(jnp.int32, (BLOCK, BLOCK), 1)
    ).astype(F32)
    place = lax.broadcasted_iota(jnp.int32, (BLOCK, columns), 0).astype(F32)
    inner[...] = jnp.where(gap >= 0, jnp.exp(g_row * jnp.maximum(gap, 0.0)), 0.0)
    inner_t[...] = jnp.where(gap <= 0, jnp.exp(g_row * jnp.maximum(-gap, 0.0)), 0.0)
    decays[0] = jnp.exp(g_row * (place + 1.0))
    decays[1] = jnp.exp(g_row * (BLOCK - 1.0 - place))
    block_decay = jnp.exp(g_row * BLOCK)
    state[...] = jnp.zeros_like(state)
    back[...] = jnp.zeros_like(back)
    parts = [slice(j * columns, (j + 1) * columns) for j in range(3)]
    count = BLOCK // rows

    def slots(i):
        places = []
        for w in range(count):
            p = i * count + w
            pz, px = p // SIDE, p % SIDE
            b = (px // 2 - u) * (px // 2 - u)
            places.append(span((pz * SIDE + 2 * (px + b * (3 - 2 * px) - 2 * u) + b) * rows, rows, rows))
        return places

    def get(places, part):
        return jnp.concatenate([p_all[place, part] for place in places], axis=0)

    def put(places, part, grad):
        grad = grad.astype(BF16)
        for w, place in enumerate(places):
            g_all[place, part] = grad[w * rows : (w + 1) * rows]
        grad = grad.T
        for w, place in enumerate(places):
            g_turn[part, place] = grad[:, w * rows : (w + 1) * rows]

    def forward(i):
        places = slots(i)
        k, v = get(places, parts[1]), get(places, parts[2])
        ct = c_all[span(i * BLOCK, BLOCK, BLOCK), :]
        mixed = (dot(ct, v, NT) * inner[...]).astype(BF16)
        held = state[...]
        grad_q = dot(mixed, k) + dot(ct, held.astype(BF16), NT) * decays[0]
        weighted = (k.astype(F32) * decays[1]).astype(BF16)
        state[...] = held * block_decay + dot(weighted, v, TN)
        put(places, parts[0], grad_q)

    def backward(i):
        places = slots(i)
        q, k, v = (get(places, part) for part in parts)
        ct = c_all[span(i * BLOCK, BLOCK, BLOCK), :]
        mixed_t = (dot(v, ct, NT) * inner_t[...]).astype(BF16)
        scores_t = (dot(k, q, NT) * inner_t[...]).astype(BF16)
        held = back[...]
        held_bf = held.astype(BF16)
        grad_v = dot(scores_t, ct) + dot(k, held_bf) * decays[1]
        grad_k = (dot(mixed_t, q) + dot(v, held_bf, NT) * decays[1]) * scale
        weighted = (q.astype(F32) * decays[0]).astype(BF16)
        back[...] = held * block_decay + dot(weighted, ct, TN)
        put(places, parts[1], grad_k)
        put(places, parts[2], grad_v)

    steps = rows * blocks // BLOCK

    @pl.loop(0, steps // DEEP)
    def _(t):
        for w in range(DEEP):
            forward(DEEP * t + w)
            backward(steps - 1 - DEEP * t - w)

    pieces = tuple(pl.ds(first, size) for first, size in PIECES)
    beta = pl.ds(BACK, half - BACK)
    chunk = half // 2

    def pick_rows(r, hf):
        return span(turned(z, r) * four + hf * two, two, two)

    def other(r, i):
        cols = span(i * chunk, chunk, chunk)
        value = dot(g_all[r_rows(r), :], w_turn[:, span((1 - c) * half + i * chunk, chunk, chunk)])
        pout[r_rows(r), cols] = value.astype(BF16)
        net.start(("p", r, i), pout.at[r_rows(r), cols], pin.at[r_rows(r), cols], mate)

    def summed(r, i):
        cols = span(i * chunk, chunk, chunk)
        net.wait(("p", r, i), pin.at[r_rows(r), cols])
        value = dot(g_all[r_rows(r), :], w_turn[:, span(c * half + i * chunk, chunk, chunk)])
        psum[r_rows(r), cols] = (value + pin[r_rows(r), cols].astype(F32)).astype(BF16)
        if i == 1:
            net.start(("b0", r), psum.at[pick_rows(r, 1 - xl), beta], rb0.at[r % SIDE], pair)

    def add(place, cols, *refs):
        total = psum[place, cols].astype(F32)
        for ref in refs:
            total = total + ref.astype(F32)
        psum[place, cols] = total.astype(BF16)

    def a1(i, e):
        return ra1.at[e, :, pieces[i]]

    def a2(i, e, hf):
        return ra2.at[e, pl.ds(hf * two, two), pieces[i]]

    def a3(i):
        return ra3.at[:, pieces[i]]

    def alpha_send(i, r, hf, way, name, dst):
        net.start(name, psum.at[pick_rows(r, hf), pieces[i]], dst, zs[way])

    def alpha_first(i):
        alpha_send(i, 2, 0, 1, ("a1", i, 0), a1(i, 0))
        alpha_send(i, 2, 1, -1, ("a1", i, 1), a1(i, 1))

    def alpha_plain(i, r):
        e = 0 if r == 1 else 1
        alpha_send(i, r, 1 - e, r, ("a2", i), a2(i, e, 1 - e))

    def alpha_added(i):
        for e, r in ((0, 1), (1, -1)):
            net.wait(("a1", i, e), a1(i, e))
            add(pick_rows(r, e), pieces[i], a1(i, e)[...])
            alpha_send(i, r, e, r, ("a2", i), a2(i, e, e))

    def alpha_last(i):
        net.wait(("a2", i), ra2.at[:, :, pieces[i]])
        for hf in range(2):
            add(pick_rows(0, hf), pieces[i], a2(i, 0, hf)[...], a2(i, 1, hf)[...])
        net.start(("a3", i), psum.at[pick_rows(0, 1 - xl), pieces[i]], a3(i), pair)

    def deliver(cols):
        dst = dbuf.at[c, :, cols]
        net.start(("d",), psum.at[b_rows(0, 1), cols], dst, at(xx=cross, cc=u), offset=c, width=2)
        net.start(("d",), psum.at[b_rows(0, 0), cols], dst, mate, offset=c, width=2, when=away)

    def alpha_deliver(i):
        net.wait(("a3", i), a3(i))
        add(pick_rows(0, xl), pieces[i], a3(i)[...])
        deliver(pieces[i])

    def b_rows(r, b):
        return span(turned(z, r) * four + xl * two + b * rows, rows, rows)

    def b2(e, b):
        return rb2.at[e, pl.ds(b * rows, rows)]

    def beta_send(r, b, way, name, dst):
        net.start(name, psum.at[b_rows(r, b), beta], dst, zs[way])

    def beta_take(r):
        net.wait(("b0", r), rb0.at[r % SIDE])
        add(pick_rows(r, xl), beta, rb0[r % SIDE])

    def beta_first():
        beta_take(2)
        beta_send(2, 0, 1, ("b1", 0), rb1.at[0])
        beta_send(2, 1, -1, ("b1", 1), rb1.at[1])

    def beta_plain():
        for r, b, e in ((1, 1, 0), (-1, 0, 1)):
            beta_take(r)
            beta_send(r, b, r, ("b2",), b2(e, b))

    def beta_added():
        for r, b, e in ((1, 0, 0), (-1, 1, 1)):
            net.wait(("b1", e), rb1.at[e])
            add(b_rows(r, b), beta, rb1[e])
            beta_send(r, b, r, ("b2",), b2(e, b))

    def beta_last():
        beta_take(0)
        net.wait(("b2",), rb2)
        add(pick_rows(0, xl), beta, rb2[0], rb2[1])
        deliver(beta)

    lanes = [pl.ds(hf * depth, depth) for hf in range(2)]

    def w_grad(r, j):
        cols = span(turned(y, r) * 2 * depth, 2 * depth, depth)
        return dot(g_turn[parts[j], :], h_all[:, cols])

    def y_first(j):
        ysend[j] = w_grad(2, j).astype(BF16)
        for e, way in ((0, 1), (1, -1)):
            net.start(("y1", j, e), ysend.at[j, :, lanes[e]], yr1.at[j, e], ys[way])

    def y2(j, e, hf):
        return yr2.at[j, e, :, lanes[hf]]

    def y_second(j):
        for e, r in ((0, 1), (1, -1)):
            value = w_grad(r, j)
            keep = value[:, e * depth : (e + 1) * depth]
            yone[j, e, :, lanes[1 - e]] = value[:, (1 - e) * depth : (2 - e) * depth].astype(BF16)
            net.start(("y2", j), yone.at[j, e, :, lanes[1 - e]], y2(j, e, 1 - e), ys[r])
            net.wait(("y1", j, e), yr1.at[j, e])
            yone[j, e, :, lanes[e]] = (keep + yr1[j, e].astype(F32)).astype(BF16)
            net.start(("y2", j), yone.at[j, e, :, lanes[e]], y2(j, e, e), ys[r])

    def y_home(j):
        yhome[j] = w_grad(0, j)

    def y_last(j):
        net.wait(("y2", j), yr2.at[j])
        total = yhome[j] + yr2[j, 0].astype(F32) + yr2[j, 1].astype(F32)
        yhome[j] = total
        yout[j] = total.astype(BF16)
        half_of = span((1 - c) * depth, depth, depth)
        net.start(("e", 0), yout.at[j, :, half_of], yend.at[j, 0], mate, when=own)
        for hf in range(2):
            net.start(("e", 1), yout.at[j, :, lanes[hf]], yend.at[j, 1], at(xx=cross, cc=hf), when=away)

    y_first(0)
    other(2, 0)
    other(2, 1)
    y_first(1)
    summed(2, 0)
    alpha_first(0)
    alpha_first(1)
    summed(2, 1)
    y_first(2)
    other(1, 0)
    other(-1, 0)
    other(1, 1)
    other(-1, 1)
    summed(1, 0)
    alpha_plain(0, 1)
    summed(-1, 0)
    alpha_plain(0, -1)
    y_second(0)
    summed(1, 1)
    summed(-1, 1)
    beta_first()
    alpha_added(0)
    alpha_plain(1, 1)
    alpha_plain(1, -1)
    y_second(1)
    other(0, 0)
    other(0, 1)
    alpha_added(1)
    y_second(2)
    summed(0, 0)
    y_home(0)
    y_last(0)
    alpha_last(0)
    summed(0, 1)
    y_home(1)
    y_home(2)
    y_last(1)
    beta_plain()
    beta_added()
    alpha_last(1)
    alpha_deliver(0)
    y_last(2)
    beta_last()
    alpha_deliver(1)

    net.wait(("e", 1), yend.at[:, 1])
    net.wait(("e", 0), yend.at[:, 0], when=away)

    @pl.when(own)
    def _():
        here = span(c * depth, depth, depth)
        for j, out in enumerate((dq, dk, dv)):
            out[...] = (yhome[j, :, here] + yend[j, 1].astype(F32)).T * 0.125

    @pl.when(away)
    def _():
        for j, out in enumerate((dq, dk, dv)):
            out[...] = (yend[j, 0].astype(F32) + yend[j, 1].astype(F32)).T * 0.125

    for hf in range(2):
        net.wait(("d",), dbuf.at[hf], offset=hf, width=2, when=jnp.logical_or(away, c != hf))

    @pl.when(own)
    def _():
        dbuf[c] = psum[b_rows(0, 0), :]

    for hf in range(2):
        dh[:, hf * half : (hf + 1) * half] = dbuf[hf]
    net.drain()
    assert len(net.groups) <= SENDS and net.total <= RECVS, (len(net.groups), net.total)


def whole(rate, h, c, wq, wk, wv):
    rows, width = h.shape
    depth, columns = wq.shape
    blocks = SIDE * SIDE
    length = rows * blocks
    half = width // 2
    rest = half - BACK
    vmem = pl.BlockSpec(memory_space=pltpu.VMEM)
    dma = pltpu.SemaphoreType.DMA

    def buf(*shape, kind=BF16):
        return pltpu.VMEM(shape, kind)

    return pl.pallas_call(
        whole_kernel,
        out_shape=(buf(rows, width),) + (buf(depth, columns, kind=F32),) * 3,
        in_specs=[pl.BlockSpec(memory_space=pltpu.SMEM)] + [pl.BlockSpec(memory_space=pl.ANY)] * 5,
        out_specs=(vmem,) * 4,
        scratch_shapes=[
            buf(length, width),
            buf(length, columns),
            buf(depth * 8, 3 * columns),
            buf(3 * columns, depth * 8),
            buf(length, 3 * columns),
            buf(length, 3 * columns),
            buf(3 * columns, length),
            buf(columns, columns, kind=F32),
            buf(columns, columns, kind=F32),
            buf(2, 8, columns, kind=F32),
            buf(BLOCK, BLOCK, kind=F32),
            buf(BLOCK, BLOCK, kind=F32),
            buf(2, BLOCK, columns, kind=F32),
            buf(length, half),
            buf(length, half),
            buf(length, half),
            buf(2, 2 * rows, BACK),
            buf(2, 4 * rows, BACK),
            buf(2 * rows, BACK),
            buf(SIDE, 2 * rows, rest),
            buf(2, rows, rest),
            buf(2, 2 * rows, rest),
            buf(2, rows, half),
            buf(3, columns, 2 * depth),
            buf(3, 2, columns, 2 * depth),
            buf(3, columns, 2 * depth, kind=F32),
            buf(3, 2, columns, depth),
            buf(3, 2, columns, 2 * depth),
            buf(3, columns, 2 * depth),
            buf(3, 2, columns, depth),
            buf(rows, width),
            buf(rows, columns * blocks),
            buf(3, depth, columns),
            dma((5,)),
            dma((SENDS,)),
            dma((RECVS,)),
        ],
        compiler_params=pltpu.CompilerParams(
            collective_id=0, has_side_effects=True, vmem_limit_bytes=VMEM_LIMIT
        ),
        name="whole",
    )(rate, h, c, wq, wk, wv)


def finish_kernel(count, *refs):
    ins, outs, sems = refs[:count], refs[count : 2 * count], refs[2 * count]
    moves = [pltpu.make_async_copy(ins[i], outs[i], sems.at[i]) for i in range(count)]
    for move in moves:
        move.start()
    for move in moves:
        move.wait()


def finish(*arrays):
    count = len(arrays)
    return pl.pallas_call(
        functools.partial(finish_kernel, count),
        out_shape=tuple(jax.ShapeDtypeStruct(a.shape, a.dtype) for a in arrays),
        in_specs=[pl.BlockSpec(memory_space=pltpu.VMEM)] * count,
        out_specs=(pl.BlockSpec(memory_space=pl.ANY),) * count,
        scratch_shapes=[pltpu.SemaphoreType.DMA((count,))],
        compiler_params=pltpu.CompilerParams(vmem_limit_bytes=4 * 1024 * 1024),
        name="finish",
    )(*arrays)


def body(hidden_in, mix_cotangent, query_weight, key_weight, value_weight, decay_log):
    dh, dq, dk, dv = finish(
        *whole(decay_log, hidden_in[0], mix_cotangent[0], query_weight, key_weight, value_weight)
    )
    return dh[None], dq, dk, dv


def solution(mesh):
    placed = (
        P("dp", "sp", None),
        P("dp", "sp", None),
        P("dp", "sp"),
        P("dp", "sp"),
        P("dp", "sp"),
        P("sp"),
    )
    return jax.shard_map(
        body,
        mesh=mesh,
        in_specs=placed,
        out_specs=(P("dp", "sp", None), P("dp", "sp"), P("dp", "sp"), P("dp", "sp")),
        check_vma=False,
    )
```

```python
import functools

import jax
import jax.numpy as jnp
from jax import lax
from jax.experimental import pallas as pl
from jax.experimental.pallas import tpu as pltpu
from jax.sharding import PartitionSpec as P

BLOCK = 256
SIDE = 4
FIRST = 640
BACK = 512
THIN = 128
PIECES = ((0, 256, 256), (256, 256, 256), (512, THIN, 128))
EAGER = 12
DEEP = 4
F32 = jnp.float32
BF16 = jnp.bfloat16
MESH = pl.DeviceIdType.MESH
NN = (((1,), (0,)), ((), ()))
NT = (((1,), (1,)), ((), ()))
TN = (((0,), (0,)), ((), ()))
VMEM_LIMIT = 60 * 1024 * 1024
GROUP = 4 * 1024 * 1024
CELL = 32 * 1024
SENDS = 9
RECVS = 88


def dot(a, b, dims=NN):
    return lax.dot_general(a, b, dims, preferred_element_type=F32)


def span(start, size, step):
    return pl.ds(pl.multiple_of(start, step), size)


class Net:
    def __init__(self, send, recv, meter, small, somewhere):
        self.send, self.recv, self.somewhere = send, recv, somewhere
        self.meter, self.small = meter, small
        self.names, self.total, self.groups, self.open = {}, 0, [], {}

    def index(self, name, width=1):
        if name not in self.names:
            self.names[name] = self.total
            self.total += width
        return self.names[name]

    def lane(self, kind, when, size):
        group = self.open.get(kind)
        if group is None or self.groups[group][1] + size > GROUP:
            self.open[kind] = group = len(self.groups)
            self.groups.append([when, 0])
        self.groups[group][1] += size
        return group

    def copy(self, src, dst, lane, slot, where):
        return pltpu.make_async_remote_copy(
            src_ref=src, dst_ref=dst, send_sem=self.send.at[lane], recv_sem=self.recv.at[slot],
            device_id=where, device_id_type=MESH,
        )

    def start(self, name, src, dst, where, offset=0, width=1, when=None):
        slot = self.index(name, width) + offset
        size = 2 if src.dtype == BF16 else 4
        for extent in src.shape:
            size *= extent
        lane = self.lane(id(when) if size % CELL == 0 else name, when, size)
        if when is None:
            self.copy(src, dst, lane, slot, where).start()
        else:
            pl.when(when)(lambda: self.copy(src, dst, lane, slot, where).start())

    def wait(self, name, dst, offset=0, width=1, when=None):
        slot = self.index(name, width) + offset
        if when is None:
            self.copy(dst, dst, 0, slot, self.somewhere).wait_recv()
        else:
            pl.when(when)(lambda: self.copy(dst, dst, 0, slot, self.somewhere).wait_recv())

    def drain(self):
        for lane, (when, size) in enumerate(self.groups):
            ref = self.meter.at[pl.ds(0, size // (2 * self.meter.shape[1]))] if size % CELL == 0 else self.small

            def run():
                self.copy(ref, ref, lane, 0, self.somewhere).wait_send()

            if when is None:
                run()
            else:
                pl.when(when)(run)


def whole_kernel(
    rate, h_far, c_far, wq, wk, wv, dh, dq, dk, dv,
    h_all, c_all, w_all, w_turn, p_all, g_all, g_turn, state, back, rates, inner, inner_t, decays,
    pout, pin, psum, ra1, ra2, ra3, rb0, rb1, rb2, dbuf,
    ysend, yone, yhome, yr1, yr2, yout, yend, h_in, c_in, w_in, local, send, recv,
):
    s = lax.axis_index("sp")
    d = lax.axis_index("dp")
    z, x = s // SIDE, s % SIDE
    y, c = d // 2, d % 2
    u = x // 2
    xl = x - 2 * u
    own = c == u
    away = c != u
    rows, width = h_in.shape
    depth, columns = wq.shape
    half = width // 2
    four = rows * SIDE
    two = rows * 2
    blocks = SIDE * SIDE
    scale = columns ** (-0.5)

    def at(zz=None, xx=None, yy=None, cc=None):
        zz, xx = z if zz is None else zz, x if xx is None else xx
        yy, cc = y if yy is None else yy, c if cc is None else cc
        return {"sp": zz * SIDE + xx, "dp": yy * 2 + cc}

    def turned(v, by):
        return (v + by + SIDE) % SIDE

    mate = at(cc=1 - c)
    pair = at(xx=x + 1 - 2 * xl)
    zs = {1: at(zz=turned(z, 1)), -1: at(zz=turned(z, -1))}
    ys = {1: at(yy=turned(y, 1)), -1: at(yy=turned(y, -1))}
    cross = 3 - x
    net = Net(send, recv, h_all, rates.at[0], mate)
    weights = [w_in.at[j] for j in range(3)]
    loads = [
        pltpu.make_async_copy(src, dst, local.at[i])
        for i, (src, dst) in enumerate(zip((h_far, wq, wk, wv, c_far), [h_in] + weights + [c_in]))
    ]
    for load in loads:
        load.start()

    barrier = pltpu.get_barrier_semaphore()
    peers = [mate, ys[1], ys[-1]]
    for k in range(1, blocks):
        other = (s + k) % blocks
        peers += [{"sp": other, "dp": d}, {"sp": other, "dp": y * 2 + 1 - c}]
    for where in peers:
        pl.semaphore_signal(barrier, inc=1, device_id=where, device_id_type=MESH)
    rates[0] = jnp.full(rates.shape[1:], rate[0], F32)
    loads[0].wait()
    pl.semaphore_wait(barrier, len(peers))

    def r_rows(r):
        return span(turned(z, r) * four, four, four)

    def slot(r, col, b):
        return turned(z, r) * SIDE + 2 * (xl if col == 0 else 1 - xl) + b

    def h_ref(place, part, which):
        base = which * half
        lo, size = {"f": (0, half), "a": (0, FIRST), "b": (FIRST, half - FIRST)}[part]
        return h_all.at[span(place * rows, rows, rows), span(base + lo, size, 128)]

    def h_send(r, col, b, part, where, name):
        ref = h_ref(slot(r, col, b), part, c)
        net.start(name, ref, ref, where)

    def to_mate(r, col, b, part):
        h_send(r, col, b, part, mate, ("m", r))

    def h_wait(r, col, b, part, when=None):
        net.wait(("x", r, col, b, part), h_ref(slot(r, col, b), part, c), when=when)

    def w_ref(yy, cc, j):
        return w_all.at[span((yy * 2 + cc) * depth, depth, depth), pl.ds(j * columns, columns)]

    def w_near(j):
        net.start(("w0", j), weights[j], w_ref(y, c, j), mate, offset=c, width=2, when=away)

    def w_cross(j, who):
        net.start(("w0", j), weights[j], w_ref(y, c, j), at(xx=cross, cc=u), offset=c, width=2, when=who)

    mine = span(c * half, half, half)
    theirs = span((1 - c) * half, half, half)
    net.start(("x", 0, 0, 0, "f"), h_in.at[:, theirs], h_ref(slot(0, 0, 0), "f", 1 - c), mate, when=own)
    there = z * SIDE + 2 * (1 - xl) + 1
    for hf in range(2):
        net.start(
            ("x", 0, 0, 1, "f"), h_in.at[:, pl.ds(hf * half, half)], h_ref(there, "f", hf),
            at(xx=cross, cc=hf), when=away,
        )
    for load in loads[1:4]:
        load.wait()
    for j in range(3):
        w_near(j)
    for j in range(3):
        w_cross(j, away)
    net.start(("rate",), rates.at[0], rates.at[1], at(xx=cross))

    @pl.when(own)
    def _():
        h_all[span(slot(0, 0, 0) * rows, rows, rows), mine] = h_in[:, mine]
        for j in range(3):
            w_all[span(d * depth, depth, depth), j * columns : (j + 1) * columns] = weights[j][...]

    def spread(b):
        for way in (1, -1):
            h_send(0, 0, b, "f", zs[way], ("x", -way, 0, b, "f"))
        h_send(0, 0, b, "f", pair, ("x", 0, 1, b, "f"))
        to_mate(0, 0, b, "f")

    def w_spread(j, who):
        for cc in range(2):
            far = who if who is away else jnp.logical_and(own, c != cc)
            net.wait(("w0", j), w_ref(y, cc, j), offset=cc, width=2, when=far)
            for way in (1, -1):
                name = ("w1", j, -way) if (way == 1) == (cc == 0) else ("wt", j)
                net.start(name, w_ref(y, cc, j), w_ref(y, cc, j), ys[way], when=who)

    def w_forward(j, who):
        for way, cc in ((1, 0), (-1, 1)):
            ref = w_ref(turned(y, -way), cc, j)
            net.wait(("w1", j, -way), ref, when=who)
            net.start(("wt", j), ref, ref, ys[way], when=who)

    def from_pair(b):
        h_wait(0, 1, b, "f")
        for way in (1, -1):
            h_send(0, 1, b, "a", zs[way], ("x", -way, 1, b, "a"))
        to_mate(0, 1, b, "f")

    def from_side(b):
        for r in (-1, 1):
            h_wait(r, 0, b, "f")
            h_send(r, 0, b, "b", pair, ("x", r, 1, b, "b"))
            to_mate(r, 0, b, "f")

    def side_forward(b):
        fast = 1 if b == 0 else -1
        h_send(-fast, 0, b, "f", zs[fast], ("x", 2, 0, b, "f"))

    def from_corner(b):
        fast = 1 if b == 0 else -1
        for r in (-fast, fast):
            h_wait(r, 1, b, "a")
            if r == -fast:
                h_send(r, 1, b, "a", zs[fast], ("x", 2, 1, b, "a"))
            to_mate(r, 1, b, "a")

    def from_far(b):
        h_wait(2, 0, b, "f")
        h_send(2, 0, b, "b", pair, ("x", 2, 1, b, "b"))
        to_mate(2, 0, b, "f")

    def c_send(dz, dx):
        hz, hx = turned(z, dz), turned(x, dx)
        head = hz * SIDE + hx
        far = (hx // 2 - c) * (hx // 2 - c)
        net.start(
            ("c",), c_in.at[:, span(head * columns, columns, columns)],
            c_all.at[span(s * rows, rows, rows)],
            {"sp": hz * SIDE + hx + far * (3 - 2 * hx), "dp": y * 2 + c + far * (1 - 2 * c)},
            when=away if (dz, dx) == (0, 0) else None,
        )

    diagonal = [(dz, (dz + k) % SIDE) for k in range(SIDE) for dz in (2, 1, 3, 0)]

    h_wait(0, 0, 0, "f", when=away)
    spread(0)
    for j in range(3):
        w_spread(j, own)
    h_wait(0, 0, 1, "f")
    spread(1)
    for j in range(3):
        w_cross(j, own)
    from_side(0)
    from_pair(0)
    w_forward(0, own)
    w_spread(0, away)
    from_side(1)
    from_pair(1)
    side_forward(0)
    side_forward(1)
    w_forward(1, own)
    w_spread(1, away)
    w_forward(2, own)
    w_spread(2, away)

    def w_ready(j):
        net.wait(("wt", j), w_all.at[pl.ds(0, 4 * depth), pl.ds(j * columns, columns)])

    def mate_wait(r):
        net.wait(("m", r), h_all.at[r_rows(r), theirs])

    def project(row, j):
        place = span(row * four, four, four)
        cols = span(j * columns, columns, columns)
        value = dot(h_all[place, :], w_all[:, cols]).astype(BF16)
        factor = jnp.where(j == 1, scale, 1.0).astype(F32)
        p_all[place, cols] = (value.astype(F32) * factor).astype(BF16)

    def turn_weight(j):
        @pl.loop(0, SIDE)
        def _(t):
            place = span(t * 2 * depth, 2 * depth, 2 * depth)
            w_turn[pl.ds(j * columns, columns), place] = w_all[place, pl.ds(j * columns, columns)].T

    def project_near(j):
        @pl.loop(0, 3)
        def _(t):
            project(turned(z, t + t // 2), j)

    def betas(b):
        for r in (-1, 1):
            h_wait(r, 1, b, "b")
            to_mate(r, 1, b, "b")

    def fars(part):
        for b in range(2):
            h_wait(2, 1, b, part)
            to_mate(2, 1, b, part)

    from_corner(0)
    betas(0)
    w_forward(0, away)
    from_corner(1)
    loads[4].wait()
    for dz, dx in diagonal[:EAGER]:
        c_send(dz, dx)
    betas(1)
    w_forward(1, away)
    w_forward(2, away)
    for r in (0, 1, -1):
        mate_wait(r)
    w_ready(0)
    project_near(0)
    turn_weight(0)
    from_far(0)
    from_far(1)
    for dz, dx in diagonal[EAGER:]:
        c_send(dz, dx)

    @pl.when(own)
    def _():
        c_all[span(s * rows, rows, rows), :] = c_in[:, span(s * columns, columns, columns)]

    w_ready(1)
    project_near(1)
    w_ready(2)
    project_near(2)
    fars("a")
    fars("b")
    turn_weight(1)
    turn_weight(2)
    mate_wait(2)
    @pl.loop(0, 3)
    def _(j):
        project(turned(z, 2), j)

    net.wait(("rate",), rates.at[1])
    for who, taken in ((own, blocks - 1), (away, blocks)):
        net.wait(("c",), c_all.at[pl.ds(0, taken * rows)], when=who)

    pick = jnp.where(own, 1.0, 0.0).astype(F32)
    g = rates[0] * pick + rates[1] * (1.0 - pick)
    g_row = g[0:1, :]
    gap = (
        lax.broadcasted_iota(jnp.int32, (BLOCK, BLOCK), 0) - lax.broadcasted_iota(jnp.int32, (BLOCK, BLOCK), 1)
    ).astype(F32)
    place = lax.broadcasted_iota(jnp.int32, (BLOCK, columns), 0).astype(F32)
    inner[...] = jnp.where(gap >= 0, jnp.exp(g_row * jnp.maximum(gap, 0.0)), 0.0)
    inner_t[...] = jnp.where(gap <= 0, jnp.exp(g_row * jnp.maximum(-gap, 0.0)), 0.0)
    decays[0] = jnp.exp(g_row * (place + 1.0))
    decays[1] = jnp.exp(g_row * (BLOCK - 1.0 - place))
    block_decay = jnp.exp(g_row * BLOCK)
    state[...] = jnp.zeros_like(state)
    back[...] = jnp.zeros_like(back)
    parts = [slice(j * columns, (j + 1) * columns) for j in range(3)]
    count = BLOCK // rows

    def slots(i):
        places = []
        for w in range(count):
            p = i * count + w
            pz, px = p // SIDE, p % SIDE
            b = (px // 2 - u) * (px // 2 - u)
            places.append(span((pz * SIDE + 2 * (px + b * (3 - 2 * px) - 2 * u) + b) * rows, rows, rows))
        return places

    def get(places, part):
        return jnp.concatenate([p_all[place, part] for place in places], axis=0)

    def put(places, part, grad):
        grad = grad.astype(BF16)
        for w, place in enumerate(places):
            g_all[place, part] = grad[w * rows : (w + 1) * rows]
        grad = grad.T
        for w, place in enumerate(places):
            g_turn[part, place] = grad[:, w * rows : (w + 1) * rows]

    def forward(i):
        places = slots(i)
        k, v = get(places, parts[1]), get(places, parts[2])
        ct = c_all[span(i * BLOCK, BLOCK, BLOCK), :]
        mixed = (dot(ct, v, NT) * inner[...]).astype(BF16)
        held = state[...]
        grad_q = dot(mixed, k) + dot(ct, held.astype(BF16), NT) * decays[0]
        weighted = (k.astype(F32) * decays[1]).astype(BF16)
        state[...] = held * block_decay + dot(weighted, v, TN)
        put(places, parts[0], grad_q)

    def backward(i):
        places = slots(i)
        q, k, v = (get(places, part) for part in parts)
        ct = c_all[span(i * BLOCK, BLOCK, BLOCK), :]
        mixed_t = (dot(v, ct, NT) * inner_t[...]).astype(BF16)
        scores_t = (dot(k, q, NT) * inner_t[...]).astype(BF16)
        held = back[...]
        held_bf = held.astype(BF16)
        grad_v = dot(scores_t, ct) + dot(k, held_bf) * decays[1]
        grad_k = (dot(mixed_t, q) + dot(v, held_bf, NT) * decays[1]) * scale
        weighted = (q.astype(F32) * decays[0]).astype(BF16)
        back[...] = held * block_decay + dot(weighted, ct, TN)
        put(places, parts[1], grad_k)
        put(places, parts[2], grad_v)

    steps = rows * blocks // BLOCK

    @pl.loop(0, steps // DEEP)
    def _(t):
        for w in range(DEEP):
            forward(DEEP * t + w)
            backward(steps - 1 - DEEP * t - w)

    pieces = tuple(pl.ds(first, size) for first, size, _ in PIECES)
    tall = tuple(size for _, _, size in PIECES)
    late = (pl.ds(BACK + THIN, half - BACK - THIN), pl.ds(BACK, half - BACK))
    wide = tuple(pl.ds(0, cols.size) for cols in late)
    chunk = half // 2

    def pick_rows(r, hf):
        return span(turned(z, r) * four + hf * two, two, two)

    def other(r, i):
        cols = span(i * chunk, chunk, chunk)
        value = dot(g_all[r_rows(r), :], w_turn[:, span((1 - c) * half + i * chunk, chunk, chunk)])
        pout[r_rows(r), cols] = value.astype(BF16)
        net.start(("p", r, i), pout.at[r_rows(r), cols], pin.at[r_rows(r), cols], mate)

    def summed(r, i):
        cols = span(i * chunk, chunk, chunk)
        net.wait(("p", r, i), pin.at[r_rows(r), cols])
        value = dot(g_all[r_rows(r), :], w_turn[:, span(c * half + i * chunk, chunk, chunk)])
        psum[r_rows(r), cols] = (value + pin[r_rows(r), cols].astype(F32)).astype(BF16)
        if i == 1:
            for b in range(2):
                net.start(("b0", r, b), psum.at[b_rows(r, b, 1 - xl), late[b]], b0(r, b), pair)

    def add(place, cols, *refs):
        total = psum[place, cols].astype(F32)
        for ref in refs:
            total = total + ref.astype(F32)
        psum[place, cols] = total.astype(BF16)

    def a_rows(i, r, hf):
        return span(turned(z, r) * four + hf * two, tall[i], tall[i])

    def a1(i, e):
        return ra1.at[e, pl.ds(0, tall[i]), pieces[i]]

    def a2(i, e, hf):
        return ra2.at[e, pl.ds(hf * tall[i], tall[i]), pieces[i]]

    def a3(i):
        return ra3.at[pl.ds(0, tall[i]), pieces[i]]

    def alpha_send(i, r, hf, way, name, dst):
        net.start(name, psum.at[a_rows(i, r, hf), pieces[i]], dst, zs[way])

    def alpha_first(i):
        alpha_send(i, 2, 0, 1, ("a1", i, 0), a1(i, 0))
        alpha_send(i, 2, 1, -1, ("a1", i, 1), a1(i, 1))

    def alpha_plain(i, r):
        e = 0 if r == 1 else 1
        alpha_send(i, r, 1 - e, r, ("a2", i), a2(i, e, 1 - e))

    def alpha_added(i):
        for e, r in ((0, 1), (1, -1)):
            net.wait(("a1", i, e), a1(i, e))
            add(a_rows(i, r, e), pieces[i], a1(i, e)[...])
            alpha_send(i, r, e, r, ("a2", i), a2(i, e, e))

    def alpha_last(i):
        net.wait(("a2", i), ra2.at[:, pl.ds(0, 2 * tall[i]), pieces[i]])
        for hf in range(2):
            add(a_rows(i, 0, hf), pieces[i], a2(i, 0, hf)[...], a2(i, 1, hf)[...])
        net.start(("a3", i), psum.at[a_rows(i, 0, 1 - xl), pieces[i]], a3(i), pair)

    def deliver(cols, near, far):
        dst = dbuf.at[c, :, cols]
        if far:
            net.start(("d",), psum.at[b_rows(0, 1), cols], dst, at(xx=cross, cc=u), offset=c, width=2)
        if near:
            net.start(("d",), psum.at[b_rows(0, 0), cols], dst, mate, offset=c, width=2, when=away)

    def alpha_deliver(i):
        net.wait(("a3", i), a3(i))
        add(a_rows(i, 0, xl), pieces[i], a3(i)[...])
        deliver(pieces[i], True, tall[i] == two)

    def b_rows(r, b, side=xl):
        return span(turned(z, r) * four + side * two + b * rows, rows, rows)

    def b0(r, b):
        return rb0.at[r % SIDE, pl.ds(b * rows, rows), wide[b]]

    def b1(b):
        return rb1.at[b, :, wide[b]]

    def b2(e, b):
        return rb2.at[e, pl.ds(b * rows, rows), wide[b]]

    def beta_send(r, b, way, name, dst):
        net.start(name, psum.at[b_rows(r, b), late[b]], dst, zs[way])

    def beta_take(r):
        for b in range(2):
            net.wait(("b0", r, b), b0(r, b))
            add(b_rows(r, b), late[b], b0(r, b)[...])

    def beta_first():
        beta_take(2)
        beta_send(2, 0, 1, ("b1", 0), b1(0))
        beta_send(2, 1, -1, ("b1", 1), b1(1))

    def beta_plain():
        for r, b, e in ((1, 1, 0), (-1, 0, 1)):
            beta_take(r)
            beta_send(r, b, r, ("b2", b), b2(e, b))

    def beta_added():
        for r, b, e in ((1, 0, 0), (-1, 1, 1)):
            net.wait(("b1", e), b1(e))
            add(b_rows(r, b), late[b], b1(e)[...])
            beta_send(r, b, r, ("b2", b), b2(e, b))

    def beta_last():
        beta_take(0)
        for b in (1, 0):
            net.wait(("b2", b), rb2.at[:, pl.ds(b * rows, rows), wide[b]])
            add(b_rows(0, b), late[b], b2(0, b)[...], b2(1, b)[...])
            deliver(late[b], b == 0, b == 1)

    lanes = [pl.ds(hf * depth, depth) for hf in range(2)]

    def w_grad(r, j):
        cols = span(turned(y, r) * 2 * depth, 2 * depth, depth)
        return dot(g_turn[parts[j], :], h_all[:, cols])

    def y_first(j):
        ysend[j] = w_grad(2, j).astype(BF16)
        for e, way in ((0, 1), (1, -1)):
            net.start(("y1", j, e), ysend.at[j, :, lanes[e]], yr1.at[j, e], ys[way])

    def y2(j, e, hf):
        return yr2.at[j, e, :, lanes[hf]]

    def y_second(j):
        for e, r in ((0, 1), (1, -1)):
            value = w_grad(r, j)
            keep = value[:, e * depth : (e + 1) * depth]
            yone[j, e, :, lanes[1 - e]] = value[:, (1 - e) * depth : (2 - e) * depth].astype(BF16)
            net.start(("y2", j), yone.at[j, e, :, lanes[1 - e]], y2(j, e, 1 - e), ys[r])
            net.wait(("y1", j, e), yr1.at[j, e])
            yone[j, e, :, lanes[e]] = (keep + yr1[j, e].astype(F32)).astype(BF16)
            net.start(("y2", j), yone.at[j, e, :, lanes[e]], y2(j, e, e), ys[r])

    def y_home(j):
        yhome[j] = w_grad(0, j)

    def y_last(j):
        net.wait(("y2", j), yr2.at[j])
        total = yhome[j] + yr2[j, 0].astype(F32) + yr2[j, 1].astype(F32)
        yhome[j] = total
        yout[j] = total.astype(BF16)
        half_of = span((1 - c) * depth, depth, depth)
        net.start(("e", 0), yout.at[j, :, half_of], yend.at[j, 0], mate, when=own)
        for hf in range(2):
            net.start(("e", 1), yout.at[j, :, lanes[hf]], yend.at[j, 1], at(xx=cross, cc=hf), when=away)

    y_first(0)
    other(2, 0)
    other(2, 1)
    y_first(1)
    summed(2, 0)
    alpha_first(0)
    alpha_first(1)
    summed(2, 1)
    alpha_first(2)
    y_first(2)
    other(1, 0)
    other(-1, 0)
    other(1, 1)
    other(-1, 1)
    summed(1, 0)
    alpha_plain(0, 1)
    summed(-1, 0)
    alpha_plain(0, -1)
    y_second(0)
    summed(1, 1)
    summed(-1, 1)
    beta_first()
    alpha_added(0)
    alpha_plain(1, 1)
    alpha_plain(1, -1)
    alpha_plain(2, 1)
    alpha_plain(2, -1)
    y_second(1)
    other(0, 0)
    other(0, 1)
    alpha_added(1)
    alpha_added(2)
    y_second(2)
    summed(0, 0)
    y_home(0)
    y_last(0)
    alpha_last(0)
    summed(0, 1)
    y_home(1)
    y_home(2)
    y_last(1)
    alpha_last(2)
    beta_plain()
    beta_added()
    alpha_last(1)
    alpha_deliver(0)
    alpha_deliver(2)
    y_last(2)
    beta_last()
    alpha_deliver(1)

    net.wait(("e", 1), yend.at[:, 1])
    net.wait(("e", 0), yend.at[:, 0], when=away)

    @pl.when(own)
    def _():
        here = span(c * depth, depth, depth)
        for j, out in enumerate((dq, dk, dv)):
            out[...] = (yhome[j, :, here] + yend[j, 1].astype(F32)).T * 0.125

    @pl.when(away)
    def _():
        for j, out in enumerate((dq, dk, dv)):
            out[...] = (yend[j, 0].astype(F32) + yend[j, 1].astype(F32)).T * 0.125

    for hf in range(2):
        net.wait(("d",), dbuf.at[hf], offset=hf, width=2, when=jnp.logical_or(away, c != hf))

    @pl.when(own)
    def _():
        dbuf[c] = psum[b_rows(0, 0), :]

    for hf in range(2):
        dh[:, hf * half : (hf + 1) * half] = dbuf[hf]
    net.drain()
    assert len(net.groups) <= SENDS and net.total <= RECVS, (len(net.groups), net.total)


def whole(rate, h, c, wq, wk, wv):
    rows, width = h.shape
    depth, columns = wq.shape
    blocks = SIDE * SIDE
    length = rows * blocks
    half = width // 2
    rest = half - BACK
    vmem = pl.BlockSpec(memory_space=pltpu.VMEM)
    dma = pltpu.SemaphoreType.DMA

    def buf(*shape, kind=BF16):
        return pltpu.VMEM(shape, kind)

    return pl.pallas_call(
        whole_kernel,
        out_shape=(buf(rows, width),) + (buf(depth, columns, kind=F32),) * 3,
        in_specs=[pl.BlockSpec(memory_space=pltpu.SMEM)] + [pl.BlockSpec(memory_space=pl.ANY)] * 5,
        out_specs=(vmem,) * 4,
        scratch_shapes=[
            buf(length, width),
            buf(length, columns),
            buf(depth * 8, 3 * columns),
            buf(3 * columns, depth * 8),
            buf(length, 3 * columns),
            buf(length, 3 * columns),
            buf(3 * columns, length),
            buf(columns, columns, kind=F32),
            buf(columns, columns, kind=F32),
            buf(2, 8, columns, kind=F32),
            buf(BLOCK, BLOCK, kind=F32),
            buf(BLOCK, BLOCK, kind=F32),
            buf(2, BLOCK, columns, kind=F32),
            buf(length, half),
            buf(length, half),
            buf(length, half),
            buf(2, 2 * rows, BACK + THIN),
            buf(2, 4 * rows, BACK + THIN),
            buf(2 * rows, BACK + THIN),
            buf(SIDE, 2 * rows, rest),
            buf(2, rows, rest),
            buf(2, 2 * rows, rest),
            buf(2, rows, half),
            buf(3, columns, 2 * depth),
            buf(3, 2, columns, 2 * depth),
            buf(3, columns, 2 * depth, kind=F32),
            buf(3, 2, columns, depth),
            buf(3, 2, columns, 2 * depth),
            buf(3, columns, 2 * depth),
            buf(3, 2, columns, depth),
            buf(rows, width),
            buf(rows, columns * blocks),
            buf(3, depth, columns),
            dma((5,)),
            dma((SENDS,)),
            dma((RECVS,)),
        ],
        compiler_params=pltpu.CompilerParams(
            collective_id=0, has_side_effects=True, vmem_limit_bytes=VMEM_LIMIT
        ),
        name="whole",
    )(rate, h, c, wq, wk, wv)


def finish_kernel(count, *refs):
    ins, outs, sems = refs[:count], refs[count : 2 * count], refs[2 * count]
    moves = [pltpu.make_async_copy(ins[i], outs[i], sems.at[i]) for i in range(count)]
    for move in moves:
        move.start()
    for move in moves:
        move.wait()


def finish(*arrays):
    count = len(arrays)
    return pl.pallas_call(
        functools.partial(finish_kernel, count),
        out_shape=tuple(jax.ShapeDtypeStruct(a.shape, a.dtype) for a in arrays),
        in_specs=[pl.BlockSpec(memory_space=pltpu.VMEM)] * count,
        out_specs=(pl.BlockSpec(memory_space=pl.ANY),) * count,
        scratch_shapes=[pltpu.SemaphoreType.DMA((count,))],
        compiler_params=pltpu.CompilerParams(vmem_limit_bytes=4 * 1024 * 1024),
        name="finish",
    )(*arrays)


def body(hidden_in, mix_cotangent, query_weight, key_weight, value_weight, decay_log):
    dh, dq, dk, dv = finish(
        *whole(decay_log, hidden_in[0], mix_cotangent[0], query_weight, key_weight, value_weight)
    )
    return dh[None], dq, dk, dv


def solution(mesh):
    placed = (
        P("dp", "sp", None),
        P("dp", "sp", None),
        P("dp", "sp"),
        P("dp", "sp"),
        P("dp", "sp"),
        P("sp"),
    )
    return jax.shard_map(
        body,
        mesh=mesh,
        in_specs=placed,
        out_specs=(P("dp", "sp", None), P("dp", "sp"), P("dp", "sp"), P("dp", "sp")),
        check_vma=False,
    )
```

```python
import functools

import jax
import jax.numpy as jnp
from jax import lax
from jax.experimental import pallas as pl
from jax.experimental.pallas import tpu as pltpu
from jax.sharding import PartitionSpec as P

BLOCK = 256
SIDE = 4
FIRST = 512
BACK = 512
PIECES = ((0, 256), (256, 256))
EAGER = 12
DEEP = 4
F32 = jnp.float32
BF16 = jnp.bfloat16
MESH = pl.DeviceIdType.MESH
NN = (((1,), (0,)), ((), ()))
NT = (((1,), (1,)), ((), ()))
TN = (((0,), (0,)), ((), ()))
VMEM_LIMIT = 60 * 1024 * 1024
GROUP = 4 * 1024 * 1024
CELL = 32 * 1024
SENDS = 9
RECVS = 79


def dot(a, b, dims=NN):
    return lax.dot_general(a, b, dims, preferred_element_type=F32)


def span(start, size, step):
    return pl.ds(pl.multiple_of(start, step), size)


class Net:
    def __init__(self, send, recv, meter, small, somewhere):
        self.send, self.recv, self.somewhere = send, recv, somewhere
        self.meter, self.small = meter, small
        self.names, self.total, self.groups, self.open = {}, 0, [], {}

    def index(self, name, width=1):
        if name not in self.names:
            self.names[name] = self.total
            self.total += width
        return self.names[name]

    def lane(self, kind, when, size):
        group = self.open.get(kind)
        if group is None or self.groups[group][1] + size > GROUP:
            self.open[kind] = group = len(self.groups)
            self.groups.append([when, 0])
        self.groups[group][1] += size
        return group

    def copy(self, src, dst, lane, slot, where):
        return pltpu.make_async_remote_copy(
            src_ref=src, dst_ref=dst, send_sem=self.send.at[lane], recv_sem=self.recv.at[slot],
            device_id=where, device_id_type=MESH,
        )

    def start(self, name, src, dst, where, offset=0, width=1, when=None):
        slot = self.index(name, width) + offset
        size = 2 if src.dtype == BF16 else 4
        for extent in src.shape:
            size *= extent
        lane = self.lane(id(when) if size % CELL == 0 else name, when, size)
        if when is None:
            self.copy(src, dst, lane, slot, where).start()
        else:
            pl.when(when)(lambda: self.copy(src, dst, lane, slot, where).start())

    def wait(self, name, dst, offset=0, width=1, when=None):
        slot = self.index(name, width) + offset
        if when is None:
            self.copy(dst, dst, 0, slot, self.somewhere).wait_recv()
        else:
            pl.when(when)(lambda: self.copy(dst, dst, 0, slot, self.somewhere).wait_recv())

    def drain(self):
        for lane, (when, size) in enumerate(self.groups):
            ref = self.meter.at[pl.ds(0, size // (2 * self.meter.shape[1]))] if size % CELL == 0 else self.small

            def run():
                self.copy(ref, ref, lane, 0, self.somewhere).wait_send()

            if when is None:
                run()
            else:
                pl.when(when)(run)


def whole_kernel(
    rate, h_far, c_far, wq, wk, wv, dh, dq, dk, dv,
    h_all, c_all, w_all, w_turn, p_all, g_all, g_turn, state, back, rates, inner, inner_t, decays,
    pout, pin, psum, ra1, ra2, ra3, rb0, rb1, rb2, dbuf,
    ysend, yone, yhome, yr1, yr2, yout, yend, h_in, c_in, w_in, local, send, recv,
):
    s = lax.axis_index("sp")
    d = lax.axis_index("dp")
    z, x = s // SIDE, s % SIDE
    y, c = d // 2, d % 2
    u = x // 2
    xl = x - 2 * u
    own = c == u
    away = c != u
    rows, width = h_in.shape
    depth, columns = wq.shape
    half = width // 2
    four = rows * SIDE
    two = rows * 2
    blocks = SIDE * SIDE
    scale = columns ** (-0.5)

    def at(zz=None, xx=None, yy=None, cc=None):
        zz, xx = z if zz is None else zz, x if xx is None else xx
        yy, cc = y if yy is None else yy, c if cc is None else cc
        return {"sp": zz * SIDE + xx, "dp": yy * 2 + cc}

    def turned(v, by):
        return (v + by + SIDE) % SIDE

    mate = at(cc=1 - c)
    pair = at(xx=x + 1 - 2 * xl)
    zs = {1: at(zz=turned(z, 1)), -1: at(zz=turned(z, -1))}
    ys = {1: at(yy=turned(y, 1)), -1: at(yy=turned(y, -1))}
    cross = 3 - x
    net = Net(send, recv, h_all, rates.at[0], mate)
    weights = [w_in.at[j] for j in range(3)]
    loads = [
        pltpu.make_async_copy(src, dst, local.at[i])
        for i, (src, dst) in enumerate(zip((h_far, wq, wk, wv, c_far), [h_in] + weights + [c_in]))
    ]
    for load in loads:
        load.start()

    barrier = pltpu.get_barrier_semaphore()
    peers = [mate, ys[1], ys[-1]]
    for k in range(1, blocks):
        other = (s + k) % blocks
        peers += [{"sp": other, "dp": d}, {"sp": other, "dp": y * 2 + 1 - c}]
    for where in peers:
        pl.semaphore_signal(barrier, inc=1, device_id=where, device_id_type=MESH)
    rates[0] = jnp.full(rates.shape[1:], rate[0], F32)
    loads[0].wait()
    pl.semaphore_wait(barrier, len(peers))

    def r_rows(r):
        return span(turned(z, r) * four, four, four)

    def slot(r, col, b):
        return turned(z, r) * SIDE + 2 * (xl if col == 0 else 1 - xl) + b

    def h_ref(place, part, which):
        base = which * half
        lo, size = {"f": (0, half), "a": (0, FIRST), "b": (FIRST, half - FIRST)}[part]
        return h_all.at[span(place * rows, rows, rows), span(base + lo, size, 128)]

    def h_send(r, col, b, part, where, name):
        ref = h_ref(slot(r, col, b), part, c)
        net.start(name, ref, ref, where)

    def to_mate(r, col, b, part):
        h_send(r, col, b, part, mate, ("m", r))

    def h_wait(r, col, b, part, when=None):
        net.wait(("x", r, col, b, part), h_ref(slot(r, col, b), part, c), when=when)

    def w_ref(yy, cc, j):
        return w_all.at[span((yy * 2 + cc) * depth, depth, depth), pl.ds(j * columns, columns)]

    def w_near(j):
        net.start(("w0", j), weights[j], w_ref(y, c, j), mate, offset=c, width=2, when=away)

    def w_cross(j, who):
        net.start(("w0", j), weights[j], w_ref(y, c, j), at(xx=cross, cc=u), offset=c, width=2, when=who)

    mine = span(c * half, half, half)
    theirs = span((1 - c) * half, half, half)
    net.start(("x", 0, 0, 0, "f"), h_in.at[:, theirs], h_ref(slot(0, 0, 0), "f", 1 - c), mate, when=own)
    there = z * SIDE + 2 * (1 - xl) + 1
    for hf in range(2):
        net.start(
            ("x", 0, 0, 1, "f"), h_in.at[:, pl.ds(hf * half, half)], h_ref(there, "f", hf),
            at(xx=cross, cc=hf), when=away,
        )
    for load in loads[1:4]:
        load.wait()
    for j in range(3):
        w_near(j)
    for j in range(3):
        w_cross(j, away)
    net.start(("rate",), rates.at[0], rates.at[1], at(xx=cross))

    @pl.when(own)
    def _():
        h_all[span(slot(0, 0, 0) * rows, rows, rows), mine] = h_in[:, mine]
        for j in range(3):
            w_all[span(d * depth, depth, depth), j * columns : (j + 1) * columns] = weights[j][...]

    def spread(b):
        for way in (1, -1):
            h_send(0, 0, b, "f", zs[way], ("x", -way, 0, b, "f"))
        h_send(0, 0, b, "f", pair, ("x", 0, 1, b, "f"))
        to_mate(0, 0, b, "f")

    def w_spread(j, who):
        for cc in range(2):
            far = who if who is away else jnp.logical_and(own, c != cc)
            net.wait(("w0", j), w_ref(y, cc, j), offset=cc, width=2, when=far)
            for way in (1, -1):
                name = ("w1", j, -way) if (way == 1) == (cc == 0) else ("wt", j)
                net.start(name, w_ref(y, cc, j), w_ref(y, cc, j), ys[way], when=who)

    def w_forward(j, who):
        for way, cc in ((1, 0), (-1, 1)):
            ref = w_ref(turned(y, -way), cc, j)
            net.wait(("w1", j, -way), ref, when=who)
            net.start(("wt", j), ref, ref, ys[way], when=who)

    def from_pair(b):
        h_wait(0, 1, b, "f")
        for way in (1, -1):
            h_send(0, 1, b, "a", zs[way], ("x", -way, 1, b, "a"))
        to_mate(0, 1, b, "f")

    def from_side(b):
        for r in (-1, 1):
            h_wait(r, 0, b, "f")
            h_send(r, 0, b, "b", pair, ("x", r, 1, b, "b"))
            to_mate(r, 0, b, "f")

    def side_forward(b):
        fast = 1 if b == 0 else -1
        h_send(-fast, 0, b, "f", zs[fast], ("x", 2, 0, b, "f"))

    def from_corner(b):
        fast = 1 if b == 0 else -1
        for r in (-fast, fast):
            h_wait(r, 1, b, "a")
            if r == -fast:
                h_send(r, 1, b, "a", zs[fast], ("x", 2, 1, b, "a"))
            to_mate(r, 1, b, "a")

    def from_far(b):
        h_wait(2, 0, b, "f")
        h_send(2, 0, b, "b", pair, ("x", 2, 1, b, "b"))
        to_mate(2, 0, b, "f")

    def c_send(dz, dx):
        hz, hx = turned(z, dz), turned(x, dx)
        head = hz * SIDE + hx
        far = (hx // 2 - c) * (hx // 2 - c)
        net.start(
            ("c",), c_in.at[:, span(head * columns, columns, columns)],
            c_all.at[span(s * rows, rows, rows)],
            {"sp": hz * SIDE + hx + far * (3 - 2 * hx), "dp": y * 2 + c + far * (1 - 2 * c)},
            when=away if (dz, dx) == (0, 0) else None,
        )

    diagonal = [(dz, (dz + k) % SIDE) for k in range(SIDE) for dz in (2, 1, 3, 0)]

    h_wait(0, 0, 0, "f", when=away)
    spread(0)
    for j in range(3):
        w_spread(j, own)
    h_wait(0, 0, 1, "f")
    spread(1)
    for j in range(3):
        w_cross(j, own)
    from_side(0)
    from_pair(0)
    w_forward(0, own)
    w_spread(0, away)
    from_side(1)
    from_pair(1)
    side_forward(0)
    side_forward(1)
    w_forward(1, own)
    w_spread(1, away)
    w_forward(2, own)
    w_spread(2, away)

    def w_ready(j):
        net.wait(("wt", j), w_all.at[pl.ds(0, 4 * depth), pl.ds(j * columns, columns)])

    def mate_wait(r):
        net.wait(("m", r), h_all.at[r_rows(r), theirs])

    def project(row, j):
        place = span(row * four, four, four)
        cols = span(j * columns, columns, columns)
        value = dot(h_all[place, :], w_all[:, cols]).astype(BF16)
        factor = jnp.where(j == 1, scale, 1.0).astype(F32)
        p_all[place, cols] = (value.astype(F32) * factor).astype(BF16)

    def turn_weight(j):
        @pl.loop(0, SIDE)
        def _(t):
            place = span(t * 2 * depth, 2 * depth, 2 * depth)
            w_turn[pl.ds(j * columns, columns), place] = w_all[place, pl.ds(j * columns, columns)].T

    def project_near(j):
        @pl.loop(0, 3)
        def _(t):
            project(turned(z, t + t // 2), j)

    def betas(b):
        for r in (-1, 1):
            h_wait(r, 1, b, "b")
            to_mate(r, 1, b, "b")

    def fars(part):
        for b in range(2):
            h_wait(2, 1, b, part)
            to_mate(2, 1, b, part)

    from_corner(0)
    betas(0)
    w_forward(0, away)
    from_corner(1)
    loads[4].wait()
    for dz, dx in diagonal[:EAGER]:
        c_send(dz, dx)
    betas(1)
    w_forward(1, away)
    w_forward(2, away)
    for r in (0, 1, -1):
        mate_wait(r)
    w_ready(0)
    project_near(0)
    turn_weight(0)
    from_far(0)
    from_far(1)
    for dz, dx in diagonal[EAGER:]:
        c_send(dz, dx)

    @pl.when(own)
    def _():
        c_all[span(s * rows, rows, rows), :] = c_in[:, span(s * columns, columns, columns)]

    w_ready(1)
    project_near(1)
    w_ready(2)
    project_near(2)
    fars("a")
    fars("b")
    turn_weight(1)
    turn_weight(2)
    mate_wait(2)
    @pl.loop(0, 3)
    def _(j):
        project(turned(z, 2), j)

    net.wait(("rate",), rates.at[1])
    for who, taken in ((own, blocks - 1), (away, blocks)):
        net.wait(("c",), c_all.at[pl.ds(0, taken * rows)], when=who)

    pick = jnp.where(own, 1.0, 0.0).astype(F32)
    g = rates[0] * pick + rates[1] * (1.0 - pick)
    g_row = g[0:1, :]
    gap = (
        lax.broadcasted_iota(jnp.int32, (BLOCK, BLOCK), 0) - lax.broadcasted_iota(jnp.int32, (BLOCK, BLOCK), 1)
    ).astype(F32)
    place = lax.broadcasted_iota(jnp.int32, (BLOCK, columns), 0).astype(F32)
    inner[...] = jnp.where(gap >= 0, jnp.exp(g_row * jnp.maximum(gap, 0.0)), 0.0)
    inner_t[...] = jnp.where(gap <= 0, jnp.exp(g_row * jnp.maximum(-gap, 0.0)), 0.0)
    decays[0] = jnp.exp(g_row * (place + 1.0))
    decays[1] = jnp.exp(g_row * (BLOCK - 1.0 - place))
    block_decay = jnp.exp(g_row * BLOCK)
    state[...] = jnp.zeros_like(state)
    back[...] = jnp.zeros_like(back)
    parts = [slice(j * columns, (j + 1) * columns) for j in range(3)]
    count = BLOCK // rows

    def slots(i):
        places = []
        for w in range(count):
            p = i * count + w
            pz, px = p // SIDE, p % SIDE
            b = (px // 2 - u) * (px // 2 - u)
            places.append(span((pz * SIDE + 2 * (px + b * (3 - 2 * px) - 2 * u) + b) * rows, rows, rows))
        return places

    def get(places, part):
        return jnp.concatenate([p_all[place, part] for place in places], axis=0)

    def put(places, part, grad):
        grad = grad.astype(BF16)
        for w, place in enumerate(places):
            g_all[place, part] = grad[w * rows : (w + 1) * rows]
        grad = grad.T
        for w, place in enumerate(places):
            g_turn[part, place] = grad[:, w * rows : (w + 1) * rows]

    def forward(i):
        places = slots(i)
        k, v = get(places, parts[1]), get(places, parts[2])
        ct = c_all[span(i * BLOCK, BLOCK, BLOCK), :]
        mixed = (dot(ct, v, NT) * inner[...]).astype(BF16)
        held = state[...]
        grad_q = dot(mixed, k) + dot(ct, held.astype(BF16), NT) * decays[0]
        weighted = (k.astype(F32) * decays[1]).astype(BF16)
        state[...] = held * block_decay + dot(weighted, v, TN)
        put(places, parts[0], grad_q)

    def backward(i):
        places = slots(i)
        q, k, v = (get(places, part) for part in parts)
        ct = c_all[span(i * BLOCK, BLOCK, BLOCK), :]
        mixed_t = (dot(v, ct, NT) * inner_t[...]).astype(BF16)
        scores_t = (dot(k, q, NT) * inner_t[...]).astype(BF16)
        held = back[...]
        held_bf = held.astype(BF16)
        grad_v = dot(scores_t, ct) + dot(k, held_bf) * decays[1]
        grad_k = (dot(mixed_t, q) + dot(v, held_bf, NT) * decays[1]) * scale
        weighted = (q.astype(F32) * decays[0]).astype(BF16)
        back[...] = held * block_decay + dot(weighted, ct, TN)
        put(places, parts[1], grad_k)
        put(places, parts[2], grad_v)

    steps = rows * blocks // BLOCK

    @pl.loop(0, steps // DEEP)
    def _(t):
        for w in range(DEEP):
            forward(DEEP * t + w)
            backward(steps - 1 - DEEP * t - w)

    pieces = tuple(pl.ds(first, size) for first, size in PIECES)
    beta = pl.ds(BACK, half - BACK)
    chunk = half // 2

    def pick_rows(r, hf):
        return span(turned(z, r) * four + hf * two, two, two)

    def other(r, i):
        cols = span(i * chunk, chunk, chunk)
        value = dot(g_all[r_rows(r), :], w_turn[:, span((1 - c) * half + i * chunk, chunk, chunk)])
        pout[r_rows(r), cols] = value.astype(BF16)
        net.start(("p", r, i), pout.at[r_rows(r), cols], pin.at[r_rows(r), cols], mate)

    def summed(r, i):
        cols = span(i * chunk, chunk, chunk)
        net.wait(("p", r, i), pin.at[r_rows(r), cols])
        value = dot(g_all[r_rows(r), :], w_turn[:, span(c * half + i * chunk, chunk, chunk)])
        psum[r_rows(r), cols] = (value + pin[r_rows(r), cols].astype(F32)).astype(BF16)
        if i == 1:
            net.start(("b0", r), psum.at[pick_rows(r, 1 - xl), beta], rb0.at[r % SIDE], pair)

    def add(place, cols, *refs):
        total = psum[place, cols].astype(F32)
        for ref in refs:
            total = total + ref.astype(F32)
        psum[place, cols] = total.astype(BF16)

    def a1(i, e):
        return ra1.at[e, :, pieces[i]]

    def a2(i, e, hf):
        return ra2.at[e, pl.ds(hf * two, two), pieces[i]]

    def a3(i):
        return ra3.at[:, pieces[i]]

    def alpha_send(i, r, hf, way, name, dst):
        net.start(name, psum.at[pick_rows(r, hf), pieces[i]], dst, zs[way])

    def alpha_first(i):
        alpha_send(i, 2, 0, 1, ("a1", i, 0), a1(i, 0))
        alpha_send(i, 2, 1, -1, ("a1", i, 1), a1(i, 1))

    def alpha_plain(i, r):
        e = 0 if r == 1 else 1
        alpha_send(i, r, 1 - e, r, ("a2", i), a2(i, e, 1 - e))

    def alpha_added(i):
        for e, r in ((0, 1), (1, -1)):
            net.wait(("a1", i, e), a1(i, e))
            add(pick_rows(r, e), pieces[i], a1(i, e)[...])
            alpha_send(i, r, e, r, ("a2", i), a2(i, e, e))

    def alpha_last(i):
        net.wait(("a2", i), ra2.at[:, :, pieces[i]])
        for hf in range(2):
            add(pick_rows(0, hf), pieces[i], a2(i, 0, hf)[...], a2(i, 1, hf)[...])
        net.start(("a3", i), psum.at[pick_rows(0, 1 - xl), pieces[i]], a3(i), pair)

    def deliver(cols):
        dst = dbuf.at[c, :, cols]
        net.start(("d",), psum.at[b_rows(0, 1), cols], dst, at(xx=cross, cc=u), offset=c, width=2)
        net.start(("d",), psum.at[b_rows(0, 0), cols], dst, mate, offset=c, width=2, when=away)

    def alpha_deliver(i):
        net.wait(("a3", i), a3(i))
        add(pick_rows(0, xl), pieces[i], a3(i)[...])
        deliver(pieces[i])

    def b_rows(r, b):
        return span(turned(z, r) * four + xl * two + b * rows, rows, rows)

    def b2(e, b):
        return rb2.at[e, pl.ds(b * rows, rows)]

    def beta_send(r, b, way, name, dst):
        net.start(name, psum.at[b_rows(r, b), beta], dst, zs[way])

    def beta_take(r):
        net.wait(("b0", r), rb0.at[r % SIDE])
        add(pick_rows(r, xl), beta, rb0[r % SIDE])

    def beta_first():
        beta_take(2)
        beta_send(2, 0, 1, ("b1", 0), rb1.at[0])
        beta_send(2, 1, -1, ("b1", 1), rb1.at[1])

    def beta_plain():
        for r, b, e in ((1, 1, 0), (-1, 0, 1)):
            beta_take(r)
            beta_send(r, b, r, ("b2",), b2(e, b))

    def beta_added():
        for r, b, e in ((1, 0, 0), (-1, 1, 1)):
            net.wait(("b1", e), rb1.at[e])
            add(b_rows(r, b), beta, rb1[e])
            beta_send(r, b, r, ("b2",), b2(e, b))

    def beta_last():
        beta_take(0)
        net.wait(("b2",), rb2)
        add(pick_rows(0, xl), beta, rb2[0], rb2[1])
        deliver(beta)

    lanes = [pl.ds(hf * depth, depth) for hf in range(2)]

    def w_grad(r, j):
        cols = span(turned(y, r) * 2 * depth, 2 * depth, depth)
        return dot(g_turn[parts[j], :], h_all[:, cols])

    def y_first(j):
        ysend[j] = w_grad(2, j).astype(BF16)
        for e, way in ((0, 1), (1, -1)):
            net.start(("y1", j, e), ysend.at[j, :, lanes[e]], yr1.at[j, e], ys[way])

    def y2(j, e, hf):
        return yr2.at[j, e, :, lanes[hf]]

    def y_second(j):
        for e, r in ((0, 1), (1, -1)):
            value = w_grad(r, j)
            keep = value[:, e * depth : (e + 1) * depth]
            yone[j, e, :, lanes[1 - e]] = value[:, (1 - e) * depth : (2 - e) * depth].astype(BF16)
            net.start(("y2", j), yone.at[j, e, :, lanes[1 - e]], y2(j, e, 1 - e), ys[r])
            net.wait(("y1", j, e), yr1.at[j, e])
            yone[j, e, :, lanes[e]] = (keep + yr1[j, e].astype(F32)).astype(BF16)
            net.start(("y2", j), yone.at[j, e, :, lanes[e]], y2(j, e, e), ys[r])

    def y_home(j):
        yhome[j] = w_grad(0, j)

    def y_last(j):
        net.wait(("y2", j), yr2.at[j])
        total = yhome[j] + yr2[j, 0].astype(F32) + yr2[j, 1].astype(F32)
        yhome[j] = total
        yout[j] = total.astype(BF16)
        half_of = span((1 - c) * depth, depth, depth)
        net.start(("e", 0), yout.at[j, :, half_of], yend.at[j, 0], mate, when=own)
        for hf in range(2):
            net.start(("e", 1), yout.at[j, :, lanes[hf]], yend.at[j, 1], at(xx=cross, cc=hf), when=away)

    y_first(0)
    other(2, 0)
    other(2, 1)
    y_first(1)
    summed(2, 0)
    alpha_first(0)
    alpha_first(1)
    summed(2, 1)
    y_first(2)
    other(1, 0)
    other(-1, 0)
    other(1, 1)
    other(-1, 1)
    summed(1, 0)
    alpha_plain(0, 1)
    summed(-1, 0)
    alpha_plain(0, -1)
    y_second(0)
    summed(1, 1)
    summed(-1, 1)
    beta_first()
    alpha_added(0)
    alpha_plain(1, 1)
    alpha_plain(1, -1)
    y_second(1)
    other(0, 0)
    other(0, 1)
    alpha_added(1)
    y_second(2)
    summed(0, 0)
    y_home(0)
    y_last(0)
    alpha_last(0)
    summed(0, 1)
    y_home(1)
    y_home(2)
    y_last(1)
    beta_plain()
    beta_added()
    alpha_last(1)
    alpha_deliver(0)
    y_last(2)
    beta_last()
    alpha_deliver(1)

    net.wait(("e", 1), yend.at[:, 1])
    net.wait(("e", 0), yend.at[:, 0], when=away)

    @pl.when(own)
    def _():
        here = span(c * depth, depth, depth)
        for j, out in enumerate((dq, dk, dv)):
            out[...] = (yhome[j, :, here] + yend[j, 1].astype(F32)).T * 0.125

    @pl.when(away)
    def _():
        for j, out in enumerate((dq, dk, dv)):
            out[...] = (yend[j, 0].astype(F32) + yend[j, 1].astype(F32)).T * 0.125

    for hf in range(2):
        net.wait(("d",), dbuf.at[hf], offset=hf, width=2, when=jnp.logical_or(away, c != hf))

    @pl.when(own)
    def _():
        dbuf[c] = psum[b_rows(0, 0), :]

    for hf in range(2):
        dh[:, hf * half : (hf + 1) * half] = dbuf[hf]
    net.drain()
    assert len(net.groups) <= SENDS and net.total <= RECVS, (len(net.groups), net.total)


def whole(rate, h, c, wq, wk, wv):
    rows, width = h.shape
    depth, columns = wq.shape
    blocks = SIDE * SIDE
    length = rows * blocks
    half = width // 2
    rest = half - BACK
    vmem = pl.BlockSpec(memory_space=pltpu.VMEM)
    dma = pltpu.SemaphoreType.DMA

    def buf(*shape, kind=BF16):
        return pltpu.VMEM(shape, kind)

    return pl.pallas_call(
        whole_kernel,
        out_shape=(buf(rows, width),) + (buf(depth, columns, kind=F32),) * 3,
        in_specs=[pl.BlockSpec(memory_space=pltpu.SMEM)] + [pl.BlockSpec(memory_space=pl.ANY)] * 5,
        out_specs=(vmem,) * 4,
        scratch_shapes=[
            buf(length, width),
            buf(length, columns),
            buf(depth * 8, 3 * columns),
            buf(3 * columns, depth * 8),
            buf(length, 3 * columns),
            buf(length, 3 * columns),
            buf(3 * columns, length),
            buf(columns, columns, kind=F32),
            buf(columns, columns, kind=F32),
            buf(2, 8, columns, kind=F32),
            buf(BLOCK, BLOCK, kind=F32),
            buf(BLOCK, BLOCK, kind=F32),
            buf(2, BLOCK, columns, kind=F32),
            buf(length, half),
            buf(length, half),
            buf(length, half),
            buf(2, 2 * rows, BACK),
            buf(2, 4 * rows, BACK),
            buf(2 * rows, BACK),
            buf(SIDE, 2 * rows, rest),
            buf(2, rows, rest),
            buf(2, 2 * rows, rest),
            buf(2, rows, half),
            buf(3, columns, 2 * depth),
            buf(3, 2, columns, 2 * depth),
            buf(3, columns, 2 * depth, kind=F32),
            buf(3, 2, columns, depth),
            buf(3, 2, columns, 2 * depth),
            buf(3, columns, 2 * depth),
            buf(3, 2, columns, depth),
            buf(rows, width),
            buf(rows, columns * blocks),
            buf(3, depth, columns),
            dma((5,)),
            dma((SENDS,)),
            dma((RECVS,)),
        ],
        compiler_params=pltpu.CompilerParams(
            collective_id=0, has_side_effects=True, vmem_limit_bytes=VMEM_LIMIT
        ),
        name="whole",
    )(rate, h, c, wq, wk, wv)


def finish_kernel(count, *refs):
    ins, outs, sems = refs[:count], refs[count : 2 * count], refs[2 * count]
    moves = [pltpu.make_async_copy(ins[i], outs[i], sems.at[i]) for i in range(count)]
    for move in moves:
        move.start()
    for move in moves:
        move.wait()


def finish(*arrays):
    count = len(arrays)
    return pl.pallas_call(
        functools.partial(finish_kernel, count),
        out_shape=tuple(jax.ShapeDtypeStruct(a.shape, a.dtype) for a in arrays),
        in_specs=[pl.BlockSpec(memory_space=pltpu.VMEM)] * count,
        out_specs=(pl.BlockSpec(memory_space=pl.ANY),) * count,
        scratch_shapes=[pltpu.SemaphoreType.DMA((count,))],
        compiler_params=pltpu.CompilerParams(vmem_limit_bytes=4 * 1024 * 1024),
        name="finish",
    )(*arrays)


def body(hidden_in, mix_cotangent, query_weight, key_weight, value_weight, decay_log):
    dh, dq, dk, dv = finish(
        *whole(decay_log, hidden_in[0], mix_cotangent[0], query_weight, key_weight, value_weight)
    )
    return dh[None], dq, dk, dv


def solution(mesh):
    placed = (
        P("dp", "sp", None),
        P("dp", "sp", None),
        P("dp", "sp"),
        P("dp", "sp"),
        P("dp", "sp"),
        P("sp"),
    )
    return jax.shard_map(
        body,
        mesh=mesh,
        in_specs=placed,
        out_specs=(P("dp", "sp", None), P("dp", "sp"), P("dp", "sp"), P("dp", "sp")),
        check_vma=False,
    )
```
